32 devices in a mesh: sp: 8 (over z, x), tp: 4 (over y, core).
Axes of the slice: x: 2, y: 2, z: 4, core: 2. Of those that a mesh axis runs over, the one named last changes fastest.
Arguments:
- target_rows: bfloat16 [512, 2048], P(('sp', 'tp')), may hold values from -6 to 6
- source_rows: bfloat16 [2048, 2048], P(('sp', 'tp')), may hold values from -6 to 6
- norm_gain: bfloat16 [2048], replicated, may hold values from 0.099609375 to 1.8984375
- query_weight: bfloat16 [2048, 4096], P(None, 'tp'), may hold values from -0.125 to 0.125
- key_weight: bfloat16 [2048, 4096], P(None, 'tp'), may hold values from -0.125 to 0.125
- value_weight: bfloat16 [2048, 4096], P(None, 'tp'), may hold values from -0.125 to 0.125
- output_weight: bfloat16 [4096, 2048], P('tp'), may hold values from -0.09375 to 0.09375
- saved_output: bfloat16 [512, 4096], P('sp', 'tp'), may hold values from -3 to 3
- norm_offset: bfloat16 [512, 16], P('sp', 'tp'), may hold values from 0.25 to 1.25
- output_grad: bfloat16 [512, 2048], P(('sp', 'tp')), may hold values from -192 to 192
Outputs:
- target_grad: float32 [512, 2048], P(('sp', 'tp'))
- source_grad: float32 [2048, 2048], P(('sp', 'tp'))
- query_weight_grad: float32 [2048, 4096], P('sp', 'tp')
The draws below stay inside these ranges and needn't reach their ends.
All inputs are finite; a program needn't handle non-finite values.
Results may differ from the reference program's by a relative error of at most 0.033.
Values may be sent and summed in bfloat16 or wider, within the bound.
A program may use at most 64 MiB of HBM per device.

```python
import math
import jax
import jax.numpy as jnp
from jax import lax

D = 2048
HEADS = 16
HEAD_DIM = 256
TARGET = 512
SOURCE = 2048


def block_scale(rng, dims, pieces, low, top_value):
    def one(axis_at, shards_of):
        steps = jax.random.uniform(jax.random.fold_in(jax.random.fold_in(rng, 6), axis_at), (shards_of,), jnp.float32, low / len(pieces), top_value / len(pieces))
        return jnp.repeat(jnp.exp(steps), dims[axis_at] // shards_of).reshape((-1,) + (1,) * (len(dims) - axis_at - 1))

    factor_of = one(*pieces[0])
    for cut in pieces[1:]:
        factor_of = factor_of * one(*cut)
    return factor_of


def bell_draw(key, extent, scale, bound, cuts=(), kind=jnp.bfloat16):
    values = jax.random.normal(key, extent, jnp.float32) * scale
    if len(cuts) > 0:
        values = block_scale(key, extent, cuts, -0.22, 0.18) * values
    return jnp.clip(values, min=-bound, max=bound).astype(kind)


def setup_inputs(seed: int = 0) -> dict:
    streams_of = jax.random.split(jax.random.key(seed), 11)
    target_rows = bell_draw(streams_of[0], (TARGET, D), 1.0, 6.0, ((0, 32),))
    source_rows = bell_draw(streams_of[1], (SOURCE, D), 1.0, 6.0, ((0, 32),))
    norm_gain = jnp.clip(1.0 + 0.18 * jax.random.normal(streams_of[2], (D,), jnp.float32), 0.099609375, 1.8984375).astype(jnp.bfloat16)
    query_weight = bell_draw(streams_of[3], (D, HEADS * HEAD_DIM), D ** -0.5, 0.125, ((1, 4),))
    key_weight = bell_draw(streams_of[4], (D, HEADS * HEAD_DIM), D ** -0.5, 0.125, ((1, 4),))
    value_weight = bell_draw(streams_of[5], (D, HEADS * HEAD_DIM), D ** -0.5, 0.125, ((1, 4),))
    output_weight = bell_draw(streams_of[6], (HEADS * HEAD_DIM, D), (HEADS * HEAD_DIM) ** -0.5, 0.09375, ((0, 4),))
    saved_output = bell_draw(streams_of[7], (TARGET, HEADS * HEAD_DIM), 0.5, 3.0, ((0, 8), (1, 4)))
    norm_offset = jnp.clip(0.25 + 1.0 * jax.random.uniform(streams_of[8], (TARGET, HEADS), jnp.float32) ** block_scale(streams_of[8], (TARGET, HEADS), ((0, 8), (1, 4)), -0.2, 0.2), 0.25, 1.25).astype(jnp.bfloat16)
    output_grad = bell_draw(streams_of[9], (TARGET, D), 32.0, 192.0, ((0, 32),))
    return {"target_rows": target_rows, "source_rows": source_rows, "norm_gain": norm_gain, "query_weight": query_weight, "key_weight": key_weight, "value_weight": value_weight, "output_weight": output_weight, "saved_output": saved_output, "norm_offset": norm_offset, "output_grad": output_grad}


EPSILON = 1e-06

def head_grads(operands):
    query_rows, head_gradient, shifts, deltas, key_row_block, value_row_block = operands
    score_scale = HEAD_DIM ** (-0.5)
    score_matrix = jnp.dot(query_rows, key_row_block.T, preferred_element_type=jnp.float32)
    prob_rows = jnp.exp(score_matrix * score_scale - shifts[:, None])
    prob_grad = jnp.dot(head_gradient, value_row_block.T, preferred_element_type=jnp.float32)
    score_grad = prob_rows * (prob_grad - deltas.astype(jnp.float32)[:, None]) * score_scale
    probability_rounded = prob_rows.astype(jnp.bfloat16)
    score_rounded = score_grad.astype(jnp.bfloat16)
    query_grad = jnp.dot(score_rounded, key_row_block, preferred_element_type=jnp.float32)
    key_grad = jnp.dot(score_rounded.T, query_rows, preferred_element_type=jnp.float32)
    value_grad = jnp.dot(probability_rounded.T, head_gradient, preferred_element_type=jnp.float32)
    return (query_grad, key_grad, value_grad)

def by_head(array, row_count):
    return array.reshape(row_count, HEADS, HEAD_DIM).transpose(1, 0, 2)

def from_head(array, row_count):
    return array.transpose(1, 0, 2).reshape(row_count, HEADS * HEAD_DIM)

def reference(target_rows, source_rows, norm_gain, query_weight, key_weight, value_weight, output_weight, saved_output, norm_offset, output_grad):
    target_float = target_rows.astype(jnp.float32)
    gain_float = norm_gain.astype(jnp.float32)
    inverse = lax.rsqrt(lax.optimization_barrier(jnp.mean(target_float * target_float, axis=1, keepdims=True)) + EPSILON)
    normed = (target_float * inverse * gain_float).astype(jnp.bfloat16)
    query_rows = jnp.dot(normed, query_weight, preferred_element_type=jnp.float32).astype(jnp.bfloat16)
    key_row_block = jnp.dot(source_rows, key_weight, preferred_element_type=jnp.float32).astype(jnp.bfloat16)
    value_row_block = jnp.dot(source_rows, value_weight, preferred_element_type=jnp.float32).astype(jnp.bfloat16)
    head_gradient = jnp.dot(output_grad, output_weight.T, preferred_element_type=jnp.float32).astype(jnp.bfloat16)
    products = head_gradient.astype(jnp.float32) * saved_output.astype(jnp.float32)
    deltas = lax.optimization_barrier(jnp.sum(products.reshape(TARGET, HEADS, HEAD_DIM), axis=2)).astype(jnp.bfloat16)
    shifts = (math.log(SOURCE) + norm_offset.astype(jnp.float32)).T
    outputs = lax.map(head_grads, (by_head(query_rows, TARGET), by_head(head_gradient, TARGET), shifts, deltas.T, by_head(key_row_block, SOURCE), by_head(value_row_block, SOURCE)))
    query_flat = from_head(outputs[0].astype(jnp.bfloat16), TARGET)
    key_flat = from_head(outputs[1].astype(jnp.bfloat16), SOURCE)
    value_flat = from_head(outputs[2].astype(jnp.bfloat16), SOURCE)
    normed_grad = jnp.dot(query_flat, query_weight.T, preferred_element_type=jnp.float32)
    scaled = normed_grad * gain_float
    target_grad = inverse * scaled - target_float * inverse ** 3 * lax.optimization_barrier(jnp.mean(scaled * target_float, axis=1, keepdims=True))
    source_grad = jnp.dot(key_flat, key_weight.T, preferred_element_type=jnp.float32) + jnp.dot(value_flat, value_weight.T, preferred_element_type=jnp.float32)
    weight_grad = jnp.dot(normed.T, query_flat, preferred_element_type=jnp.float32)
    return (target_grad, source_grad, weight_grad)
```

```python
import functools
import math

import jax
import jax.numpy as jnp
from jax import lax
from jax.experimental import pallas as pl
from jax.experimental.pallas import tpu as pltpu
from jax.sharding import PartitionSpec as P

HEAD_DIM = 256
EPSILON = 1e-06
MESH = pl.DeviceIdType.MESH
BF = jnp.bfloat16
F32 = jnp.float32
VMEM = pl.BlockSpec(memory_space=pltpu.VMEM)


def contract_last(left, right):
    return lax.dot_general(left, right, (((1,), (1,)), ((), ())), preferred_element_type=F32)


def push(src, dst, send, recv, device):
    return pltpu.make_async_remote_copy(
        src_ref=src, dst_ref=dst, send_sem=send, recv_sem=recv, device_id=device, device_id_type=MESH
    )


def greet(devices):
    barrier = pltpu.get_barrier_semaphore()
    for device in devices:
        pl.semaphore_signal(barrier, inc=1, device_id=device, device_id_type=MESH)
    pl.semaphore_wait(barrier, len(devices))


class Place:
    def __init__(self, sp, tp):
        self.sp, self.tp, self.Z, self.Y = sp, tp, sp // 2, tp // 2
        self.s, self.t = lax.axis_index("sp"), lax.axis_index("tp")
        self.z, self.x = self.s // 2, self.s % 2
        self.y, self.c = self.t // 2, self.t % 2
        self.partner = (self.s, self.y * 2 + 1 - self.c)
        self.across = (self.z * 2 + 1 - self.x, self.t)

    def chip_y(self, d):
        return (self.s, lax.rem(self.y + d + self.Y, self.Y) * 2 + self.c)

    def chip_z(self, d):
        return (lax.rem(self.z + d + self.Z, self.Z) * 2 + self.x, self.t)


class LineGather:
    def __init__(self, place, pairs, up_s, up_r, dn_s, dn_r, x_s, x_r):
        self.p, self.pairs = place, pairs
        self.sems = (up_s, up_r, dn_s, dn_r, x_s, x_r)

    def up(self, n, d, own=False):
        p, (own_ref, all_ref) = self.p, self.pairs[n]
        block = p.s - 2 * (d - 1)
        src = own_ref if own else all_ref.at[block]
        return push(src, all_ref.at[block], self.sems[0].at[n, d], self.sems[1].at[n, d], (p.s + 2, p.t))

    def up_wait(self, n, d):
        p, (_, all_ref) = self.p, self.pairs[n]
        ref = all_ref.at[p.s - 2 * d]
        return push(ref, ref, self.sems[0].at[n, d], self.sems[1].at[n, d], (p.s - 2, p.t))

    def dn(self, n, d, own=False):
        p, (own_ref, all_ref) = self.p, self.pairs[n]
        block = p.s + 2 * (d - 1)
        src = own_ref if own else all_ref.at[block]
        return push(src, all_ref.at[block], self.sems[2].at[n, d], self.sems[3].at[n, d], (p.s - 2, p.t))

    def dn_wait(self, n, d):
        p, (_, all_ref) = self.p, self.pairs[n]
        ref = all_ref.at[p.s + 2 * d]
        return push(ref, ref, self.sems[2].at[n, d], self.sems[3].at[n, d], (p.s + 2, p.t))

    def over(self, n, d):
        p, (own_ref, all_ref) = self.p, self.pairs[n]
        block = p.s - 2 * d
        k = d + p.Z - 1
        src = own_ref if d == 0 else all_ref.at[block]
        return push(src, all_ref.at[block], self.sems[4].at[n, k], self.sems[5].at[n, k], p.across)

    def over_wait(self, n, d):
        p, (_, all_ref) = self.p, self.pairs[n]
        ref = all_ref.at[p.z * 2 + 1 - p.x - 2 * d]
        k = d + p.Z - 1
        return push(ref, ref, self.sems[4].at[n, k], self.sems[5].at[n, k], p.across)

    def start(self, count):
        p = self.p

        @pl.when(p.z + 1 < p.Z)
        def _():
            for n in count:
                self.up(n, 1, True).start()

        @pl.when(p.z >= 1)
        def _():
            for n in count:
                self.dn(n, 1, True).start()

        for n in count:
            self.over(n, 0).start()

    def step(self, d):
        p = self.p
        for n in range(len(self.pairs)):

            @pl.when(p.z - d >= 0)
            def _():
                self.up_wait(n, d).wait_recv()

                @pl.when(p.z + 1 < p.Z)
                def _():
                    self.up(n, d + 1).start()

                self.over(n, d).start()

            @pl.when(p.z + d < p.Z)
            def _():
                self.dn_wait(n, d).wait_recv()

                @pl.when(p.z >= 1)
                def _():
                    self.dn(n, d + 1).start()

                self.over(n, -d).start()

    def arrive(self, sign, d):
        for n in range(len(self.pairs)):
            self.over_wait(n, sign * d).wait_recv()

    def side(self, sign, d):
        return self.p.z - d >= 0 if sign > 0 else self.p.z + d < self.p.Z

    def finish(self):
        p = self.p
        for n in range(len(self.pairs)):
            for d in range(p.Z):
                for sign in (1, -1) if d else (1,):

                    @pl.when(self.side(sign, d))
                    def _():
                        self.over(n, sign * d).wait_send()

            for d in range(1, p.Z):

                @pl.when(jnp.logical_and(p.z - d + 1 >= 0, p.z + 1 < p.Z))
                def _():
                    self.up(n, d).wait_send()

                @pl.when(jnp.logical_and(p.z + d - 1 < p.Z, p.z >= 1))
                def _():
                    self.dn(n, d).wait_send()


def line_sems(p_z, n):
    return [pltpu.SemaphoreType.DMA((n, p_z + 1))] * 4 + [pltpu.SemaphoreType.DMA((n, 2 * p_z))] * 2


class PairScatter:
    def __init__(self, p, part, first, summed, second, fs, fr, ss, sr):
        self.p, self.part, self.first, self.summed, self.second = p, part, first, summed, second
        self.sems = (fs, fr, ss, sr)
        self.started = []

    def start(self):
        p = self.p
        for d in range(p.Y):
            y = lax.rem(p.y + d, p.Y)
            copy = push(
                self.part(y * 2 + 1 - p.c), self.first.at[d], self.sems[0].at[d], self.sems[1].at[d], p.partner
            )
            copy.start()
            self.started.append(copy)

    def middle(self):
        p = self.p
        for d in list(range(1, p.Y)) + [0]:
            y = lax.rem(p.y + d, p.Y)
            self.started[d].wait_recv()
            total = self.part(y * 2 + p.c)[...].astype(F32) + self.first[d].astype(F32)
            self.summed[d] = total.astype(BF)
            if d:
                copy = push(
                    self.summed.at[d], self.second.at[d], self.sems[2].at[d], self.sems[3].at[d], p.chip_y(d)
                )
                copy.start()
                self.started.append(copy)

    def finish(self):
        p = self.p
        total = self.part(p.t)[...].astype(F32) + self.first[0].astype(F32)
        for d in range(1, p.Y):
            self.started[p.Y + d - 1].wait_recv()
            total = total + self.second[d].astype(F32)
        for copy in self.started:
            copy.wait_send()
        return total


class PairGather:
    def __init__(self, p, own, spot, ys, yr, ps, pr):
        self.p, self.own, self.spot, self.sems = p, own, spot, (ys, yr, ps, pr)
        self.started = []

    def start(self):
        p = self.p
        for d in range(1, p.Y):
            copy = push(self.own, self.spot(p.t), self.sems[0].at[d], self.sems[1].at[d], p.chip_y(d))
            copy.start()
            self.started.append(copy)
        copy = push(self.own, self.spot(p.t), self.sems[2].at[0], self.sems[3].at[0], p.partner)
        copy.start()
        self.started.append(copy)

    def forward(self):
        p = self.p
        for d in range(1, p.Y):
            ref = self.spot(lax.rem(p.y - d + p.Y, p.Y) * 2 + p.c)
            push(ref, ref, self.sems[0].at[d], self.sems[1].at[d], p.chip_y(-d)).wait_recv()
            copy = push(ref, ref, self.sems[2].at[d], self.sems[3].at[d], p.partner)
            copy.start()
            self.started.append(copy)

    def arrive(self):
        p = self.p
        for d in range(p.Y):
            ref = self.spot(lax.rem(p.y - d + p.Y, p.Y) * 2 + 1 - p.c)
            push(ref, ref, self.sems[2].at[d], self.sems[3].at[d], p.partner).wait_recv()

    def finish(self):
        for copy in self.started:
            copy.wait_send()


def layer_kernel(
    sp, tp, shift_base,
    raw, to, src, gain, saved, offs, wq_h, wk_h, wv_h, wo_h,
    flat_all, src_out, tgt_out, cols_all,
    tn, pieces, wq, wk, wv, wo, tn_all, to_all, src_all, cols, tn_b, to_b,
    q_all, hg_all, small_all, k_s, v_s, p_s, d_s, part, kf, vf, sg,
    xr, xz, zr, sg1, sg2, sg3, ng, ng1, ng2, ng3,
    wsem, loc, es, er, *sems
):
    p = Place(sp, tp)
    pair_sems = [sems[4 * i : 4 * i + 4] for i in range(6)]
    xs_s, xs_r, zs_s, zs_r = sems[24:28]
    line_a, line_b = sems[28:34], sems[34:40]
    rows, block = raw.shape[0], saved.shape[0]
    width, model = wq.shape[1], wq.shape[0]
    heads = width // HEAD_DIM
    scale = HEAD_DIM ** (-0.5)
    loads = [
        pltpu.make_async_copy(h, v, wsem.at[i])
        for i, (h, v) in enumerate(((wq_h, wq), (wo_h, wo), (wk_h, wk), (wv_h, wv)))
    ]
    for copy in loads:
        copy.start()
    raw_value, gain_value = raw[...].astype(F32), gain[...].astype(F32).reshape(1, model)
    inverse = lax.rsqrt(jnp.mean(raw_value * raw_value, axis=1, keepdims=True) + EPSILON)
    normed_value = (raw_value * inverse * gain_value).astype(BF)
    tn[...] = normed_value
    slice_width = model // sp
    for s in range(sp):
        pieces[s] = normed_value[:, s * slice_width : (s + 1) * slice_width]
    greet(
        [p.partner]
        + [p.chip_y(d) for d in range(1, p.Y)]
        + [(lax.rem(p.s + e, sp), p.t) for e in range(1, sp)]
    )
    g_tn = PairGather(p, tn, lambda t: tn_all.at[t], *pair_sems[0])
    g_to = PairGather(p, to, lambda t: to_all.at[t], *pair_sems[1])
    g_src = PairGather(p, src, lambda t: src_all.at[t], *pair_sems[2])
    g_cols = PairGather(p, cols, lambda t: cols_all.at[:, t], *pair_sems[3])
    for g in (g_tn, g_to, g_src):
        g.start()
    swaps = []
    for e in range(1, sp):
        s = lax.rem(p.s + e, sp)
        copy = push(pieces.at[s], cols.at[p.s], es.at[e], er.at[e], (s, p.t))
        copy.start()
        swaps.append(copy)
    mine = [
        pltpu.make_async_copy(tn, tn_all.at[p.t], loc.at[0]),
        pltpu.make_async_copy(to, to_all.at[p.t], loc.at[1]),
        pltpu.make_async_copy(src, src_all.at[p.t], loc.at[2]),
        pltpu.make_async_copy(pieces.at[p.s], cols.at[p.s], loc.at[3]),
    ]
    for copy in mine:
        copy.start()
    for copy in mine:
        copy.wait()
    tile = min(width, 256)
    gather = LineGather(
        p, ((q_all.at[p.s], q_all), (hg_all.at[p.s], hg_all), (small_all.at[p.s], small_all)), *line_a
    )

    g_tn.forward()
    g_to.forward()
    g_tn.arrive()
    for t in range(tp):
        tn_b[t * rows : (t + 1) * rows, :] = tn_all[t]
    loads[0].wait()
    for j in range(0, width, tile):
        q_all[p.s, :, j : j + tile] = jnp.dot(
            tn_b[...], wq[:, j : j + tile], preferred_element_type=F32
        ).astype(BF)
    gather.start((0,))
    g_to.arrive()
    for t in range(tp):
        to_b[t * rows : (t + 1) * rows, :] = to_all[t]
    loads[1].wait()
    lane = lax.broadcasted_iota(jnp.int32, (block, 128), 1)
    pick = lax.broadcasted_iota(jnp.int32, (heads, 128), 0) == lax.broadcasted_iota(jnp.int32, (heads, 128), 1)
    small = lax.dot_general(
        offs[...].astype(F32), pick.astype(F32), (((0,), (0,)), ((), ())), precision=lax.Precision.HIGHEST,
        preferred_element_type=F32,
    )
    for h in range(heads):
        cut = slice(h * HEAD_DIM, (h + 1) * HEAD_DIM)
        part_h = contract_last(to_b[...], wo[cut, :]).astype(BF)
        hg_all[p.s, :, cut] = part_h
        delta = jnp.sum(part_h.astype(F32) * saved[:, cut].astype(F32), axis=1, keepdims=True)
        small = jnp.where(lane == heads + h, delta, small)
    small_all[p.s] = small.astype(BF)
    gather.start((1, 2))

    g_src.forward()
    g_src.arrive()
    gather.step(1)
    source_count = k_s.shape[0]
    loads[2].wait()
    loads[3].wait()

    @pl.loop(0, width // tile)
    def _(j):
        cut = pl.ds(pl.multiple_of(j * tile, tile), tile)
        rows_value = src_all[...].reshape(source_count, model)
        k_s[:, cut] = jnp.dot(rows_value, wk[:, cut], preferred_element_type=F32).astype(BF)
        v_s[:, cut] = jnp.dot(rows_value, wv[:, cut], preferred_element_type=F32).astype(BF)

    for e in range(1, sp):
        s = lax.rem(p.s - e + sp, sp)
        push(cols.at[s], cols.at[s], es.at[e], er.at[e], (s, p.t)).wait_recv()
    g_cols.start()
    keep = pltpu.make_async_copy(cols, cols_all.at[:, p.t], loc.at[4])
    keep.start()

    def into(k):
        z = lax.rem(p.z + k, p.Z)
        return push(part.at[z * 2 + 1 - p.x], xr.at[k], xs_s.at[k], xs_r.at[k], p.across)

    def attend(z):
        pair = pl.ds(2 * z, 2)
        spot = pl.ds(pl.multiple_of(z * (2 * block), 2 * block), 2 * block)
        tiny = small_all[pair].reshape(2 * block, 128).astype(F32)
        for h in range(heads):
            cut = slice(h * HEAD_DIM, (h + 1) * HEAD_DIM)
            q_h = q_all[pair, :, cut].reshape(2 * block, HEAD_DIM)
            g_h = hg_all[pair, :, cut].reshape(2 * block, HEAD_DIM)
            prob = jnp.exp(contract_last(q_h, k_s[:, cut]) * scale - (shift_base + tiny[:, h : h + 1]))
            grad = contract_last(g_h, v_s[:, cut])
            score = (prob * (grad - tiny[:, heads + h : heads + h + 1]) * scale).astype(BF)
            p_s[h, spot, :] = prob.astype(BF)
            d_s[h, spot, :] = score
            term = jnp.dot(score, k_s[:, cut], preferred_element_type=F32).astype(BF)
            part[pair, :, cut] = term.reshape(2, block, HEAD_DIM)

    def reached(sign, d):
        gather.arrive(sign, d)
        attend(p.z - sign * d)
        into((-sign * d) % p.Z).start()

    for d in range(1, p.Z):
        if d > 1:
            gather.step(d)
        for sign in (1, -1) if d > 1 else (1,):

            @pl.when(gather.side(sign, d - 1))
            def _():
                reached(sign, d - 1)

        if d == 1:
            g_cols.forward()
    for sign in (1, -1):

        @pl.when(gather.side(sign, p.Z - 1))
        def _():
            reached(sign, p.Z - 1)

    order = sorted(range(1, p.Z), key=lambda k: min(k, p.Z - k))
    hops = {}

    def relay(k):
        into(k).wait_recv()
        z = lax.rem(p.z + k, p.Z)
        xz[k] = (part[z * 2 + p.x].astype(F32) + xr[k].astype(F32)).astype(BF)
        hops[k] = push(xz.at[k], zr.at[k], zs_s.at[k], zs_r.at[k], p.chip_z(k))
        hops[k].start()

    for k in order[:1]:
        relay(k)
    count = sp * block

    for h in range(heads):
        cut = slice(h * HEAD_DIM, (h + 1) * HEAD_DIM)
        dims = (((0,), (0,)), ((), ()))
        q_h = q_all[:, :, cut].reshape(count, HEAD_DIM)
        g_h = hg_all[:, :, cut].reshape(count, HEAD_DIM)
        kf[:, cut] = lax.dot_general(d_s[h], q_h, dims, preferred_element_type=F32).astype(BF)
        vf[:, cut] = lax.dot_general(p_s[h], g_h, dims, preferred_element_type=F32).astype(BF)
    for k in order[1:2]:
        relay(k)
    stile = min(model, 256)

    def source_term(j):
        cut = pl.ds(pl.multiple_of(j * stile, stile), stile)
        value = contract_last(kf[...], wk[cut, :]) + contract_last(vf[...], wv[cut, :])
        sg[:, :, cut] = value.astype(BF).reshape(tp, source_count // tp, stile)

    half = model // stile // 2
    pl.loop(0, half)(source_term)
    for k in order[2:]:
        relay(k)
    pl.loop(half, model // stile)(source_term)
    source = PairScatter(p, lambda t: sg.at[t], sg1, sg2, sg3, *pair_sems[4])
    source.start()
    source.middle()
    into(0).wait_recv()
    total = part[p.s].astype(F32) + xr[0].astype(F32)
    for k in order:
        hops[k].wait_recv()
        total = total + zr[k].astype(F32)
    flat = total.astype(BF)
    flat_all[p.s] = flat
    spread = LineGather(p, ((flat_all.at[p.s], flat_all),), *line_b)
    spread.start((0,))
    for j in range(0, model, stile):
        columns = contract_last(flat, wq[j : j + stile, :]).astype(BF)
        for t in range(tp):
            ng[t, :, j : j + stile] = columns[t * rows : (t + 1) * rows]
    normed = PairScatter(p, lambda t: ng.at[t], ng1, ng2, ng3, *pair_sems[5])
    normed.start()
    for d in range(1, p.Z):
        spread.step(d)
        if d == 1:
            normed.middle()
    src_out[...] = source.finish()
    raw_value, gain_value = raw[...].astype(F32), gain[...].astype(F32).reshape(1, model)
    inverse = lax.rsqrt(jnp.mean(raw_value * raw_value, axis=1, keepdims=True) + EPSILON)
    scaled = normed.finish() * gain_value
    tgt_out[...] = inverse * scaled - raw_value * (inverse * inverse * inverse) * jnp.mean(
        scaled * raw_value, axis=1, keepdims=True
    )
    g_cols.arrive()
    for d in range(p.Z):
        for sign in (1, -1) if d else (1,):

            @pl.when(spread.side(sign, d))
            def _():
                spread.arrive(sign, d)

    gather.finish()
    spread.finish()
    for g in (g_tn, g_to, g_src, g_cols):
        g.finish()
    for copy in swaps:
        copy.wait_send()
    keep.wait()
    for k in range(p.Z):
        into(k).wait_send()
    for k in order:
        hops[k].wait_send()


def body(
    target_rows,
    source_rows,
    norm_gain,
    query_weight,
    key_weight,
    value_weight,
    output_weight,
    saved_output,
    norm_offset,
    output_grad,
):
    tp, sp = lax.axis_size("tp"), lax.axis_size("sp")
    Z, Y = sp // 2, tp // 2
    model, width = query_weight.shape
    heads = width // HEAD_DIM
    rows, srows = target_rows.shape[0], source_rows.shape[0]
    block = rows * tp
    count = block * sp
    source_count = srows * tp
    shift_base = math.log(source_count * sp)
    slice_width = model // sp
    dma = pltpu.SemaphoreType.DMA

    vm = pltpu.VMEM
    whole = pl.BlockSpec(memory_space=pl.ANY)
    flat_all, source_grad, target_grad, cols_all = pl.pallas_call(
        functools.partial(layer_kernel, sp, tp, shift_base),
        out_shape=[
            jax.ShapeDtypeStruct((sp, block, width), BF),
            jax.ShapeDtypeStruct((srows, model), F32),
            jax.ShapeDtypeStruct((rows, model), F32),
            jax.ShapeDtypeStruct((sp, tp, rows, slice_width), BF),
        ],
        in_specs=[VMEM] * 6 + [whole] * 4,
        out_specs=[VMEM] * 4,
        scratch_shapes=[vm((rows, model), BF), vm((sp, rows, slice_width), BF)]
        + [vm((model, width), BF)] * 3
        + [vm((width, model), BF)]
        + [vm((tp, rows, model), BF)] * 2
        + [vm((tp, srows, model), BF), vm((sp, rows, slice_width), BF)]
        + [vm((block, model), BF)] * 2
        + [vm((sp, block, width), BF)] * 2
        + [vm((sp, block, 128), BF)]
        + [vm((source_count, width), BF)] * 2
        + [vm((heads, count, source_count), BF)] * 2
        + [vm((sp, block, width), BF)]
        + [vm((source_count, width), BF)] * 2
        + [vm((tp, srows, model), BF)]
        + [vm((Z, block, width), BF)] * 3
        + [vm((Y, srows, model), BF)] * 3
        + [vm((tp, rows, model), BF)]
        + [vm((Y, rows, model), BF)] * 3
        + [dma((4,)), dma((5,)), dma((sp,)), dma((sp,))]
        + [dma((Y,))] * 24
        + [dma((Z,))] * 4
        + line_sems(Z, 3)
        + line_sems(Z, 1),
        name="layer_kernel",
        compiler_params=pltpu.CompilerParams(
            collective_id=1, has_side_effects=True, vmem_limit_bytes=58 * 2**20
        ),
    )(
        target_rows,
        output_grad,
        source_rows,
        norm_gain,
        saved_output,
        norm_offset.T,
        query_weight,
        key_weight,
        value_weight,
        output_weight,
    )
    weight_grad = lax.dot_general(
        cols_all.reshape(count, slice_width),
        flat_all.reshape(count, width),
        (((0,), (0,)), ((), ())),
        preferred_element_type=F32,
    )
    return (target_grad, source_grad, weight_grad)


class Net:
    def __init__(self, send, recv):
        self.sems, self.ids, self.started = (send, recv), {}, []

    def _copy(self, name, src, dst, device):
        n = self.ids.setdefault(name, len(self.ids))
        return push(src, dst, self.sems[0].at[n], self.sems[1].at[n], device)

    def go(self, name, src, dst, device):
        copy = self._copy(name, src, dst, device)
        copy.start()
        self.started.append(copy)

    def wait(self, name, landed, device):
        self._copy(name, landed, landed, device).wait_recv()

    def close(self):
        for copy in self.started:
            copy.wait_send()


TRANSFERS = 160


def grid_kernel(
    sp, tp, shift_base,
    raw, to, src, gain, saved, offs, wq_h, wk_h, wv_h, wo_h,
    ws, src_out, tgt_out,
    tn_all, to_all, src_all, pieces, cols, q_st, g_st, sm_st, q_all, g_all, sm_all,
    wq, wk, wv, wo, k_s, v_s, p_s, d_s, part, xr, xz, zr, flat_all, fl, kf, vf,
    sg, sd, ss, es, fs, fr, ng, ng1, ng2, ng3, wt,
    wsem, send, recv, *sems
):
    p = Place(sp, tp)
    s, t, y, c, x = p.s, p.t, p.y, p.c, p.x
    u, v = p.z // 2, p.z % 2
    net = Net(send, recv)

    def at(u, v, x):
        return ((u * 2 + v) * 2 + x, t)

    C, Y, V, X, U = p.partner, p.chip_y(1), at(u, 1 - v, x), at(u, v, 1 - x), at(1 - u, v, x)
    ty, tc, tyc = (1 - y) * 2 + c, y * 2 + 1 - c, (1 - y) * 2 + 1 - c
    rows, block, srows = raw.shape[0], saved.shape[0], src.shape[0]
    model, width = wq.shape
    heads = width // HEAD_DIM
    hh, half = heads // 2, width // 2
    sblock = srows * tp
    sw = model // sp
    scale = HEAD_DIM ** (-0.5)
    mine = pl.ds(pl.multiple_of(v * half, half), half)
    loads = [
        pltpu.make_async_copy(h, w, wsem.at[i])
        for i, (h, w) in enumerate(((wq_h, wq), (wo_h, wo), (wk_h.at[:, mine], wk), (wv_h.at[:, mine], wv)))
    ]
    for copy in loads:
        copy.start()
    raw_value, gain_value = raw[...].astype(F32), gain[...].astype(F32).reshape(1, model)
    inverse = lax.rsqrt(jnp.mean(raw_value * raw_value, axis=1, keepdims=True) + EPSILON)
    normed_value = (raw_value * inverse * gain_value).astype(BF)
    tn_all[t] = normed_value
    to_all[t] = to[...]
    src_all[v, t] = src[...]
    for a in range(2):
        for b in range(2):
            for k in range(2):
                n = (2 * a + k) * 2 + b
                pieces[a, b, :, k * sw : (k + 1) * sw] = normed_value[:, n * sw : (n + 1) * sw]
    others = [
        (a, b, d, u + a - 2 * u * a, v + b - 2 * v * b, x + d - 2 * x * d)
        for a in range(2) for b in range(2) for d in range(2) if a + b + d
    ]
    greet([C, Y] + [at(*o[3:]) for o in others])
    A, B = pl.ds(0, srows // 2), pl.ds(srows // 2, srows // 2)

    def same(name, ref, device):
        net.go(name, ref, ref, device)

    same("tnY", tn_all.at[t], Y)
    same("sVB", src_all.at[v, t, B], V)
    same("tnC", tn_all.at[t], C)
    same("toY", to_all.at[t], Y)
    same("toC", to_all.at[t], C)
    same("sYA", src_all.at[v, t, A], Y)
    same("sVA", src_all.at[v, t, A], V)
    same("sYB", src_all.at[v, t, B], Y)
    same("sC", src_all.at[v, t], C)
    spot = (u * 2 + x) * 2 + v
    for a, b, d, u2, v2, x2 in others:
        net.go(f"p{a}{b}{d}", pieces.at[u2, x2], cols.at[spot, t], at(u2, v2, x2))
    cols[spot, t] = pieces[u, x]

    net.wait("tnY", tn_all.at[ty], Y)
    same("tnF", tn_all.at[ty], C)
    net.wait("toY", to_all.at[ty], Y)
    same("toF", to_all.at[ty], C)
    net.wait("tnC", tn_all.at[tc], C)
    net.wait("tnF", tn_all.at[tyc], C)
    loads[0].wait()
    tn_b = tn_all[...].reshape(block, model)
    for k in range(2):
        for j in range(0, half, HEAD_DIM):
            q_st[k, :, j : j + HEAD_DIM] = jnp.dot(
                tn_b, wq[:, k * half + j : k * half + j + HEAD_DIM], preferred_element_type=F32
            ).astype(BF)
    net.go("qV", q_st.at[1 - v], q_all.at[u, x, v], V)
    q_all[u, x, v] = q_st[v]
    same("q0U", q_all.at[u, x, v], U)
    same("q0X", q_all.at[u, x, v], X)
    net.wait("toC", to_all.at[tc], C)
    net.wait("toF", to_all.at[tyc], C)
    loads[1].wait()
    to_b = to_all[...].reshape(block, model)
    lines, lanes = sm_st.shape[1], 2 * block
    line = lax.broadcasted_iota(jnp.int32, (lines, lanes), 0)
    place = (
        lax.broadcasted_iota(jnp.int32, (block, lanes), 1)
        == lax.broadcasted_iota(jnp.int32, (block, lanes), 0) + v * block
    ).astype(F32)
    spread = jnp.dot(offs[...].astype(F32), place, precision=lax.Precision.HIGHEST, preferred_element_type=F32)
    ones = jnp.ones((lines, HEAD_DIM), F32)
    for k in range(2):
        small = jnp.zeros((lines, lanes), F32)
        for h in range(hh):
            n = k * hh + h
            cut = slice(n * HEAD_DIM, (n + 1) * HEAD_DIM)
            part_h = contract_last(to_b, wo[cut, :]).astype(BF)
            g_st[k, :, h * HEAD_DIM : (h + 1) * HEAD_DIM] = part_h
            product = part_h.astype(F32) * saved[:, cut].astype(F32)
            padded = jnp.concatenate(
                [jnp.where(v == 0, product, 0.0), jnp.where(v == 1, product, 0.0)], axis=0
            )
            delta = lax.dot_general(
                ones, padded, (((1,), (1,)), ((), ())), precision=lax.Precision.HIGHEST, preferred_element_type=F32
            )
            small = jnp.where(line == h, jnp.broadcast_to(spread[n : n + 1], small.shape), small)
            small = jnp.where(line == hh + h, delta, small)
        sm_st[k] = small.astype(BF)
    net.go("mV", sm_st.at[1 - v], sm_all.at[u, x, v], V)
    net.go("gV", g_st.at[1 - v], g_all.at[u, x, v], V)
    g_all[u, x, v] = g_st[v]
    sm_all[u, x, v] = sm_st[v]
    same("m0U", sm_all.at[u, x, v], U)
    same("g0U", g_all.at[u, x, v], U)
    same("m0X", sm_all.at[u, x, v], X)
    same("g0X", g_all.at[u, x, v], X)

    net.wait("sVB", src_all.at[1 - v, t, B], V)
    same("fVB", src_all.at[1 - v, t, B], Y)
    same("cVB", src_all.at[1 - v, t, B], C)
    net.wait("sYA", src_all.at[v, ty, A], Y)
    same("fYA", src_all.at[v, ty, A], V)
    same("cYA", src_all.at[v, ty, A], C)
    net.wait("qV", q_all.at[u, x, 1 - v], V)
    same("q1U", q_all.at[u, x, 1 - v], U)
    same("q1X", q_all.at[u, x, 1 - v], X)
    net.wait("sVA", src_all.at[1 - v, t, A], V)
    same("cVA", src_all.at[1 - v, t, A], C)
    net.wait("sYB", src_all.at[v, ty, B], Y)
    same("cYB", src_all.at[v, ty, B], C)
    net.wait("mV", sm_all.at[u, x, 1 - v], V)
    net.wait("gV", g_all.at[u, x, 1 - v], V)
    same("m1U", sm_all.at[u, x, 1 - v], U)
    same("g1U", g_all.at[u, x, 1 - v], U)
    same("m1X", sm_all.at[u, x, 1 - v], X)
    same("g1X", g_all.at[u, x, 1 - v], X)
    for a, b, d, u2, v2, x2 in others:
        net.wait(f"p{a}{b}{d}", cols.at[(u2 * 2 + x2) * 2 + v2, t], at(u2, v2, x2))
    same("kY", cols.at[:, t], Y)
    same("kC", cols.at[:, t], C)
    net.wait("q0U", q_all.at[1 - u, x, v], U)
    same("q2X", q_all.at[1 - u, x, v], X)
    net.wait("fVB", src_all.at[1 - v, ty, B], Y)
    same("dVB", src_all.at[1 - v, ty, B], C)
    net.wait("fYA", src_all.at[1 - v, ty, A], V)
    same("dYA", src_all.at[1 - v, ty, A], C)

    def project(k):
        spot = pl.ds(pl.multiple_of(k * sblock, sblock), sblock)

        @pl.loop(0, half // HEAD_DIM)
        def _(j):
            cut = pl.ds(pl.multiple_of(j * HEAD_DIM, HEAD_DIM), HEAD_DIM)
            value = src_all[k].reshape(sblock, model)
            k_s[spot, cut] = jnp.dot(value, wk[:, cut], preferred_element_type=F32).astype(BF)
            v_s[spot, cut] = jnp.dot(value, wv[:, cut], preferred_element_type=F32).astype(BF)

    net.wait("sC", src_all.at[v, tc], C)
    net.wait("cYA", src_all.at[v, tyc, A], C)
    net.wait("cYB", src_all.at[v, tyc, B], C)
    loads[2].wait()
    loads[3].wait()
    project(v)
    net.wait("q1U", q_all.at[1 - u, x, 1 - v], U)
    same("q3X", q_all.at[1 - u, x, 1 - v], X)
    net.wait("cVB", src_all.at[1 - v, tc, B], C)
    net.wait("cVA", src_all.at[1 - v, tc, A], C)
    net.wait("dVB", src_all.at[1 - v, tyc, B], C)
    net.wait("dYA", src_all.at[1 - v, tyc, A], C)
    project(1 - v)
    net.wait("m0U", sm_all.at[1 - u, x, v], U)
    same("m2X", sm_all.at[1 - u, x, v], X)
    net.wait("g0U", g_all.at[1 - u, x, v], U)
    same("g2X", g_all.at[1 - u, x, v], X)

    def attend(w, after=None):
        little = sm_all[w].astype(F32)
        little = jnp.concatenate([little[0, 0] + little[0, 1], little[1, 0] + little[1, 1]], axis=1)
        for h in range(hh):
            cut = slice(h * HEAD_DIM, (h + 1) * HEAD_DIM)
            q_h = q_all[w, :, :, :, cut].reshape(4 * block, HEAD_DIM)
            g_h = g_all[w, :, :, :, cut].reshape(4 * block, HEAD_DIM)
            prob = jnp.exp(contract_last(k_s[:, cut], q_h) * scale - (shift_base + little[h : h + 1]))
            grad = contract_last(v_s[:, cut], g_h)
            score = (prob * (grad - little[hh + h : hh + h + 1]) * scale).astype(BF)
            p_s[w, h] = prob.astype(BF)
            d_s[w, h] = score
            term = lax.dot_general(score, k_s[:, cut], (((0,), (0,)), ((), ())), preferred_element_type=F32)
            part[w, :, h] = term.astype(BF).reshape(2, 2, block, HEAD_DIM)
            if after is not None:
                after(h)

    for n, k in ((0, v), (1, 1 - v)):
        net.wait(f"q{n}X", q_all.at[u, 1 - x, k], X)
        net.wait(f"m{n}X", sm_all.at[u, 1 - x, k], X)
        net.wait(f"g{n}X", g_all.at[u, 1 - x, k], X)
    attend(u)
    net.go("aX", part.at[u, 1 - x], xr.at[0], X)
    net.wait("m1U", sm_all.at[1 - u, x, 1 - v], U)
    same("m3X", sm_all.at[1 - u, x, 1 - v], X)
    net.wait("g1U", g_all.at[1 - u, x, 1 - v], U)
    same("g3X", g_all.at[1 - u, x, 1 - v], X)
    net.wait("kY", cols.at[:, ty], Y)
    same("kF", cols.at[:, ty], C)
    for n, k in ((2, v), (3, 1 - v)):
        net.wait(f"q{n}X", q_all.at[1 - u, 1 - x, k], X)
        net.wait(f"m{n}X", sm_all.at[1 - u, 1 - x, k], X)
        net.wait(f"g{n}X", g_all.at[1 - u, 1 - x, k], X)
    attend(1 - u, lambda h: net.go(f"b{h}X", part.at[1 - u, 1 - x, h], xr.at[1, h], X))
    for h in range(hh):
        cut = slice(h * HEAD_DIM, (h + 1) * HEAD_DIM)
        k_h, v_h = 0.0, 0.0
        for w in range(2):
            q_h = q_all[w, :, :, :, cut].reshape(4 * block, HEAD_DIM)
            g_h = g_all[w, :, :, :, cut].reshape(4 * block, HEAD_DIM)
            k_h = k_h + jnp.dot(d_s[w, h], q_h, preferred_element_type=F32)
            v_h = v_h + jnp.dot(p_s[w, h], g_h, preferred_element_type=F32)
        kf[:, cut] = k_h.astype(BF)
        vf[:, cut] = v_h.astype(BF)
    stile = min(model // 2, 256)

    def source_half(n):
        @pl.loop(0, model // 2 // stile)
        def _(j):
            here = pl.ds(pl.multiple_of(n * (model // 2) + j * stile, stile), stile)
            cut = pl.ds(pl.multiple_of(j * stile, stile), stile)
            value = contract_last(kf[...], wk[here, :]) + contract_last(vf[...], wv[here, :])
            sg[n, :, :, :, cut] = value.astype(BF).reshape(2, tp, srows, stile)

        for a in range(2):
            for b in range(2):
                net.go(f"d{n}{a}{b}", sg.at[n, a, b * 2 + 1 - c], sd.at[n, a, b], C)

    source_half(0)
    source_half(1)
    for h in range(hh):
        net.wait(f"b{h}X", xr.at[1, h], X)
        xz[h] = (part[1 - u, x, h].astype(F32) + xr[1, h].astype(F32)).astype(BF)
        net.go(f"z{h}U", xz.at[h], zr.at[h], U)

    def source_sum(n):
        for a in range(2):
            for b in range(2):
                net.wait(f"d{n}{a}{b}", sd.at[n, a, b], C)
                ss[n, a, b] = (sg[n, a, b * 2 + c].astype(F32) + sd[n, a, b].astype(F32)).astype(BF)

    source_sum(0)
    net.go("e01", ss.at[0, 1 - v, 1 - y], es.at[0, 1], Y)
    net.go("e00", ss.at[0, v, 1 - y], es.at[0, 0], Y)
    source_sum(1)
    net.go("e11", ss.at[1, 1 - v, 1 - y], es.at[1, 1], V)
    net.go("e10", ss.at[1, 1 - v, y], es.at[1, 0], V)
    net.wait("aX", xr.at[0], X)
    for h in range(hh):
        net.wait(f"z{h}U", zr.at[h], U)
        total = part[u, x, h].astype(F32) + xr[0, h].astype(F32) + zr[h].astype(F32)
        flat_all[u, x, h] = total.astype(BF)
        same(f"r{h}U", flat_all.at[u, x, h], U)
        same(f"r{h}X", flat_all.at[u, x, h], X)
        net.go(f"n{h}V", flat_all.at[u, x, h, 1 - v], fl.at[v, h], V)
        fl[v, h] = flat_all[u, x, h, v]
    net.wait("kC", cols.at[:, tc], C)
    net.wait("kF", cols.at[:, tyc], C)
    net.wait("e01", es.at[0, 1], Y)
    fs[0] = (ss[0, 1 - v, y].astype(F32) + es[0, 1].astype(F32)).astype(BF)
    net.go("f0", fs.at[0], fr.at[0], V)
    net.wait("e11", es.at[1, 1], V)
    fs[1] = (ss[1, v, 1 - y].astype(F32) + es[1, 1].astype(F32)).astype(BF)
    net.go("f1", fs.at[1], fr.at[1], Y)
    for h in range(hh):
        net.wait(f"n{h}V", fl.at[1 - v, h], V)
    ntile = min(model, 256)
    for j in range(0, model, ntile):
        columns = 0.0
        for k in range(2):
            for h in range(hh):
                n = (k * hh + h) * HEAD_DIM
                columns = columns + contract_last(fl[k, h], wq[j : j + ntile, n : n + HEAD_DIM])
        ng[:, :, j : j + ntile] = columns.astype(BF).reshape(tp, rows, ntile)
    normed = PairScatter(p, lambda n: ng.at[n], ng1, ng2, ng3, *sems)
    normed.start()
    net.wait("r0U", flat_all.at[1 - u, x, 0], U)
    same("w0X", flat_all.at[1 - u, x, 0], X)
    normed.middle()
    for h in range(1, hh):
        net.wait(f"r{h}U", flat_all.at[1 - u, x, h], U)
        same(f"w{h}X", flat_all.at[1 - u, x, h], X)
    cols_value = cols[...].reshape(sp * block, 2 * sw)
    for h in range(hh):
        net.wait(f"r{h}X", flat_all.at[u, 1 - x, h], X)
        net.wait(f"w{h}X", flat_all.at[1 - u, 1 - x, h], X)
        flat_h = flat_all[:, :, h].reshape(sp * block, HEAD_DIM)
        for k in range(2):
            wt[h, k] = lax.dot_general(
                cols_value[:, k * sw : (k + 1) * sw], flat_h, (((0,), (0,)), ((), ())), preferred_element_type=F32
            ).astype(BF)
        net.go(f"W{h}", wt.at[h, 1 - v], ws.at[v, h], V)
        ws[v, h] = wt[h, v]
    for n, (key, last) in enumerate((("e00", Y), ("e10", V))):
        net.wait(key, es.at[n, 0], last)
        net.wait(f"f{n}", fr.at[n], (V, Y)[n])
        src_out[:, n * (model // 2) : (n + 1) * (model // 2)] = (
            ss[n, v, y].astype(F32) + es[n, 0].astype(F32) + fr[n].astype(F32)
        )
    raw_value, gain_value = raw[...].astype(F32), gain[...].astype(F32).reshape(1, model)
    inverse = lax.rsqrt(jnp.mean(raw_value * raw_value, axis=1, keepdims=True) + EPSILON)
    scaled = normed.finish() * gain_value
    tgt_out[...] = inverse * scaled - raw_value * (inverse * inverse * inverse) * jnp.mean(
        scaled * raw_value, axis=1, keepdims=True
    )
    for h in range(hh):
        net.wait(f"W{h}", ws.at[1 - v, h], V)
    net.close()


def finish_kernel(ws, src_in, tgt_in, weight_out, src_out, tgt_out):
    parts, hh = ws.shape[0], ws.shape[1]
    for k in range(parts):
        for h in range(hh):
            n = (k * hh + h) * HEAD_DIM
            weight_out[:, n : n + HEAD_DIM] = ws[k, h].astype(F32)
    src_out[...] = src_in[...]
    tgt_out[...] = tgt_in[...]


def grid_body(
    target_rows, source_rows, norm_gain, query_weight, key_weight, value_weight, output_weight,
    saved_output, norm_offset, output_grad
):
    tp, sp = lax.axis_size("tp"), lax.axis_size("sp")
    model, width = query_weight.shape
    heads = width // HEAD_DIM
    hh, half = heads // 2, width // 2
    rows, srows = target_rows.shape[0], source_rows.shape[0]
    block, sblock, sw = rows * tp, srows * tp, model // sp
    Y = tp // 2
    dma, vm = pltpu.SemaphoreType.DMA, pltpu.VMEM
    whole = pl.BlockSpec(memory_space=pl.ANY)
    pair = (2, 2, 2, block, half)
    ws, source_grad, target_grad = pl.pallas_call(
        functools.partial(grid_kernel, sp, tp, math.log(sblock * sp)),
        out_shape=[
            jax.ShapeDtypeStruct((2, hh, sw, HEAD_DIM), BF),
            jax.ShapeDtypeStruct((srows, model), F32),
            jax.ShapeDtypeStruct((rows, model), F32),
        ],
        in_specs=[VMEM] * 6 + [whole] * 4,
        out_specs=[VMEM] * 3,
        scratch_shapes=[vm((tp, rows, model), BF)] * 2
        + [vm((2, tp, srows, model), BF)]
        + [vm((2, 2, rows, 2 * sw), BF), vm((sp, tp, rows, 2 * sw), BF)]
        + [vm((2, block, half), BF)] * 2
        + [vm((2, 16, 2 * block), BF)]
        + [vm(pair, BF)] * 2
        + [vm((2, 2, 2, 16, 2 * block), BF)]
        + [vm((model, width), BF)]
        + [vm((model, half), BF)] * 2
        + [vm((width, model), BF)]
        + [vm((2 * sblock, half), BF)] * 2
        + [vm((2, hh, 2 * sblock, 4 * block), BF)] * 2
        + [vm((2, 2, hh, 2, block, HEAD_DIM), BF)]
        + [vm((2, hh, 2, block, HEAD_DIM), BF)]
        + [vm((hh, 2, block, HEAD_DIM), BF)] * 2
        + [vm((2, 2, hh, 2, block, HEAD_DIM), BF)]
        + [vm((2, hh, block, HEAD_DIM), BF)]
        + [vm((2 * sblock, half), BF)] * 2
        + [vm((2, 2, tp, srows, model // 2), BF)]
        + [vm((2, 2, Y, srows, model // 2), BF)] * 2
        + [vm((2, 2, srows, model // 2), BF)]
        + [vm((2, srows, model // 2), BF)] * 2
        + [vm((tp, rows, model), BF)]
        + [vm((Y, rows, model), BF)] * 3
        + [vm((hh, 2, sw, HEAD_DIM), BF)]
        + [dma((4,)), dma((TRANSFERS,)), dma((TRANSFERS,))]
        + [dma((Y,))] * 4,
        name="grid_kernel",
        compiler_params=pltpu.CompilerParams(
            collective_id=1, has_side_effects=True, vmem_limit_bytes=58 * 2**20
        ),
    )(
        target_rows, output_grad, source_rows, norm_gain, saved_output, norm_offset.T,
        query_weight, key_weight, value_weight, output_weight,
    )
    weight_grad, source_grad, target_grad = pl.pallas_call(
        finish_kernel,
        out_shape=[
            jax.ShapeDtypeStruct((sw, width), F32),
            jax.ShapeDtypeStruct((srows, model), F32),
            jax.ShapeDtypeStruct((rows, model), F32),
        ],
        in_specs=[VMEM] * 3,
        out_specs=[VMEM] * 3,
        name="finish_kernel",
    )(ws, source_grad, target_grad)
    return (target_grad, source_grad, weight_grad)


def on_grid(target_rows, query_weight):
    pairs = (lax.axis_size("sp"), lax.axis_size("tp")) == (2**3, 2**2)
    heads = query_weight.shape[1] // HEAD_DIM
    return pairs and heads % 2 == 0 and 2 * target_rows.shape[0] * lax.axis_size("tp") % 128 == 0


def layer(*args):
    return (grid_body if on_grid(args[0], args[3]) else body)(*args)


def solution(mesh):
    in_specs = (
        P(("sp", "tp"), None),
        P(("sp", "tp"), None),
        P(),
        P(None, "tp"),
        P(None, "tp"),
        P(None, "tp"),
        P("tp", None),
        P("sp", "tp"),
        P("sp", "tp"),
        P(("sp", "tp"), None),
    )
    out_specs = (P(("sp", "tp"), None), P(("sp", "tp"), None), P("sp", "tp"))
    return jax.shard_map(layer, mesh=mesh, in_specs=in_specs, out_specs=out_specs, check_vma=False)
```

```python
import functools
import math

import jax
import jax.numpy as jnp
from jax import lax
from jax.experimental import pallas as pl
from jax.experimental.pallas import tpu as pltpu
from jax.sharding import PartitionSpec as P

HEAD_DIM = 256
EPSILON = 1e-06
MESH = pl.DeviceIdType.MESH
BF = jnp.bfloat16
F32 = jnp.float32
VMEM = pl.BlockSpec(memory_space=pltpu.VMEM)


def contract_last(left, right):
    return lax.dot_general(left, right, (((1,), (1,)), ((), ())), preferred_element_type=F32)


def push(src, dst, send, recv, device):
    return pltpu.make_async_remote_copy(
        src_ref=src, dst_ref=dst, send_sem=send, recv_sem=recv, device_id=device, device_id_type=MESH
    )


def greet(devices):
    barrier = pltpu.get_barrier_semaphore()
    for device in devices:
        pl.semaphore_signal(barrier, inc=1, device_id=device, device_id_type=MESH)
    pl.semaphore_wait(barrier, len(devices))


class Place:
    def __init__(self, sp, tp):
        self.sp, self.tp, self.Z, self.Y = sp, tp, sp // 2, tp // 2
        self.s, self.t = lax.axis_index("sp"), lax.axis_index("tp")
        self.z, self.x = self.s // 2, self.s % 2
        self.y, self.c = self.t // 2, self.t % 2
        self.partner = (self.s, self.y * 2 + 1 - self.c)
        self.across = (self.z * 2 + 1 - self.x, self.t)

    def chip_y(self, d):
        return (self.s, lax.rem(self.y + d + self.Y, self.Y) * 2 + self.c)

    def chip_z(self, d):
        return (lax.rem(self.z + d + self.Z, self.Z) * 2 + self.x, self.t)


class LineGather:
    def __init__(self, place, pairs, up_s, up_r, dn_s, dn_r, x_s, x_r):
        self.p, self.pairs = place, pairs
        self.sems = (up_s, up_r, dn_s, dn_r, x_s, x_r)

    def up(self, n, d, own=False):
        p, (own_ref, all_ref) = self.p, self.pairs[n]
        block = p.s - 2 * (d - 1)
        src = own_ref if own else all_ref.at[block]
        return push(src, all_ref.at[block], self.sems[0].at[n, d], self.sems[1].at[n, d], (p.s + 2, p.t))

    def up_wait(self, n, d):
        p, (_, all_ref) = self.p, self.pairs[n]
        ref = all_ref.at[p.s - 2 * d]
        return push(ref, ref, self.sems[0].at[n, d], self.sems[1].at[n, d], (p.s - 2, p.t))

    def dn(self, n, d, own=False):
        p, (own_ref, all_ref) = self.p, self.pairs[n]
        block = p.s + 2 * (d - 1)
        src = own_ref if own else all_ref.at[block]
        return push(src, all_ref.at[block], self.sems[2].at[n, d], self.sems[3].at[n, d], (p.s - 2, p.t))

    def dn_wait(self, n, d):
        p, (_, all_ref) = self.p, self.pairs[n]
        ref = all_ref.at[p.s + 2 * d]
        return push(ref, ref, self.sems[2].at[n, d], self.sems[3].at[n, d], (p.s + 2, p.t))

    def over(self, n, d):
        p, (own_ref, all_ref) = self.p, self.pairs[n]
        block = p.s - 2 * d
        k = d + p.Z - 1
        src = own_ref if d == 0 else all_ref.at[block]
        return push(src, all_ref.at[block], self.sems[4].at[n, k], self.sems[5].at[n, k], p.across)

    def over_wait(self, n, d):
        p, (_, all_ref) = self.p, self.pairs[n]
        ref = all_ref.at[p.z * 2 + 1 - p.x - 2 * d]
        k = d + p.Z - 1
        return push(ref, ref, self.sems[4].at[n, k], self.sems[5].at[n, k], p.across)

    def start(self, count):
        p = self.p

        @pl.when(p.z + 1 < p.Z)
        def _():
            for n in count:
                self.up(n, 1, True).start()

        @pl.when(p.z >= 1)
        def _():
            for n in count:
                self.dn(n, 1, True).start()

        for n in count:
            self.over(n, 0).start()

    def step(self, d):
        p = self.p
        for n in range(len(self.pairs)):

            @pl.when(p.z - d >= 0)
            def _():
                self.up_wait(n, d).wait_recv()

                @pl.when(p.z + 1 < p.Z)
                def _():
                    self.up(n, d + 1).start()

                self.over(n, d).start()

            @pl.when(p.z + d < p.Z)
            def _():
                self.dn_wait(n, d).wait_recv()

                @pl.when(p.z >= 1)
                def _():
                    self.dn(n, d + 1).start()

                self.over(n, -d).start()

    def arrive(self, sign, d):
        for n in range(len(self.pairs)):
            self.over_wait(n, sign * d).wait_recv()

    def side(self, sign, d):
        return self.p.z - d >= 0 if sign > 0 else self.p.z + d < self.p.Z

    def finish(self):
        p = self.p
        for n in range(len(self.pairs)):
            for d in range(p.Z):
                for sign in (1, -1) if d else (1,):

                    @pl.when(self.side(sign, d))
                    def _():
                        self.over(n, sign * d).wait_send()

            for d in range(1, p.Z):

                @pl.when(jnp.logical_and(p.z - d + 1 >= 0, p.z + 1 < p.Z))
                def _():
                    self.up(n, d).wait_send()

                @pl.when(jnp.logical_and(p.z + d - 1 < p.Z, p.z >= 1))
                def _():
                    self.dn(n, d).wait_send()


def line_sems(p_z, n):
    return [pltpu.SemaphoreType.DMA((n, p_z + 1))] * 4 + [pltpu.SemaphoreType.DMA((n, 2 * p_z))] * 2


class PairScatter:
    def __init__(self, p, part, first, summed, second, fs, fr, ss, sr):
        self.p, self.part, self.first, self.summed, self.second = p, part, first, summed, second
        self.sems = (fs, fr, ss, sr)
        self.started = []

    def start(self):
        p = self.p
        for d in range(p.Y):
            y = lax.rem(p.y + d, p.Y)
            copy = push(
                self.part(y * 2 + 1 - p.c), self.first.at[d], self.sems[0].at[d], self.sems[1].at[d], p.partner
            )
            copy.start()
            self.started.append(copy)

    def middle(self):
        p = self.p
        for d in list(range(1, p.Y)) + [0]:
            y = lax.rem(p.y + d, p.Y)
            self.started[d].wait_recv()
            total = self.part(y * 2 + p.c)[...].astype(F32) + self.first[d].astype(F32)
            self.summed[d] = total.astype(BF)
            if d:
                copy = push(
                    self.summed.at[d], self.second.at[d], self.sems[2].at[d], self.sems[3].at[d], p.chip_y(d)
                )
                copy.start()
                self.started.append(copy)

    def finish(self):
        p = self.p
        total = self.part(p.t)[...].astype(F32) + self.first[0].astype(F32)
        for d in range(1, p.Y):
            self.started[p.Y + d - 1].wait_recv()
            total = total + self.second[d].astype(F32)
        for copy in self.started:
            copy.wait_send()
        return total


class PairGather:
    def __init__(self, p, own, spot, ys, yr, ps, pr):
        self.p, self.own, self.spot, self.sems = p, own, spot, (ys, yr, ps, pr)
        self.started = []

    def start(self):
        p = self.p
        for d in range(1, p.Y):
            copy = push(self.own, self.spot(p.t), self.sems[0].at[d], self.sems[1].at[d], p.chip_y(d))
            copy.start()
            self.started.append(copy)
        copy = push(self.own, self.spot(p.t), self.sems[2].at[0], self.sems[3].at[0], p.partner)
        copy.start()
        self.started.append(copy)

    def forward(self):
        p = self.p
        for d in range(1, p.Y):
            ref = self.spot(lax.rem(p.y - d + p.Y, p.Y) * 2 + p.c)
            push(ref, ref, self.sems[0].at[d], self.sems[1].at[d], p.chip_y(-d)).wait_recv()
            copy = push(ref, ref, self.sems[2].at[d], self.sems[3].at[d], p.partner)
            copy.start()
            self.started.append(copy)

    def arrive(self):
        p = self.p
        for d in range(p.Y):
            ref = self.spot(lax.rem(p.y - d + p.Y, p.Y) * 2 + 1 - p.c)
            push(ref, ref, self.sems[2].at[d], self.sems[3].at[d], p.partner).wait_recv()

    def finish(self):
        for copy in self.started:
            copy.wait_send()


def layer_kernel(
    sp, tp, shift_base,
    raw, to, src, gain, saved, offs, wq_h, wk_h, wv_h, wo_h,
    flat_all, src_out, tgt_out, cols_all,
    tn, pieces, wq, wk, wv, wo, tn_all, to_all, src_all, cols, tn_b, to_b,
    q_all, hg_all, small_all, k_s, v_s, p_s, d_s, part, kf, vf, sg,
    xr, xz, zr, sg1, sg2, sg3, ng, ng1, ng2, ng3,
    wsem, loc, es, er, *sems
):
    p = Place(sp, tp)
    pair_sems = [sems[4 * i : 4 * i + 4] for i in range(6)]
    xs_s, xs_r, zs_s, zs_r = sems[24:28]
    line_a, line_b = sems[28:34], sems[34:40]
    rows, block = raw.shape[0], saved.shape[0]
    width, model = wq.shape[1], wq.shape[0]
    heads = width // HEAD_DIM
    scale = HEAD_DIM ** (-0.5)
    loads = [
        pltpu.make_async_copy(h, v, wsem.at[i])
        for i, (h, v) in enumerate(((wq_h, wq), (wo_h, wo), (wk_h, wk), (wv_h, wv)))
    ]
    for copy in loads:
        copy.start()
    raw_value, gain_value = raw[...].astype(F32), gain[...].astype(F32).reshape(1, model)
    inverse = lax.rsqrt(jnp.mean(raw_value * raw_value, axis=1, keepdims=True) + EPSILON)
    normed_value = (raw_value * inverse * gain_value).astype(BF)
    tn[...] = normed_value
    slice_width = model // sp
    for s in range(sp):
        pieces[s] = normed_value[:, s * slice_width : (s + 1) * slice_width]
    greet(
        [p.partner]
        + [p.chip_y(d) for d in range(1, p.Y)]
        + [(lax.rem(p.s + e, sp), p.t) for e in range(1, sp)]
    )
    g_tn = PairGather(p, tn, lambda t: tn_all.at[t], *pair_sems[0])
    g_to = PairGather(p, to, lambda t: to_all.at[t], *pair_sems[1])
    g_src = PairGather(p, src, lambda t: src_all.at[t], *pair_sems[2])
    g_cols = PairGather(p, cols, lambda t: cols_all.at[:, t], *pair_sems[3])
    for g in (g_tn, g_to, g_src):
        g.start()
    swaps = []
    for e in range(1, sp):
        s = lax.rem(p.s + e, sp)
        copy = push(pieces.at[s], cols.at[p.s], es.at[e], er.at[e], (s, p.t))
        copy.start()
        swaps.append(copy)
    mine = [
        pltpu.make_async_copy(tn, tn_all.at[p.t], loc.at[0]),
        pltpu.make_async_copy(to, to_all.at[p.t], loc.at[1]),
        pltpu.make_async_copy(src, src_all.at[p.t], loc.at[2]),
        pltpu.make_async_copy(pieces.at[p.s], cols.at[p.s], loc.at[3]),
    ]
    for copy in mine:
        copy.start()
    for copy in mine:
        copy.wait()
    tile = min(width, 256)
    gather = LineGather(
        p, ((q_all.at[p.s], q_all), (hg_all.at[p.s], hg_all), (small_all.at[p.s], small_all)), *line_a
    )

    g_tn.forward()
    g_to.forward()
    g_tn.arrive()
    for t in range(tp):
        tn_b[t * rows : (t + 1) * rows, :] = tn_all[t]
    loads[0].wait()
    for j in range(0, width, tile):
        q_all[p.s, :, j : j + tile] = jnp.dot(
            tn_b[...], wq[:, j : j + tile], preferred_element_type=F32
        ).astype(BF)
    gather.start((0,))
    g_to.arrive()
    for t in range(tp):
        to_b[t * rows : (t + 1) * rows, :] = to_all[t]
    loads[1].wait()
    lane = lax.broadcasted_iota(jnp.int32, (block, 128), 1)
    pick = lax.broadcasted_iota(jnp.int32, (heads, 128), 0) == lax.broadcasted_iota(jnp.int32, (heads, 128), 1)
    small = lax.dot_general(
        offs[...].astype(F32), pick.astype(F32), (((0,), (0,)), ((), ())), precision=lax.Precision.HIGHEST,
        preferred_element_type=F32,
    )
    for h in range(heads):
        cut = slice(h * HEAD_DIM, (h + 1) * HEAD_DIM)
        part_h = contract_last(to_b[...], wo[cut, :]).astype(BF)
        hg_all[p.s, :, cut] = part_h
        delta = jnp.sum(part_h.astype(F32) * saved[:, cut].astype(F32), axis=1, keepdims=True)
        small = jnp.where(lane == heads + h, delta, small)
    small_all[p.s] = small.astype(BF)
    gather.start((1, 2))

    g_src.forward()
    g_src.arrive()
    gather.step(1)
    source_count = k_s.shape[0]
    loads[2].wait()
    loads[3].wait()

    @pl.loop(0, width // tile)
    def _(j):
        cut = pl.ds(pl.multiple_of(j * tile, tile), tile)
        rows_value = src_all[...].reshape(source_count, model)
        k_s[:, cut] = jnp.dot(rows_value, wk[:, cut], preferred_element_type=F32).astype(BF)
        v_s[:, cut] = jnp.dot(rows_value, wv[:, cut], preferred_element_type=F32).astype(BF)

    for e in range(1, sp):
        s = lax.rem(p.s - e + sp, sp)
        push(cols.at[s], cols.at[s], es.at[e], er.at[e], (s, p.t)).wait_recv()
    g_cols.start()
    keep = pltpu.make_async_copy(cols, cols_all.at[:, p.t], loc.at[4])
    keep.start()

    def into(k):
        z = lax.rem(p.z + k, p.Z)
        return push(part.at[z * 2 + 1 - p.x], xr.at[k], xs_s.at[k], xs_r.at[k], p.across)

    def attend(z):
        pair = pl.ds(2 * z, 2)
        spot = pl.ds(pl.multiple_of(z * (2 * block), 2 * block), 2 * block)
        tiny = small_all[pair].reshape(2 * block, 128).astype(F32)
        for h in range(heads):
            cut = slice(h * HEAD_DIM, (h + 1) * HEAD_DIM)
            q_h = q_all[pair, :, cut].reshape(2 * block, HEAD_DIM)
            g_h = hg_all[pair, :, cut].reshape(2 * block, HEAD_DIM)
            prob = jnp.exp(contract_last(q_h, k_s[:, cut]) * scale - (shift_base + tiny[:, h : h + 1]))
            grad = contract_last(g_h, v_s[:, cut])
            score = (prob * (grad - tiny[:, heads + h : heads + h + 1]) * scale).astype(BF)
            p_s[h, spot, :] = prob.astype(BF)
            d_s[h, spot, :] = score
            term = jnp.dot(score, k_s[:, cut], preferred_element_type=F32).astype(BF)
            part[pair, :, cut] = term.reshape(2, block, HEAD_DIM)

    def reached(sign, d):
        gather.arrive(sign, d)
        attend(p.z - sign * d)
        into((-sign * d) % p.Z).start()

    for d in range(1, p.Z):
        if d > 1:
            gather.step(d)
        for sign in (1, -1) if d > 1 else (1,):

            @pl.when(gather.side(sign, d - 1))
            def _():
                reached(sign, d - 1)

        if d == 1:
            g_cols.forward()
    for sign in (1, -1):

        @pl.when(gather.side(sign, p.Z - 1))
        def _():
            reached(sign, p.Z - 1)

    order = sorted(range(1, p.Z), key=lambda k: min(k, p.Z - k))
    hops = {}

    def relay(k):
        into(k).wait_recv()
        z = lax.rem(p.z + k, p.Z)
        xz[k] = (part[z * 2 + p.x].astype(F32) + xr[k].astype(F32)).astype(BF)
        hops[k] = push(xz.at[k], zr.at[k], zs_s.at[k], zs_r.at[k], p.chip_z(k))
        hops[k].start()

    for k in order[:1]:
        relay(k)
    count = sp * block

    for h in range(heads):
        cut = slice(h * HEAD_DIM, (h + 1) * HEAD_DIM)
        dims = (((0,), (0,)), ((), ()))
        q_h = q_all[:, :, cut].reshape(count, HEAD_DIM)
        g_h = hg_all[:, :, cut].reshape(count, HEAD_DIM)
        kf[:, cut] = lax.dot_general(d_s[h], q_h, dims, preferred_element_type=F32).astype(BF)
        vf[:, cut] = lax.dot_general(p_s[h], g_h, dims, preferred_element_type=F32).astype(BF)
    for k in order[1:2]:
        relay(k)
    stile = min(model, 256)

    def source_term(j):
        cut = pl.ds(pl.multiple_of(j * stile, stile), stile)
        value = contract_last(kf[...], wk[cut, :]) + contract_last(vf[...], wv[cut, :])
        sg[:, :, cut] = value.astype(BF).reshape(tp, source_count // tp, stile)

    half = model // stile // 2
    pl.loop(0, half)(source_term)
    for k in order[2:]:
        relay(k)
    pl.loop(half, model // stile)(source_term)
    source = PairScatter(p, lambda t: sg.at[t], sg1, sg2, sg3, *pair_sems[4])
    source.start()
    source.middle()
    into(0).wait_recv()
    total = part[p.s].astype(F32) + xr[0].astype(F32)
    for k in order:
        hops[k].wait_recv()
        total = total + zr[k].astype(F32)
    flat = total.astype(BF)
    flat_all[p.s] = flat
    spread = LineGather(p, ((flat_all.at[p.s], flat_all),), *line_b)
    spread.start((0,))
    for j in range(0, model, stile):
        columns = contract_last(flat, wq[j : j + stile, :]).astype(BF)
        for t in range(tp):
            ng[t, :, j : j + stile] = columns[t * rows : (t + 1) * rows]
    normed = PairScatter(p, lambda t: ng.at[t], ng1, ng2, ng3, *pair_sems[5])
    normed.start()
    for d in range(1, p.Z):
        spread.step(d)
        if d == 1:
            normed.middle()
    src_out[...] = source.finish()
    raw_value, gain_value = raw[...].astype(F32), gain[...].astype(F32).reshape(1, model)
    inverse = lax.rsqrt(jnp.mean(raw_value * raw_value, axis=1, keepdims=True) + EPSILON)
    scaled = normed.finish() * gain_value
    tgt_out[...] = inverse * scaled - raw_value * (inverse * inverse * inverse) * jnp.mean(
        scaled * raw_value, axis=1, keepdims=True
    )
    g_cols.arrive()
    for d in range(p.Z):
        for sign in (1, -1) if d else (1,):

            @pl.when(spread.side(sign, d))
            def _():
                spread.arrive(sign, d)

    gather.finish()
    spread.finish()
    for g in (g_tn, g_to, g_src, g_cols):
        g.finish()
    for copy in swaps:
        copy.wait_send()
    keep.wait()
    for k in range(p.Z):
        into(k).wait_send()
    for k in order:
        hops[k].wait_send()


def body(
    target_rows,
    source_rows,
    norm_gain,
    query_weight,
    key_weight,
    value_weight,
    output_weight,
    saved_output,
    norm_offset,
    output_grad,
):
    tp, sp = lax.axis_size("tp"), lax.axis_size("sp")
    Z, Y = sp // 2, tp // 2
    model, width = query_weight.shape
    heads = width // HEAD_DIM
    rows, srows = target_rows.shape[0], source_rows.shape[0]
    block = rows * tp
    count = block * sp
    source_count = srows * tp
    shift_base = math.log(source_count * sp)
    slice_width = model // sp
    dma = pltpu.SemaphoreType.DMA

    vm = pltpu.VMEM
    whole = pl.BlockSpec(memory_space=pl.ANY)
    flat_all, source_grad, target_grad, cols_all = pl.pallas_call(
        functools.partial(layer_kernel, sp, tp, shift_base),
        out_shape=[
            jax.ShapeDtypeStruct((sp, block, width), BF),
            jax.ShapeDtypeStruct((srows, model), F32),
            jax.ShapeDtypeStruct((rows, model), F32),
            jax.ShapeDtypeStruct((sp, tp, rows, slice_width), BF),
        ],
        in_specs=[VMEM] * 6 + [whole] * 4,
        out_specs=[VMEM] * 4,
        scratch_shapes=[vm((rows, model), BF), vm((sp, rows, slice_width), BF)]
        + [vm((model, width), BF)] * 3
        + [vm((width, model), BF)]
        + [vm((tp, rows, model), BF)] * 2
        + [vm((tp, srows, model), BF), vm((sp, rows, slice_width), BF)]
        + [vm((block, model), BF)] * 2
        + [vm((sp, block, width), BF)] * 2
        + [vm((sp, block, 128), BF)]
        + [vm((source_count, width), BF)] * 2
        + [vm((heads, count, source_count), BF)] * 2
        + [vm((sp, block, width), BF)]
        + [vm((source_count, width), BF)] * 2
        + [vm((tp, srows, model), BF)]
        + [vm((Z, block, width), BF)] * 3
        + [vm((Y, srows, model), BF)] * 3
        + [vm((tp, rows, model), BF)]
        + [vm((Y, rows, model), BF)] * 3
        + [dma((4,)), dma((5,)), dma((sp,)), dma((sp,))]
        + [dma((Y,))] * 24
        + [dma((Z,))] * 4
        + line_sems(Z, 3)
        + line_sems(Z, 1),
        name="layer_kernel",
        compiler_params=pltpu.CompilerParams(
            collective_id=1, has_side_effects=True, vmem_limit_bytes=58 * 2**20
        ),
    )(
        target_rows,
        output_grad,
        source_rows,
        norm_gain,
        saved_output,
        norm_offset.T,
        query_weight,
        key_weight,
        value_weight,
        output_weight,
    )
    weight_grad = lax.dot_general(
        cols_all.reshape(count, slice_width),
        flat_all.reshape(count, width),
        (((0,), (0,)), ((), ())),
        preferred_element_type=F32,
    )
    return (target_grad, source_grad, weight_grad)


class Net:
    def __init__(self, send, recv):
        self.sems, self.ids, self.started = (send, recv), {}, []

    def _copy(self, name, src, dst, device):
        n = self.ids.setdefault(name, len(self.ids))
        return push(src, dst, self.sems[0].at[n], self.sems[1].at[n], device)

    def go(self, name, src, dst, device):
        copy = self._copy(name, src, dst, device)
        copy.start()
        self.started.append(copy)

    def same(self, name, ref, device):
        self.go(name, ref, ref, device)

    def wait(self, name, landed, device):
        self._copy(name, landed, landed, device).wait_recv()

    def drain(self, count=None):
        count = len(self.started) if count is None else count
        for copy in self.started[:count]:
            copy.wait_send()
        self.started = self.started[count:]


TRANSFERS = 176
Y_FIRST = (False, False, True, True)


def grid_kernel(
    sp, tp, shift_base,
    raw_h, to_h, src_h, gain_h, saved_h, offs_h, wq_h, wk_h, wv_h, wo_h,
    ws_h, src_h_out, tgt_h_out,
    raw, gain, saved, offs, ws, src_out, tgt_out,
    tn_all, to_all, src_all, pieces, cols, q_st, g_st, sm_st, q_all, g_all, sm_all,
    wq, wkv, wo, kv, p_s, d_s, part, xr, xs, ur, flat_all, fl, kv_sum, kvf,
    sg, sd, ss, es, fs, fr, na, ng, ng1, ng2, ng3, wt,
    wsem, osem, send, recv, *sems
):
    p = Place(sp, tp)
    s, t, y, c, x = p.s, p.t, p.y, p.c, p.x
    u, v = p.z // 2, p.z % 2
    net = Net(send, recv)

    def at(u, v, x):
        return ((u * 2 + v) * 2 + x, t)

    C, Y, V, X, U = p.partner, p.chip_y(1), at(u, 1 - v, x), at(u, v, 1 - x), at(1 - u, v, x)
    ty, tc, tyc = (1 - y) * 2 + c, y * 2 + 1 - c, (1 - y) * 2 + 1 - c
    others = [
        (a, b, d, u + a - 2 * u * a, v + b - 2 * v * b, x + d - 2 * x * d)
        for a in range(2) for b in range(2) for d in range(2) if a + b + d
    ]
    barrier = pltpu.get_barrier_semaphore()
    friends = [C, Y] + [at(*o[3:]) for o in others]
    for device in friends:
        pl.semaphore_signal(barrier, inc=1, device_id=device, device_id_type=MESH)
    rows, block, srows = raw.shape[0], saved.shape[0], src_h.shape[0]
    model, width = wq.shape
    heads = width // HEAD_DIM
    hh, half = heads // 2, width // 2
    sblock = srows * tp
    sw = model // sp
    quarters = len(Y_FIRST)
    mq = model // quarters
    scale = HEAD_DIM ** (-0.5)
    mine = pl.ds(pl.multiple_of(v * half, half), half)
    loads = [
        pltpu.make_async_copy(h, w, wsem.at[i])
        for i, (h, w) in enumerate(
            (
                (wq_h, wq), (wo_h, wo), (wk_h.at[:, mine], wkv.at[:, :half]), (wv_h.at[:, mine], wkv.at[:, half:]),
                (raw_h, raw), (gain_h, gain), (src_h, src_all.at[v, t]), (to_h, to_all.at[t]),
                (saved_h, saved), (offs_h, offs),
            )
        )
    ]
    for n in (4, 5, 6, 7, 0, 1, 8, 9, 2, 3):
        loads[n].start()
    loads[4].wait()
    loads[5].wait()
    raw_value, gain_value = raw[...].astype(F32), gain[...].astype(F32).reshape(1, model)
    inverse = lax.rsqrt(jnp.mean(raw_value * raw_value, axis=1, keepdims=True) + EPSILON)
    normed_value = (raw_value * inverse * gain_value).astype(BF)
    tn_all[t] = normed_value
    for a in range(2):
        for b in range(2):
            for k in range(2):
                n = (2 * a + k) * 2 + b
                pieces[a, b, :, k * sw : (k + 1) * sw] = normed_value[:, n * sw : (n + 1) * sw]
    loads[6].wait()
    loads[7].wait()
    pl.semaphore_wait(barrier, len(friends))
    A, B = pl.ds(0, srows // 2), pl.ds(srows // 2, srows // 2)

    net.same("tnY", tn_all.at[t], Y)
    net.same("sVB", src_all.at[v, t, B], V)
    net.same("tnC", tn_all.at[t], C)
    net.same("toY", to_all.at[t], Y)
    net.same("toC", to_all.at[t], C)
    net.same("sYA", src_all.at[v, t, A], Y)
    net.same("sVA", src_all.at[v, t, A], V)
    net.same("sYB", src_all.at[v, t, B], Y)
    net.same("sC", src_all.at[v, t], C)
    net.wait("tnY", tn_all.at[ty], Y)
    net.same("tnF", tn_all.at[ty], C)
    net.wait("toY", to_all.at[ty], Y)
    net.same("toF", to_all.at[ty], C)
    net.wait("tnC", tn_all.at[tc], C)
    net.wait("tnF", tn_all.at[tyc], C)
    loads[0].wait()
    tn_b = tn_all[...].reshape(block, model)
    for k in range(2):
        for j in range(0, half, HEAD_DIM):
            q_st[k, :, j : j + HEAD_DIM] = jnp.dot(
                tn_b, wq[:, k * half + j : k * half + j + HEAD_DIM], preferred_element_type=F32
            ).astype(BF)
    net.go("qV", q_st.at[1 - v], q_all.at[u, x, v], V)
    q_all[u, x, v] = q_st[v]
    net.same("q0U", q_all.at[u, x, v], U)
    net.same("q0X", q_all.at[u, x, v], X)
    net.wait("sVB", src_all.at[1 - v, t, B], V)
    net.same("fVB", src_all.at[1 - v, t, B], Y)
    net.same("cVB", src_all.at[1 - v, t, B], C)
    net.wait("toC", to_all.at[tc], C)
    net.wait("toF", to_all.at[tyc], C)
    loads[1].wait()
    loads[8].wait()
    loads[9].wait()
    to_b = to_all[...].reshape(block, model)
    products = []
    for n in range(heads):
        cut = slice(n * HEAD_DIM, (n + 1) * HEAD_DIM)
        part_h = contract_last(to_b, wo[cut, :]).astype(BF)
        g_st[n // hh, :, n % hh * HEAD_DIM : (n % hh + 1) * HEAD_DIM] = part_h
        products.append(part_h.astype(F32) * saved[:, cut].astype(F32))
    net.go("gV", g_st.at[1 - v], g_all.at[u, x, v], V)
    g_all[u, x, v] = g_st[v]
    net.same("g0U", g_all.at[u, x, v], U)
    net.same("g0X", g_all.at[u, x, v], X)
    lines, lanes = sm_st.shape[1], 2 * block
    place = (
        lax.broadcasted_iota(jnp.int32, (block, lanes), 1)
        == lax.broadcasted_iota(jnp.int32, (block, lanes), 0) + v * block
    ).astype(F32)
    spread = jnp.dot(offs[...].astype(F32), place, precision=lax.Precision.HIGHEST, preferred_element_type=F32)
    product = jnp.concatenate(products, axis=1)
    line = lax.broadcasted_iota(jnp.int32, (2 * lines, width), 0)
    head = lax.broadcasted_iota(jnp.int32, (2 * lines, width), 1) // HEAD_DIM
    pick = (line == head // hh * lines + hh + head % hh).astype(BF)
    deltas = 0.0
    for term in range(3):
        narrow = product.astype(BF)
        product = product - narrow.astype(F32)
        padded = jnp.concatenate(
            [jnp.where(v == 0, narrow, jnp.zeros_like(narrow)), jnp.where(v == 1, narrow, jnp.zeros_like(narrow))],
            axis=0,
        )
        deltas = deltas + contract_last(pick, padded)
    line = lax.broadcasted_iota(jnp.int32, (lines, lanes), 0)
    for k in range(2):
        small = deltas[k * lines : (k + 1) * lines]
        for h in range(hh):
            n = k * hh + h
            small = jnp.where(line == h, jnp.broadcast_to(spread[n : n + 1], small.shape), small)
        sm_st[k] = small.astype(BF)
    net.go("mV", sm_st.at[1 - v], sm_all.at[u, x, v], V)
    sm_all[u, x, v] = sm_st[v]
    net.same("m0U", sm_all.at[u, x, v], U)
    net.same("m0X", sm_all.at[u, x, v], X)

    net.wait("sYA", src_all.at[v, ty, A], Y)
    net.same("cYA", src_all.at[v, ty, A], C)
    net.wait("qV", q_all.at[u, x, 1 - v], V)
    net.same("q1U", q_all.at[u, x, 1 - v], U)
    net.same("q1X", q_all.at[u, x, 1 - v], X)
    net.wait("sVA", src_all.at[1 - v, t, A], V)
    net.same("fVA", src_all.at[1 - v, t, A], Y)
    net.same("cVA", src_all.at[1 - v, t, A], C)
    net.wait("gV", g_all.at[u, x, 1 - v], V)
    net.same("g1U", g_all.at[u, x, 1 - v], U)
    net.same("g1X", g_all.at[u, x, 1 - v], X)
    net.wait("sYB", src_all.at[v, ty, B], Y)
    net.same("cYB", src_all.at[v, ty, B], C)
    net.wait("mV", sm_all.at[u, x, 1 - v], V)
    net.same("m1U", sm_all.at[u, x, 1 - v], U)
    net.same("m1X", sm_all.at[u, x, 1 - v], X)
    def project(k, y):
        count = 2 * srows
        spot = pl.ds(pl.multiple_of(k * sblock + y * count, count), count)

        @pl.loop(0, 2)
        def _(j):
            cut = pl.ds(pl.multiple_of(j * half, half), half)
            value = src_all[k, pl.ds(2 * y, 2)].reshape(count, model)
            kv[spot, cut] = jnp.dot(value, wkv[:, cut], preferred_element_type=F32).astype(BF)

    net.wait("sC", src_all.at[v, tc], C)
    loads[2].wait()
    loads[3].wait()
    project(v, y)
    spot = (u * 2 + x) * 2 + v
    for a, b, d, u2, v2, x2 in others:
        net.go(f"p{a}{b}{d}", pieces.at[u2, x2], cols.at[spot, t], at(u2, v2, x2))
    cols[spot, t] = pieces[u, x]
    net.wait("q0U", q_all.at[1 - u, x, v], U)
    net.same("q2X", q_all.at[1 - u, x, v], X)
    net.wait("cVB", src_all.at[1 - v, tc, B], C)
    net.wait("cVA", src_all.at[1 - v, tc, A], C)
    project(1 - v, y)
    net.wait("cYA", src_all.at[v, tyc, A], C)
    net.wait("cYB", src_all.at[v, tyc, B], C)
    net.wait("fVB", src_all.at[1 - v, ty, B], Y)
    net.same("dVB", src_all.at[1 - v, ty, B], C)
    net.wait("g0U", g_all.at[1 - u, x, v], U)
    net.same("g2X", g_all.at[1 - u, x, v], X)
    project(v, 1 - y)
    net.wait("fVA", src_all.at[1 - v, ty, A], Y)
    net.same("dVA", src_all.at[1 - v, ty, A], C)
    net.wait("m0U", sm_all.at[1 - u, x, v], U)
    net.same("m2X", sm_all.at[1 - u, x, v], X)
    net.wait("q1U", q_all.at[1 - u, x, 1 - v], U)
    net.same("q3X", q_all.at[1 - u, x, 1 - v], X)
    net.wait("dVB", src_all.at[1 - v, tyc, B], C)
    net.wait("dVA", src_all.at[1 - v, tyc, A], C)
    project(1 - v, 1 - y)

    def attend(w, after):
        little = sm_all[w].astype(F32)
        little = jnp.concatenate([little[0, 0] + little[0, 1], little[1, 0] + little[1, 1]], axis=1)
        for h in range(hh):
            cut = slice(h * HEAD_DIM, (h + 1) * HEAD_DIM)
            q_h = q_all[w, :, :, :, cut].reshape(4 * block, HEAD_DIM)
            g_h = g_all[w, :, :, :, cut].reshape(4 * block, HEAD_DIM)
            prob = jnp.exp(contract_last(kv[:, cut], q_h) * scale - (shift_base + little[h : h + 1]))
            grad = contract_last(kv[:, half + h * HEAD_DIM : half + (h + 1) * HEAD_DIM], g_h)
            score = (prob * (grad - little[hh + h : hh + h + 1]) * scale).astype(BF)
            p_s[h] = prob.astype(BF)
            d_s[h] = score
            term = lax.dot_general(score, kv[:, cut], (((0,), (0,)), ((), ())), preferred_element_type=F32)
            part[w, :, h] = term.astype(BF).reshape(2, 2, block, HEAD_DIM)
            after(h)

    def source_terms(w):
        for h in range(hh):
            cut = slice(h * HEAD_DIM, (h + 1) * HEAD_DIM)
            q_h = q_all[w, :, :, :, cut].reshape(4 * block, HEAD_DIM)
            g_h = g_all[w, :, :, :, cut].reshape(4 * block, HEAD_DIM)
            yield cut, jnp.dot(d_s[h], q_h, preferred_element_type=F32)
            cut = slice(half + h * HEAD_DIM, half + (h + 1) * HEAD_DIM)
            yield cut, jnp.dot(p_s[h], g_h, preferred_element_type=F32)

    def send_near(h):
        net.go(f"a{h}X", part.at[u, 1 - x, h], xr.at[0, h], X)

    def send_far(h):
        for k in range(2):
            net.go(f"b{h}{k}X", part.at[1 - u, 1 - x, h, k], xr.at[1, h, k], X)

    for n, k in ((0, v), (1, 1 - v)):
        net.wait(f"q{n}X", q_all.at[u, 1 - x, k], X)
        net.wait(f"m{n}X", sm_all.at[u, 1 - x, k], X)
        net.wait(f"g{n}X", g_all.at[u, 1 - x, k], X)
    attend(u, lambda h: None if h else send_near(h))
    net.wait("g1U", g_all.at[1 - u, x, 1 - v], U)
    net.same("g3X", g_all.at[1 - u, x, 1 - v], X)
    net.wait("m1U", sm_all.at[1 - u, x, 1 - v], U)
    net.same("m3X", sm_all.at[1 - u, x, 1 - v], X)
    for h in range(1, hh):
        send_near(h)
    for cut, value in source_terms(u):
        kv_sum[:, cut] = value

    def near(h):
        net.wait(f"a{h}X", xr.at[0, h], X)
        xs[0, h] = (part[u, x, h].astype(F32) + xr[0, h].astype(F32)).astype(BF)
        net.go(f"s{h}U", xs.at[0, h], ur.at[1, h], U)

    near(0)
    early = len(net.started)
    for n, k in ((2, v), (3, 1 - v)):
        net.wait(f"q{n}X", q_all.at[1 - u, 1 - x, k], X)
        net.wait(f"m{n}X", sm_all.at[1 - u, 1 - x, k], X)
        net.wait(f"g{n}X", g_all.at[1 - u, 1 - x, k], X)
    attend(1 - u, send_far)
    for h in range(1, hh):
        near(h)
    for cut, value in source_terms(1 - u):
        kvf[:, cut] = (kv_sum[:, cut] + value).astype(BF)
    for a, b, d, u2, v2, x2 in others:
        net.wait(f"p{a}{b}{d}", cols.at[(u2 * 2 + x2) * 2 + v2, t], at(u2, v2, x2))
    net.same("kY", cols.at[:, t], Y)
    net.same("kC", cols.at[:, t], C)
    stile = min(mq, 256)

    def source(n):
        for j in range(0, mq, stile):
            value = contract_last(kvf[...], wkv[n * mq + j : n * mq + j + stile, :]).astype(BF)
            sg[n, :, :, :, j : j + stile] = value.reshape(4, 2, srows, stile)
        net.go(f"d{n}", sg.at[n, :, 1 - c], sd.at[n], C)

    def source_sum(n):
        net.wait(f"d{n}", sd.at[n], C)
        for k in range(4):
            ss[n, k] = (sg[n, k, c].astype(F32) + sd[n, k].astype(F32)).astype(BF)
        first, keep = (Y, 2 * v + 1 - y) if Y_FIRST[n] else (V, 2 * (1 - v) + y)
        net.go(f"e{n}1", ss.at[n, 2 * (1 - v) + 1 - y], es.at[n, 1], first)
        net.go(f"e{n}0", ss.at[n, keep], es.at[n, 0], first)

    def source_pass(n):
        first, last = (Y, V) if Y_FIRST[n] else (V, Y)
        keep = 2 * (1 - v) + y if Y_FIRST[n] else 2 * v + 1 - y
        net.wait(f"e{n}1", es.at[n, 1], first)
        fs[n] = (ss[n, keep].astype(F32) + es[n, 1].astype(F32)).astype(BF)
        net.go(f"f{n}", fs.at[n], fr.at[n], last)

    kept = []

    def keep(ref, out):
        copy = pltpu.make_async_copy(ref, out, osem.at[len(kept)])
        copy.start()
        kept.append(copy)

    def source_end(n):
        first, last = (Y, V) if Y_FIRST[n] else (V, Y)
        net.wait(f"e{n}0", es.at[n, 0], first)
        net.wait(f"f{n}", fr.at[n], last)
        src_out[n] = ss[n, 2 * v + y].astype(F32) + es[n, 0].astype(F32) + fr[n].astype(F32)
        keep(src_out.at[n], src_h_out.at[n])

    def far(h):
        for k in range(2):
            net.wait(f"b{h}{k}X", xr.at[1, h, k], X)
            xs[1, h, k] = (part[1 - u, x, h, k].astype(F32) + xr[1, h, k].astype(F32)).astype(BF)
            net.go(f"z{h}{k}U", xs.at[1, h, k], ur.at[0, h, k], U)

    def flat_far(h):
        net.wait(f"s{h}U", ur.at[1, h], U)
        flat_all[1 - u, x, h] = (xs[1, h].astype(F32) + ur[1, h].astype(F32)).astype(BF)
        net.same(f"w{h}X", flat_all.at[1 - u, x, h], X)

    def flat_near(h):
        for k in range(2):
            net.wait(f"z{h}{k}U", ur.at[0, h, k], U)
            flat_all[u, x, h, k] = (xs[0, h, k].astype(F32) + ur[0, h, k].astype(F32)).astype(BF)
            net.same(f"r{h}{k}X", flat_all.at[u, x, h, k], X)
        net.go(f"n{h}V", flat_all.at[u, x, h, 1 - v], fl.at[v, h], V)
        fl[v, h] = flat_all[u, x, h, v]

    def weight(h):
        for k in range(2):
            net.wait(f"r{h}{k}X", flat_all.at[u, 1 - x, h, k], X)
        net.wait(f"w{h}X", flat_all.at[1 - u, 1 - x, h], X)
        flat_h = flat_all[:, :, h].reshape(sp * block, HEAD_DIM)
        for k in range(2):
            wt[h, k] = lax.dot_general(
                cols[:, :, :, k * sw : (k + 1) * sw].reshape(sp * block, sw), flat_h,
                (((0,), (0,)), ((), ())), preferred_element_type=F32,
            ).astype(BF)
        net.go(f"W{h}", wt.at[h, 1 - v], ws.at[v, h], V)
        ws[v, h] = wt[h, v]
        keep(ws.at[v, h], ws_h.at[v, h])

    ntile = min(model, 256)

    def normed_term(h):
        net.wait(f"n{h}V", fl.at[1 - v, h], V)
        for j in range(0, model, ntile):
            columns = 0.0 if h == 0 else na[:, j : j + ntile]
            for k in range(2):
                n = (k * hh + h) * HEAD_DIM
                columns = columns + contract_last(fl[k, h], wq[j : j + ntile, n : n + HEAD_DIM])
            if h < hh - 1:
                na[:, j : j + ntile] = columns
            else:
                ng[:, :, j : j + ntile] = columns.astype(BF).reshape(tp, rows, ntile)

    source(0)
    far(0)
    source(1)
    for h in range(1, hh):
        far(h)
    source_sum(0)
    flat_far(0)
    source(2)
    for h in range(1, hh):
        flat_far(h)
    source_sum(1)
    source(3)
    source_sum(2)
    net.wait("kY", cols.at[:, ty], Y)
    net.same("kF", cols.at[:, ty], C)
    net.drain(early)
    flat_near(0)
    source_sum(3)
    source_pass(0)
    net.wait("kC", cols.at[:, tc], C)
    net.wait("kF", cols.at[:, tyc], C)
    for h in range(1, hh):
        flat_near(h)
    source_pass(1)
    weight(0)
    source_pass(2)
    normed_term(0)
    source_end(0)
    for h in range(1, hh):
        weight(h)
    late = len(net.started) - 6
    for h in range(1, hh):
        normed_term(h)
    normed = PairScatter(p, lambda n: ng.at[n], ng1, ng2, ng3, *sems)
    normed.start()
    source_pass(3)
    normed.middle()
    source_end(1)
    raw_value, gain_value = raw[...].astype(F32), gain[...].astype(F32).reshape(1, model)
    inverse = lax.rsqrt(jnp.mean(raw_value * raw_value, axis=1, keepdims=True) + EPSILON)
    source_end(2)
    net.drain(late)
    scaled = normed.finish() * gain_value
    tgt_out[...] = inverse * scaled - raw_value * (inverse * inverse * inverse) * jnp.mean(
        scaled * raw_value, axis=1, keepdims=True
    )
    keep(tgt_out, tgt_h_out)
    source_end(3)
    for h in range(hh):
        net.wait(f"W{h}", ws.at[1 - v, h], V)
        keep(ws.at[1 - v, h], ws_h.at[1 - v, h])
    net.drain()
    for copy in kept:
        copy.wait()


def finish_kernel(ws, src_in, tgt_in, weight_out, src_out, tgt_out):
    parts, hh = ws.shape[0], ws.shape[1]
    for k in range(parts):
        for h in range(hh):
            n = (k * hh + h) * HEAD_DIM
            weight_out[:, n : n + HEAD_DIM] = ws[k, h].astype(F32)
    quarters, mq = src_in.shape[0], src_in.shape[2]
    for n in range(quarters):
        src_out[:, n * mq : (n + 1) * mq] = src_in[n]
    tgt_out[...] = tgt_in[...]


def grid_body(
    target_rows, source_rows, norm_gain, query_weight, key_weight, value_weight, output_weight,
    saved_output, norm_offset, output_grad
):
    tp, sp = lax.axis_size("tp"), lax.axis_size("sp")
    model, width = query_weight.shape
    heads = width // HEAD_DIM
    hh, half = heads // 2, width // 2
    rows, srows = target_rows.shape[0], source_rows.shape[0]
    block, sblock, sw = rows * tp, srows * tp, model // sp
    Y = tp // 2
    dma, vm = pltpu.SemaphoreType.DMA, pltpu.VMEM
    whole = pl.BlockSpec(memory_space=pl.ANY)
    quarters = len(Y_FIRST)
    mq = model // quarters
    ws, source_grad, target_grad = pl.pallas_call(
        functools.partial(grid_kernel, sp, tp, math.log(sblock * sp)),
        out_shape=[
            jax.ShapeDtypeStruct((2, hh, sw, HEAD_DIM), BF),
            jax.ShapeDtypeStruct((quarters, srows, mq), F32),
            jax.ShapeDtypeStruct((rows, model), F32),
        ],
        in_specs=[whole] * 10,
        out_specs=[whole] * 3,
        scratch_shapes=[vm((rows, model), BF), vm((model,), BF), vm((block, width), BF), vm((heads, block), BF)]
        + [vm((2, hh, sw, HEAD_DIM), BF), vm((quarters, srows, mq), F32), vm((rows, model), F32)]
        + [vm((tp, rows, model), BF)] * 2
        + [vm((2, tp, srows, model), BF)]
        + [vm((2, 2, rows, 2 * sw), BF), vm((sp, tp, rows, 2 * sw), BF)]
        + [vm((2, block, half), BF)] * 2
        + [vm((2, 16, 2 * block), BF)]
        + [vm((2, 2, 2, block, half), BF)] * 2
        + [vm((2, 2, 2, 16, 2 * block), BF)]
        + [vm((model, width), BF)] * 2
        + [vm((width, model), BF)]
        + [vm((2 * sblock, width), BF)]
        + [vm((hh, 2 * sblock, 4 * block), BF)] * 2
        + [vm((2, 2, hh, 2, block, HEAD_DIM), BF)]
        + [vm((2, hh, 2, block, HEAD_DIM), BF)] * 3
        + [vm((2, 2, hh, 2, block, HEAD_DIM), BF)]
        + [vm((2, hh, block, HEAD_DIM), BF)]
        + [vm((2 * sblock, width), F32), vm((2 * sblock, width), BF)]
        + [vm((quarters, 4, 2, srows, mq), BF)]
        + [vm((quarters, 4, srows, mq), BF)] * 2
        + [vm((quarters, 2, srows, mq), BF)]
        + [vm((quarters, srows, mq), BF)] * 2
        + [vm((block, model), F32)]
        + [vm((tp, rows, model), BF)]
        + [vm((Y, rows, model), BF)] * 3
        + [vm((hh, 2, sw, HEAD_DIM), BF)]
        + [dma((10,)), dma((quarters + 2 * hh + 1,)), dma((TRANSFERS,)), dma((TRANSFERS,))]
        + [dma((Y,))] * 4,
        name="grid_kernel",
        compiler_params=pltpu.CompilerParams(
            collective_id=1, has_side_effects=True, vmem_limit_bytes=58 * 2**20
        ),
    )(
        target_rows, output_grad, source_rows, norm_gain, saved_output, norm_offset.T,
        query_weight, key_weight, value_weight, output_weight,
    )
    weight_grad, source_grad, target_grad = pl.pallas_call(
        finish_kernel,
        out_shape=[
            jax.ShapeDtypeStruct((sw, width), F32),
            jax.ShapeDtypeStruct((srows, model), F32),
            jax.ShapeDtypeStruct((rows, model), F32),
        ],
        in_specs=[VMEM] * 3,
        out_specs=[VMEM] * 3,
        name="finish_kernel",
    )(ws, source_grad, target_grad)
    return (target_grad, source_grad, weight_grad)


def on_grid(target_rows, query_weight):
    pairs = (lax.axis_size("sp"), lax.axis_size("tp")) == (2**3, 2**2)
    heads = query_weight.shape[1] // HEAD_DIM
    return pairs and heads % 2 == 0 and 2 * target_rows.shape[0] * lax.axis_size("tp") % 128 == 0


def layer(*args):
    return (grid_body if on_grid(args[0], args[3]) else body)(*args)


def solution(mesh):
    in_specs = (
        P(("sp", "tp"), None),
        P(("sp", "tp"), None),
        P(),
        P(None, "tp"),
        P(None, "tp"),
        P(None, "tp"),
        P("tp", None),
        P("sp", "tp"),
        P("sp", "tp"),
        P(("sp", "tp"), None),
    )
    out_specs = (P(("sp", "tp"), None), P(("sp", "tp"), None), P("sp", "tp"))
    return jax.shard_map(layer, mesh=mesh, in_specs=in_specs, out_specs=out_specs, check_vma=False)
```

```python
import functools
import math

import jax
import jax.numpy as jnp
from jax import lax
from jax.experimental import pallas as pl
from jax.experimental.pallas import tpu as pltpu
from jax.sharding import PartitionSpec as P

HEAD_DIM = 256
EPSILON = 1e-06
MESH = pl.DeviceIdType.MESH
BF = jnp.bfloat16
F32 = jnp.float32
VMEM = pl.BlockSpec(memory_space=pltpu.VMEM)


def contract_last(left, right):
    return lax.dot_general(left, right, (((1,), (1,)), ((), ())), preferred_element_type=F32)


def push(src, dst, send, recv, device):
    return pltpu.make_async_remote_copy(
        src_ref=src, dst_ref=dst, send_sem=send, recv_sem=recv, device_id=device, device_id_type=MESH
    )


def greet(devices):
    barrier = pltpu.get_barrier_semaphore()
    for device in devices:
        pl.semaphore_signal(barrier, inc=1, device_id=device, device_id_type=MESH)
    pl.semaphore_wait(barrier, len(devices))


class Place:
    def __init__(self, sp, tp):
        self.sp, self.tp, self.Z, self.Y = sp, tp, sp // 2, tp // 2
        self.s, self.t = lax.axis_index("sp"), lax.axis_index("tp")
        self.z, self.x = self.s // 2, self.s % 2
        self.y, self.c = self.t // 2, self.t % 2
        self.partner = (self.s, self.y * 2 + 1 - self.c)
        self.across = (self.z * 2 + 1 - self.x, self.t)

    def chip_y(self, d):
        return (self.s, lax.rem(self.y + d + self.Y, self.Y) * 2 + self.c)

    def chip_z(self, d):
        return (lax.rem(self.z + d + self.Z, self.Z) * 2 + self.x, self.t)


class LineGather:
    def __init__(self, place, pairs, up_s, up_r, dn_s, dn_r, x_s, x_r):
        self.p, self.pairs = place, pairs
        self.sems = (up_s, up_r, dn_s, dn_r, x_s, x_r)

    def up(self, n, d, own=False):
        p, (own_ref, all_ref) = self.p, self.pairs[n]
        block = p.s - 2 * (d - 1)
        src = own_ref if own else all_ref.at[block]
        return push(src, all_ref.at[block], self.sems[0].at[n, d], self.sems[1].at[n, d], (p.s + 2, p.t))

    def up_wait(self, n, d):
        p, (_, all_ref) = self.p, self.pairs[n]
        ref = all_ref.at[p.s - 2 * d]
        return push(ref, ref, self.sems[0].at[n, d], self.sems[1].at[n, d], (p.s - 2, p.t))

    def dn(self, n, d, own=False):
        p, (own_ref, all_ref) = self.p, self.pairs[n]
        block = p.s + 2 * (d - 1)
        src = own_ref if own else all_ref.at[block]
        return push(src, all_ref.at[block], self.sems[2].at[n, d], self.sems[3].at[n, d], (p.s - 2, p.t))

    def dn_wait(self, n, d):
        p, (_, all_ref) = self.p, self.pairs[n]
        ref = all_ref.at[p.s + 2 * d]
        return push(ref, ref, self.sems[2].at[n, d], self.sems[3].at[n, d], (p.s + 2, p.t))

    def over(self, n, d):
        p, (own_ref, all_ref) = self.p, self.pairs[n]
        block = p.s - 2 * d
        k = d + p.Z - 1
        src = own_ref if d == 0 else all_ref.at[block]
        return push(src, all_ref.at[block], self.sems[4].at[n, k], self.sems[5].at[n, k], p.across)

    def over_wait(self, n, d):
        p, (_, all_ref) = self.p, self.pairs[n]
        ref = all_ref.at[p.z * 2 + 1 - p.x - 2 * d]
        k = d + p.Z - 1
        return push(ref, ref, self.sems[4].at[n, k], self.sems[5].at[n, k], p.across)

    def start(self, count):
        p = self.p

        @pl.when(p.z + 1 < p.Z)
        def _():
            for n in count:
                self.up(n, 1, True).start()

        @pl.when(p.z >= 1)
        def _():
            for n in count:
                self.dn(n, 1, True).start()

        for n in count:
            self.over(n, 0).start()

    def step(self, d):
        p = self.p
        for n in range(len(self.pairs)):

            @pl.when(p.z - d >= 0)
            def _():
                self.up_wait(n, d).wait_recv()

                @pl.when(p.z + 1 < p.Z)
                def _():
                    self.up(n, d + 1).start()

                self.over(n, d).start()

            @pl.when(p.z + d < p.Z)
            def _():
                self.dn_wait(n, d).wait_recv()

                @pl.when(p.z >= 1)
                def _():
                    self.dn(n, d + 1).start()

                self.over(n, -d).start()

    def arrive(self, sign, d):
        for n in range(len(self.pairs)):
            self.over_wait(n, sign * d).wait_recv()

    def side(self, sign, d):
        return self.p.z - d >= 0 if sign > 0 else self.p.z + d < self.p.Z

    def finish(self):
        p = self.p
        for n in range(len(self.pairs)):
            for d in range(p.Z):
                for sign in (1, -1) if d else (1,):

                    @pl.when(self.side(sign, d))
                    def _():
                        self.over(n, sign * d).wait_send()

            for d in range(1, p.Z):

                @pl.when(jnp.logical_and(p.z - d + 1 >= 0, p.z + 1 < p.Z))
                def _():
                    self.up(n, d).wait_send()

                @pl.when(jnp.logical_and(p.z + d - 1 < p.Z, p.z >= 1))
                def _():
                    self.dn(n, d).wait_send()


def line_sems(p_z, n):
    return [pltpu.SemaphoreType.DMA((n, p_z + 1))] * 4 + [pltpu.SemaphoreType.DMA((n, 2 * p_z))] * 2


class PairScatter:
    def __init__(self, p, part, first, summed, second, fs, fr, ss, sr):
        self.p, self.part, self.first, self.summed, self.second = p, part, first, summed, second
        self.sems = (fs, fr, ss, sr)
        self.started = []

    def start(self):
        p = self.p
        for d in range(p.Y):
            y = lax.rem(p.y + d, p.Y)
            copy = push(
                self.part(y * 2 + 1 - p.c), self.first.at[d], self.sems[0].at[d], self.sems[1].at[d], p.partner
            )
            copy.start()
            self.started.append(copy)

    def middle(self):
        p = self.p
        for d in list(range(1, p.Y)) + [0]:
            y = lax.rem(p.y + d, p.Y)
            self.started[d].wait_recv()
            total = self.part(y * 2 + p.c)[...].astype(F32) + self.first[d].astype(F32)
            self.summed[d] = total.astype(BF)
            if d:
                copy = push(
                    self.summed.at[d], self.second.at[d], self.sems[2].at[d], self.sems[3].at[d], p.chip_y(d)
                )
                copy.start()
                self.started.append(copy)

    def finish(self):
        p = self.p
        total = self.part(p.t)[...].astype(F32) + self.first[0].astype(F32)
        for d in range(1, p.Y):
            self.started[p.Y + d - 1].wait_recv()
            total = total + self.second[d].astype(F32)
        for copy in self.started:
            copy.wait_send()
        return total


class PairGather:
    def __init__(self, p, own, spot, ys, yr, ps, pr):
        self.p, self.own, self.spot, self.sems = p, own, spot, (ys, yr, ps, pr)
        self.started = []

    def start(self):
        p = self.p
        for d in range(1, p.Y):
            copy = push(self.own, self.spot(p.t), self.sems[0].at[d], self.sems[1].at[d], p.chip_y(d))
            copy.start()
            self.started.append(copy)
        copy = push(self.own, self.spot(p.t), self.sems[2].at[0], self.sems[3].at[0], p.partner)
        copy.start()
        self.started.append(copy)

    def forward(self):
        p = self.p
        for d in range(1, p.Y):
            ref = self.spot(lax.rem(p.y - d + p.Y, p.Y) * 2 + p.c)
            push(ref, ref, self.sems[0].at[d], self.sems[1].at[d], p.chip_y(-d)).wait_recv()
            copy = push(ref, ref, self.sems[2].at[d], self.sems[3].at[d], p.partner)
            copy.start()
            self.started.append(copy)

    def arrive(self):
        p = self.p
        for d in range(p.Y):
            ref = self.spot(lax.rem(p.y - d + p.Y, p.Y) * 2 + 1 - p.c)
            push(ref, ref, self.sems[2].at[d], self.sems[3].at[d], p.partner).wait_recv()

    def finish(self):
        for copy in self.started:
            copy.wait_send()


def layer_kernel(
    sp, tp, shift_base,
    raw, to, src, gain, saved, offs, wq_h, wk_h, wv_h, wo_h,
    flat_all, src_out, tgt_out, cols_all,
    tn, pieces, wq, wk, wv, wo, tn_all, to_all, src_all, cols, tn_b, to_b,
    q_all, hg_all, small_all, k_s, v_s, p_s, d_s, part, kf, vf, sg,
    xr, xz, zr, sg1, sg2, sg3, ng, ng1, ng2, ng3,
    wsem, loc, es, er, *sems
):
    p = Place(sp, tp)
    pair_sems = [sems[4 * i : 4 * i + 4] for i in range(6)]
    xs_s, xs_r, zs_s, zs_r = sems[24:28]
    line_a, line_b = sems[28:34], sems[34:40]
    rows, block = raw.shape[0], saved.shape[0]
    width, model = wq.shape[1], wq.shape[0]
    heads = width // HEAD_DIM
    scale = HEAD_DIM ** (-0.5)
    loads = [
        pltpu.make_async_copy(h, v, wsem.at[i])
        for i, (h, v) in enumerate(((wq_h, wq), (wo_h, wo), (wk_h, wk), (wv_h, wv)))
    ]
    for copy in loads:
        copy.start()
    raw_value, gain_value = raw[...].astype(F32), gain[...].astype(F32).reshape(1, model)
    inverse = lax.rsqrt(jnp.mean(raw_value * raw_value, axis=1, keepdims=True) + EPSILON)
    normed_value = (raw_value * inverse * gain_value).astype(BF)
    tn[...] = normed_value
    slice_width = model // sp
    for s in range(sp):
        pieces[s] = normed_value[:, s * slice_width : (s + 1) * slice_width]
    greet(
        [p.partner]
        + [p.chip_y(d) for d in range(1, p.Y)]
        + [(lax.rem(p.s + e, sp), p.t) for e in range(1, sp)]
    )
    g_tn = PairGather(p, tn, lambda t: tn_all.at[t], *pair_sems[0])
    g_to = PairGather(p, to, lambda t: to_all.at[t], *pair_sems[1])
    g_src = PairGather(p, src, lambda t: src_all.at[t], *pair_sems[2])
    g_cols = PairGather(p, cols, lambda t: cols_all.at[:, t], *pair_sems[3])
    for g in (g_tn, g_to, g_src):
        g.start()
    swaps = []
    for e in range(1, sp):
        s = lax.rem(p.s + e, sp)
        copy = push(pieces.at[s], cols.at[p.s], es.at[e], er.at[e], (s, p.t))
        copy.start()
        swaps.append(copy)
    mine = [
        pltpu.make_async_copy(tn, tn_all.at[p.t], loc.at[0]),
        pltpu.make_async_copy(to, to_all.at[p.t], loc.at[1]),
        pltpu.make_async_copy(src, src_all.at[p.t], loc.at[2]),
        pltpu.make_async_copy(pieces.at[p.s], cols.at[p.s], loc.at[3]),
    ]
    for copy in mine:
        copy.start()
    for copy in mine:
        copy.wait()
    tile = min(width, 256)
    gather = LineGather(
        p, ((q_all.at[p.s], q_all), (hg_all.at[p.s], hg_all), (small_all.at[p.s], small_all)), *line_a
    )

    g_tn.forward()
    g_to.forward()
    g_tn.arrive()
    for t in range(tp):
        tn_b[t * rows : (t + 1) * rows, :] = tn_all[t]
    loads[0].wait()
    for j in range(0, width, tile):
        q_all[p.s, :, j : j + tile] = jnp.dot(
            tn_b[...], wq[:, j : j + tile], preferred_element_type=F32
        ).astype(BF)
    gather.start((0,))
    g_to.arrive()
    for t in range(tp):
        to_b[t * rows : (t + 1) * rows, :] = to_all[t]
    loads[1].wait()
    lane = lax.broadcasted_iota(jnp.int32, (block, 128), 1)
    pick = lax.broadcasted_iota(jnp.int32, (heads, 128), 0) == lax.broadcasted_iota(jnp.int32, (heads, 128), 1)
    small = lax.dot_general(
        offs[...].astype(F32), pick.astype(F32), (((0,), (0,)), ((), ())), precision=lax.Precision.HIGHEST,
        preferred_element_type=F32,
    )
    for h in range(heads):
        cut = slice(h * HEAD_DIM, (h + 1) * HEAD_DIM)
        part_h = contract_last(to_b[...], wo[cut, :]).astype(BF)
        hg_all[p.s, :, cut] = part_h
        delta = jnp.sum(part_h.astype(F32) * saved[:, cut].astype(F32), axis=1, keepdims=True)
        small = jnp.where(lane == heads + h, delta, small)
    small_all[p.s] = small.astype(BF)
    gather.start((1, 2))

    g_src.forward()
    g_src.arrive()
    gather.step(1)
    source_count = k_s.shape[0]
    loads[2].wait()
    loads[3].wait()

    @pl.loop(0, width // tile)
    def _(j):
        cut = pl.ds(pl.multiple_of(j * tile, tile), tile)
        rows_value = src_all[...].reshape(source_count, model)
        k_s[:, cut] = jnp.dot(rows_value, wk[:, cut], preferred_element_type=F32).astype(BF)
        v_s[:, cut] = jnp.dot(rows_value, wv[:, cut], preferred_element_type=F32).astype(BF)

    for e in range(1, sp):
        s = lax.rem(p.s - e + sp, sp)
        push(cols.at[s], cols.at[s], es.at[e], er.at[e], (s, p.t)).wait_recv()
    g_cols.start()
    keep = pltpu.make_async_copy(cols, cols_all.at[:, p.t], loc.at[4])
    keep.start()

    def into(k):
        z = lax.rem(p.z + k, p.Z)
        return push(part.at[z * 2 + 1 - p.x], xr.at[k], xs_s.at[k], xs_r.at[k], p.across)

    def attend(z):
        pair = pl.ds(2 * z, 2)
        spot = pl.ds(pl.multiple_of(z * (2 * block), 2 * block), 2 * block)
        tiny = small_all[pair].reshape(2 * block, 128).astype(F32)
        for h in range(heads):
            cut = slice(h * HEAD_DIM, (h + 1) * HEAD_DIM)
            q_h = q_all[pair, :, cut].reshape(2 * block, HEAD_DIM)
            g_h = hg_all[pair, :, cut].reshape(2 * block, HEAD_DIM)
            prob = jnp.exp(contract_last(q_h, k_s[:, cut]) * scale - (shift_base + tiny[:, h : h + 1]))
            grad = contract_last(g_h, v_s[:, cut])
            score = (prob * (grad - tiny[:, heads + h : heads + h + 1]) * scale).astype(BF)
            p_s[h, spot, :] = prob.astype(BF)
            d_s[h, spot, :] = score
            term = jnp.dot(score, k_s[:, cut], preferred_element_type=F32).astype(BF)
            part[pair, :, cut] = term.reshape(2, block, HEAD_DIM)

    def reached(sign, d):
        gather.arrive(sign, d)
        attend(p.z - sign * d)
        into((-sign * d) % p.Z).start()

    for d in range(1, p.Z):
        if d > 1:
            gather.step(d)
        for sign in (1, -1) if d > 1 else (1,):

            @pl.when(gather.side(sign, d - 1))
            def _():
                reached(sign, d - 1)

        if d == 1:
            g_cols.forward()
    for sign in (1, -1):

        @pl.when(gather.side(sign, p.Z - 1))
        def _():
            reached(sign, p.Z - 1)

    order = sorted(range(1, p.Z), key=lambda k: min(k, p.Z - k))
    hops = {}

    def relay(k):
        into(k).wait_recv()
        z = lax.rem(p.z + k, p.Z)
        xz[k] = (part[z * 2 + p.x].astype(F32) + xr[k].astype(F32)).astype(BF)
        hops[k] = push(xz.at[k], zr.at[k], zs_s.at[k], zs_r.at[k], p.chip_z(k))
        hops[k].start()

    for k in order[:1]:
        relay(k)
    count = sp * block

    for h in range(heads):
        cut = slice(h * HEAD_DIM, (h + 1) * HEAD_DIM)
        dims = (((0,), (0,)), ((), ()))
        q_h = q_all[:, :, cut].reshape(count, HEAD_DIM)
        g_h = hg_all[:, :, cut].reshape(count, HEAD_DIM)
        kf[:, cut] = lax.dot_general(d_s[h], q_h, dims, preferred_element_type=F32).astype(BF)
        vf[:, cut] = lax.dot_general(p_s[h], g_h, dims, preferred_element_type=F32).astype(BF)
    for k in order[1:2]:
        relay(k)
    stile = min(model, 256)

    def source_term(j):
        cut = pl.ds(pl.multiple_of(j * stile, stile), stile)
        value = contract_last(kf[...], wk[cut, :]) + contract_last(vf[...], wv[cut, :])
        sg[:, :, cut] = value.astype(BF).reshape(tp, source_count // tp, stile)

    half = model // stile // 2
    pl.loop(0, half)(source_term)
    for k in order[2:]:
        relay(k)
    pl.loop(half, model // stile)(source_term)
    source = PairScatter(p, lambda t: sg.at[t], sg1, sg2, sg3, *pair_sems[4])
    source.start()
    source.middle()
    into(0).wait_recv()
    total = part[p.s].astype(F32) + xr[0].astype(F32)
    for k in order:
        hops[k].wait_recv()
        total = total + zr[k].astype(F32)
    flat = total.astype(BF)
    flat_all[p.s] = flat
    spread = LineGather(p, ((flat_all.at[p.s], flat_all),), *line_b)
    spread.start((0,))
    for j in range(0, model, stile):
        columns = contract_last(flat, wq[j : j + stile, :]).astype(BF)
        for t in range(tp):
            ng[t, :, j : j + stile] = columns[t * rows : (t + 1) * rows]
    normed = PairScatter(p, lambda t: ng.at[t], ng1, ng2, ng3, *pair_sems[5])
    normed.start()
    for d in range(1, p.Z):
        spread.step(d)
        if d == 1:
            normed.middle()
    src_out[...] = source.finish()
    raw_value, gain_value = raw[...].astype(F32), gain[...].astype(F32).reshape(1, model)
    inverse = lax.rsqrt(jnp.mean(raw_value * raw_value, axis=1, keepdims=True) + EPSILON)
    scaled = normed.finish() * gain_value
    tgt_out[...] = inverse * scaled - raw_value * (inverse * inverse * inverse) * jnp.mean(
        scaled * raw_value, axis=1, keepdims=True
    )
    g_cols.arrive()
    for d in range(p.Z):
        for sign in (1, -1) if d else (1,):

            @pl.when(spread.side(sign, d))
            def _():
                spread.arrive(sign, d)

    gather.finish()
    spread.finish()
    for g in (g_tn, g_to, g_src, g_cols):
        g.finish()
    for copy in swaps:
        copy.wait_send()
    keep.wait()
    for k in range(p.Z):
        into(k).wait_send()
    for k in order:
        hops[k].wait_send()


def body(
    target_rows,
    source_rows,
    norm_gain,
    query_weight,
    key_weight,
    value_weight,
    output_weight,
    saved_output,
    norm_offset,
    output_grad,
):
    tp, sp = lax.axis_size("tp"), lax.axis_size("sp")
    Z, Y = sp // 2, tp // 2
    model, width = query_weight.shape
    heads = width // HEAD_DIM
    rows, srows = target_rows.shape[0], source_rows.shape[0]
    block = rows * tp
    count = block * sp
    source_count = srows * tp
    shift_base = math.log(source_count * sp)
    slice_width = model // sp
    dma = pltpu.SemaphoreType.DMA

    vm = pltpu.VMEM
    whole = pl.BlockSpec(memory_space=pl.ANY)
    flat_all, source_grad, target_grad, cols_all = pl.pallas_call(
        functools.partial(layer_kernel, sp, tp, shift_base),
        out_shape=[
            jax.ShapeDtypeStruct((sp, block, width), BF),
            jax.ShapeDtypeStruct((srows, model), F32),
            jax.ShapeDtypeStruct((rows, model), F32),
            jax.ShapeDtypeStruct((sp, tp, rows, slice_width), BF),
        ],
        in_specs=[VMEM] * 6 + [whole] * 4,
        out_specs=[VMEM] * 4,
        scratch_shapes=[vm((rows, model), BF), vm((sp, rows, slice_width), BF)]
        + [vm((model, width), BF)] * 3
        + [vm((width, model), BF)]
        + [vm((tp, rows, model), BF)] * 2
        + [vm((tp, srows, model), BF), vm((sp, rows, slice_width), BF)]
        + [vm((block, model), BF)] * 2
        + [vm((sp, block, width), BF)] * 2
        + [vm((sp, block, 128), BF)]
        + [vm((source_count, width), BF)] * 2
        + [vm((heads, count, source_count), BF)] * 2
        + [vm((sp, block, width), BF)]
        + [vm((source_count, width), BF)] * 2
        + [vm((tp, srows, model), BF)]
        + [vm((Z, block, width), BF)] * 3
        + [vm((Y, srows, model), BF)] * 3
        + [vm((tp, rows, model), BF)]
        + [vm((Y, rows, model), BF)] * 3
        + [dma((4,)), dma((5,)), dma((sp,)), dma((sp,))]
        + [dma((Y,))] * 24
        + [dma((Z,))] * 4
        + line_sems(Z, 3)
        + line_sems(Z, 1),
        name="layer_kernel",
        compiler_params=pltpu.CompilerParams(
            collective_id=1, has_side_effects=True, vmem_limit_bytes=58 * 2**20
        ),
    )(
        target_rows,
        output_grad,
        source_rows,
        norm_gain,
        saved_output,
        norm_offset.T,
        query_weight,
        key_weight,
        value_weight,
        output_weight,
    )
    weight_grad = lax.dot_general(
        cols_all.reshape(count, slice_width),
        flat_all.reshape(count, width),
        (((0,), (0,)), ((), ())),
        preferred_element_type=F32,
    )
    return (target_grad, source_grad, weight_grad)


class Net:
    def __init__(self, send, recv):
        self.send, self.recv, self.ids = send, recv, {}
        self.free, self.started = list(range(send.shape[0])), []

    def _copy(self, name, src, dst, device, slot=0):
        n = self.ids.setdefault(name, len(self.ids))
        return push(src, dst, self.send.at[slot], self.recv.at[n], device)

    def go(self, name, src, dst, device):
        if not self.free:
            self.drain(1)
        slot = self.free.pop(0)
        copy = self._copy(name, src, dst, device, slot)
        copy.start()
        self.started.append((slot, copy))

    def same(self, name, ref, device):
        self.go(name, ref, ref, device)

    def wait(self, name, landed, device):
        self._copy(name, landed, landed, device).wait_recv()

    def drain(self, count=None):
        count = len(self.started) if count is None else count
        for slot, copy in self.started[:count]:
            copy.wait_send()
            self.free.append(slot)
        self.started = self.started[count:]


SENDS = 28
Y_FIRST = (False, True, True, True)


def grid_kernel(
    sp, tp, shift_base,
    raw_h, to_h, src_h, gain_h, saved_h, offs_h, wq_h, wk_h, wv_h, wo_h,
    ws_h, src_h_out, tgt_h_out,
    raw, gain, saved, offs, ws, src_out, tgt_out,
    tn_all, to_all, src_all, pieces, cols, q_st, g_st, sm_st, q_all, g_all, sm_all,
    wq, wkv, wo, kv, p_s, d_s, part, xr, xs, ur, flat_all, fl, kv_sum, kvf,
    sg, sd, ss, es, fs, fr, na, ng, ng1, ng2, ng3, wt,
    wsem, osem, send, recv, *sems
):
    p = Place(sp, tp)
    s, t, y, c, x = p.s, p.t, p.y, p.c, p.x
    u, v = p.z // 2, p.z % 2
    net = Net(send, recv)

    def at(u, v, x):
        return ((u * 2 + v) * 2 + x, t)

    C, Y, V, X, U = p.partner, p.chip_y(1), at(u, 1 - v, x), at(u, v, 1 - x), at(1 - u, v, x)
    ty, tc, tyc = (1 - y) * 2 + c, y * 2 + 1 - c, (1 - y) * 2 + 1 - c
    others = [
        (a, b, d, u + a - 2 * u * a, v + b - 2 * v * b, x + d - 2 * x * d)
        for a in range(2) for b in range(2) for d in range(2) if a + b + d
    ]
    barrier = pltpu.get_barrier_semaphore()
    friends = [C, Y] + [at(*o[3:]) for o in others]
    for device in friends:
        pl.semaphore_signal(barrier, inc=1, device_id=device, device_id_type=MESH)
    rows, block, srows = raw.shape[0], saved.shape[0], src_h.shape[0]
    model, width = wq.shape
    heads = width // HEAD_DIM
    hh, half = heads // 2, width // 2
    sblock = srows * tp
    sw = model // sp
    quarters = len(Y_FIRST)
    mq = model // quarters
    scale = HEAD_DIM ** (-0.5)
    mine = pl.ds(pl.multiple_of(v * half, half), half)
    loads = [
        pltpu.make_async_copy(h, w, wsem.at[i])
        for i, (h, w) in enumerate(
            (
                (wq_h, wq), (wo_h, wo), (wk_h.at[:, mine], wkv.at[:, :half]), (wv_h.at[:, mine], wkv.at[:, half:]),
                (raw_h, raw), (gain_h, gain), (src_h, src_all.at[v, t]), (to_h, to_all.at[t]),
                (saved_h, saved), (offs_h, offs),
            )
        )
    ]
    for n in (4, 5, 6, 7, 0, 1, 8, 9, 2, 3):
        loads[n].start()
    loads[4].wait()
    loads[5].wait()
    raw_value, gain_value = raw[...].astype(F32), gain[...].astype(F32).reshape(1, model)
    inverse = lax.rsqrt(jnp.mean(raw_value * raw_value, axis=1, keepdims=True) + EPSILON)
    normed_value = (raw_value * inverse * gain_value).astype(BF)
    tn_all[t] = normed_value
    for a in range(2):
        for b in range(2):
            for k in range(2):
                n = (2 * a + k) * 2 + b
                pieces[a, b, :, k * sw : (k + 1) * sw] = normed_value[:, n * sw : (n + 1) * sw]
    loads[6].wait()
    loads[7].wait()
    pl.semaphore_wait(barrier, len(friends))
    A, B = pl.ds(0, srows // 2), pl.ds(srows // 2, srows // 2)

    net.same("tnY", tn_all.at[t], Y)
    net.same("sVB", src_all.at[v, t, B], V)
    net.same("tnC", tn_all.at[t], C)
    net.same("toY", to_all.at[t], Y)
    net.same("toC", to_all.at[t], C)
    net.same("sYA", src_all.at[v, t, A], Y)
    net.same("sVA", src_all.at[v, t, A], V)
    net.same("sYB", src_all.at[v, t, B], Y)
    net.same("sC", src_all.at[v, t], C)
    net.wait("tnY", tn_all.at[ty], Y)
    net.same("tnF", tn_all.at[ty], C)
    net.wait("toY", to_all.at[ty], Y)
    net.same("toF", to_all.at[ty], C)
    net.wait("tnC", tn_all.at[tc], C)
    net.wait("tnF", tn_all.at[tyc], C)
    loads[0].wait()
    tn_b = tn_all[...].reshape(block, model)
    for k in range(2):
        for j in range(0, half, HEAD_DIM):
            q_st[k, :, j : j + HEAD_DIM] = jnp.dot(
                tn_b, wq[:, k * half + j : k * half + j + HEAD_DIM], preferred_element_type=F32
            ).astype(BF)
    net.go("qV", q_st.at[1 - v], q_all.at[u, x, v], V)
    q_all[u, x, v] = q_st[v]
    net.same("q0U", q_all.at[u, x, v], U)
    net.same("q0X", q_all.at[u, x, v], X)
    net.wait("sVB", src_all.at[1 - v, t, B], V)
    net.same("fVB", src_all.at[1 - v, t, B], Y)
    net.same("cVB", src_all.at[1 - v, t, B], C)
    net.wait("toC", to_all.at[tc], C)
    net.wait("toF", to_all.at[tyc], C)
    loads[1].wait()
    loads[8].wait()
    loads[9].wait()
    to_b = to_all[...].reshape(block, model)
    products = []
    for n in range(heads):
        cut = slice(n * HEAD_DIM, (n + 1) * HEAD_DIM)
        part_h = contract_last(to_b, wo[cut, :]).astype(BF)
        g_st[n // hh, :, n % hh * HEAD_DIM : (n % hh + 1) * HEAD_DIM] = part_h
        products.append(part_h.astype(F32) * saved[:, cut].astype(F32))
    net.go("gV", g_st.at[1 - v], g_all.at[u, x, v], V)
    g_all[u, x, v] = g_st[v]
    net.same("g0U", g_all.at[u, x, v], U)
    net.same("g0X", g_all.at[u, x, v], X)
    lines, lanes = sm_st.shape[1], 2 * block
    place = (
        lax.broadcasted_iota(jnp.int32, (block, lanes), 1)
        == lax.broadcasted_iota(jnp.int32, (block, lanes), 0) + v * block
    ).astype(F32)
    spread = jnp.dot(offs[...].astype(F32), place, precision=lax.Precision.HIGHEST, preferred_element_type=F32)
    product = jnp.concatenate(products, axis=1)
    line = lax.broadcasted_iota(jnp.int32, (2 * lines, width), 0)
    head = lax.broadcasted_iota(jnp.int32, (2 * lines, width), 1) // HEAD_DIM
    pick = (line == head // hh * lines + hh + head % hh).astype(BF)
    deltas = 0.0
    for term in range(3):
        narrow = product.astype(BF)
        product = product - narrow.astype(F32)
        padded = jnp.concatenate(
            [jnp.where(v == 0, narrow, jnp.zeros_like(narrow)), jnp.where(v == 1, narrow, jnp.zeros_like(narrow))],
            axis=0,
        )
        deltas = deltas + contract_last(pick, padded)
    line = lax.broadcasted_iota(jnp.int32, (lines, lanes), 0)
    for k in range(2):
        small = deltas[k * lines : (k + 1) * lines]
        for h in range(hh):
            n = k * hh + h
            small = jnp.where(line == h, jnp.broadcast_to(spread[n : n + 1], small.shape), small)
        sm_st[k] = small.astype(BF)
    net.go("mV", sm_st.at[1 - v], sm_all.at[u, x, v], V)
    sm_all[u, x, v] = sm_st[v]
    net.same("m0U", sm_all.at[u, x, v], U)
    net.same("m0X", sm_all.at[u, x, v], X)

    net.wait("sYA", src_all.at[v, ty, A], Y)
    net.same("cYA", src_all.at[v, ty, A], C)
    net.wait("qV", q_all.at[u, x, 1 - v], V)
    net.same("q1U", q_all.at[u, x, 1 - v], U)
    net.same("q1X", q_all.at[u, x, 1 - v], X)
    net.wait("sVA", src_all.at[1 - v, t, A], V)
    net.same("fVA", src_all.at[1 - v, t, A], Y)
    net.same("cVA", src_all.at[1 - v, t, A], C)
    net.wait("gV", g_all.at[u, x, 1 - v], V)
    net.same("g1U", g_all.at[u, x, 1 - v], U)
    net.same("g1X", g_all.at[u, x, 1 - v], X)
    net.wait("sYB", src_all.at[v, ty, B], Y)
    net.same("cYB", src_all.at[v, ty, B], C)
    net.wait("mV", sm_all.at[u, x, 1 - v], V)
    net.same("m1U", sm_all.at[u, x, 1 - v], U)
    net.same("m1X", sm_all.at[u, x, 1 - v], X)
    def project(k, y):
        count = 2 * srows
        spot = pl.ds(pl.multiple_of(k * sblock + y * count, count), count)

        @pl.loop(0, 2)
        def _(j):
            cut = pl.ds(pl.multiple_of(j * half, half), half)
            value = src_all[k, pl.ds(2 * y, 2)].reshape(count, model)
            kv[spot, cut] = jnp.dot(value, wkv[:, cut], preferred_element_type=F32).astype(BF)

    net.wait("sC", src_all.at[v, tc], C)
    loads[2].wait()
    loads[3].wait()
    net.wait("fVB", src_all.at[1 - v, ty, B], Y)
    net.same("dVB", src_all.at[1 - v, ty, B], C)
    project(v, y)
    spot = (u * 2 + x) * 2 + v
    for a, b, d, u2, v2, x2 in others:
        net.go(f"p{a}{b}{d}", pieces.at[u2, x2], cols.at[spot, t], at(u2, v2, x2))
    cols[spot, t] = pieces[u, x]
    net.wait("q0U", q_all.at[1 - u, x, v], U)
    net.same("q2X", q_all.at[1 - u, x, v], X)
    net.wait("cVB", src_all.at[1 - v, tc, B], C)
    net.wait("cVA", src_all.at[1 - v, tc, A], C)
    project(1 - v, y)
    net.wait("cYA", src_all.at[v, tyc, A], C)
    net.wait("cYB", src_all.at[v, tyc, B], C)
    net.wait("g0U", g_all.at[1 - u, x, v], U)
    net.same("g2X", g_all.at[1 - u, x, v], X)
    project(v, 1 - y)
    net.wait("fVA", src_all.at[1 - v, ty, A], Y)
    net.same("dVA", src_all.at[1 - v, ty, A], C)
    net.wait("m0U", sm_all.at[1 - u, x, v], U)
    net.same("m2X", sm_all.at[1 - u, x, v], X)
    net.wait("q1U", q_all.at[1 - u, x, 1 - v], U)
    net.same("q3X", q_all.at[1 - u, x, 1 - v], X)
    net.wait("dVB", src_all.at[1 - v, tyc, B], C)
    net.wait("dVA", src_all.at[1 - v, tyc, A], C)
    project(1 - v, 1 - y)

    def attend(w, after):
        little = sm_all[w].astype(F32)
        little = jnp.concatenate([little[0, 0] + little[0, 1], little[1, 0] + little[1, 1]], axis=1)
        for h in range(hh):
            cut = slice(h * HEAD_DIM, (h + 1) * HEAD_DIM)
            q_h = q_all[w, :, :, :, cut].reshape(4 * block, HEAD_DIM)
            g_h = g_all[w, :, :, :, cut].reshape(4 * block, HEAD_DIM)
            prob = jnp.exp(contract_last(kv[:, cut], q_h) * scale - (shift_base + little[h : h + 1]))
            grad = contract_last(kv[:, half + h * HEAD_DIM : half + (h + 1) * HEAD_DIM], g_h)
            score = (prob * (grad - little[hh + h : hh + h + 1]) * scale).astype(BF)
            p_s[h] = prob.astype(BF)
            d_s[h] = score
            term = lax.dot_general(score, kv[:, cut], (((0,), (0,)), ((), ())), preferred_element_type=F32)
            part[w, :, h] = term.astype(BF).reshape(2, 2, block, HEAD_DIM)
            after(h)

    def source_terms(w):
        for h in range(hh):
            cut = slice(h * HEAD_DIM, (h + 1) * HEAD_DIM)
            q_h = q_all[w, :, :, :, cut].reshape(4 * block, HEAD_DIM)
            g_h = g_all[w, :, :, :, cut].reshape(4 * block, HEAD_DIM)
            yield cut, jnp.dot(d_s[h], q_h, preferred_element_type=F32)
            cut = slice(half + h * HEAD_DIM, half + (h + 1) * HEAD_DIM)
            yield cut, jnp.dot(p_s[h], g_h, preferred_element_type=F32)

    def send_near(h):
        net.go(f"a{h}X", part.at[u, 1 - x, h], xr.at[0, h], X)

    def send_far(h):
        for k in range(2):
            net.go(f"b{h}{k}X", part.at[1 - u, 1 - x, h, k], xr.at[1, h, k], X)

    for n, k in ((0, v), (1, 1 - v)):
        net.wait(f"q{n}X", q_all.at[u, 1 - x, k], X)
        net.wait(f"m{n}X", sm_all.at[u, 1 - x, k], X)
        net.wait(f"g{n}X", g_all.at[u, 1 - x, k], X)
    net.wait("g1U", g_all.at[1 - u, x, 1 - v], U)
    net.same("g3X", g_all.at[1 - u, x, 1 - v], X)
    net.wait("m1U", sm_all.at[1 - u, x, 1 - v], U)
    net.same("m3X", sm_all.at[1 - u, x, 1 - v], X)
    attend(u, send_near)
    for cut, value in source_terms(u):
        kv_sum[:, cut] = value

    def near(h):
        net.wait(f"a{h}X", xr.at[0, h], X)
        xs[0, h] = (part[u, x, h].astype(F32) + xr[0, h].astype(F32)).astype(BF)
        net.go(f"s{h}U", xs.at[0, h], ur.at[1, h], U)

    for n, k in ((2, v), (3, 1 - v)):
        net.wait(f"q{n}X", q_all.at[1 - u, 1 - x, k], X)
        net.wait(f"m{n}X", sm_all.at[1 - u, 1 - x, k], X)
        net.wait(f"g{n}X", g_all.at[1 - u, 1 - x, k], X)
    attend(1 - u, send_far)
    near(0)
    for cut, value in source_terms(1 - u):
        kvf[:, cut] = (kv_sum[:, cut] + value).astype(BF)
    for h in range(1, hh):
        near(h)
    for a, b, d, u2, v2, x2 in others:
        net.wait(f"p{a}{b}{d}", cols.at[(u2 * 2 + x2) * 2 + v2, t], at(u2, v2, x2))
    net.same("kY", cols.at[:, t], Y)
    net.same("kC", cols.at[:, t], C)
    stile = min(mq, 256)

    def source(n):
        for j in range(0, mq, stile):
            value = contract_last(kvf[...], wkv[n * mq + j : n * mq + j + stile, :]).astype(BF)
            sg[n, :, :, :, j : j + stile] = value.reshape(4, 2, srows, stile)
        net.go(f"d{n}", sg.at[n, :, 1 - c], sd.at[n], C)

    def source_sum(n):
        net.wait(f"d{n}", sd.at[n], C)
        for k in range(4):
            ss[n, k] = (sg[n, k, c].astype(F32) + sd[n, k].astype(F32)).astype(BF)
        net.go(f"e{n}1", ss.at[n, 2 * (1 - v) + 1 - y], es.at[n, 1], Y if Y_FIRST[n] else V)

    def source_rest(n):
        first, near = (Y, 2 * v + 1 - y) if Y_FIRST[n] else (V, 2 * (1 - v) + y)
        net.go(f"e{n}0", ss.at[n, near], es.at[n, 0], first)

    def source_pass(n):
        first, last = (Y, V) if Y_FIRST[n] else (V, Y)
        keep = 2 * (1 - v) + y if Y_FIRST[n] else 2 * v + 1 - y
        net.wait(f"e{n}1", es.at[n, 1], first)
        fs[n] = (ss[n, keep].astype(F32) + es[n, 1].astype(F32)).astype(BF)
        net.go(f"f{n}", fs.at[n], fr.at[n], last)

    kept = []

    def keep(ref, out):
        copy = pltpu.make_async_copy(ref, out, osem.at[len(kept)])
        copy.start()
        kept.append(copy)

    def source_end(n):
        first, last = (Y, V) if Y_FIRST[n] else (V, Y)
        net.wait(f"e{n}0", es.at[n, 0], first)
        net.wait(f"f{n}", fr.at[n], last)
        src_out[n] = ss[n, 2 * v + y].astype(F32) + es[n, 0].astype(F32) + fr[n].astype(F32)
        keep(src_out.at[n], src_h_out.at[n])

    def far(h):
        for k in range(2):
            net.wait(f"b{h}{k}X", xr.at[1, h, k], X)
            xs[1, h, k] = (part[1 - u, x, h, k].astype(F32) + xr[1, h, k].astype(F32)).astype(BF)
            net.go(f"z{h}{k}U", xs.at[1, h, k], ur.at[0, h, k], U)

    def flat_far(h):
        net.wait(f"s{h}U", ur.at[1, h], U)
        flat_all[1 - u, x, h] = (xs[1, h].astype(F32) + ur[1, h].astype(F32)).astype(BF)
        net.same(f"w{h}X", flat_all.at[1 - u, x, h], X)

    def flat_near(h):
        for k in range(2):
            net.wait(f"z{h}{k}U", ur.at[0, h, k], U)
            flat_all[u, x, h, k] = (xs[0, h, k].astype(F32) + ur[0, h, k].astype(F32)).astype(BF)
            net.same(f"r{h}{k}X", flat_all.at[u, x, h, k], X)
        net.go(f"n{h}V", flat_all.at[u, x, h, 1 - v], fl.at[v, h], V)
        fl[v, h] = flat_all[u, x, h, v]

    def weight(h):
        for k in range(2):
            net.wait(f"r{h}{k}X", flat_all.at[u, 1 - x, h, k], X)
        net.wait(f"w{h}X", flat_all.at[1 - u, 1 - x, h], X)
        flat_h = flat_all[:, :, h].reshape(sp * block, HEAD_DIM)
        for k in range(2):
            wt[h, k] = lax.dot_general(
                cols[:, :, :, k * sw : (k + 1) * sw].reshape(sp * block, sw), flat_h,
                (((0,), (0,)), ((), ())), preferred_element_type=F32,
            ).astype(BF)
        net.go(f"W{h}", wt.at[h, 1 - v], ws.at[v, h], V)
        ws[v, h] = wt[h, v]
        keep(ws.at[v, h], ws_h.at[v, h])

    ntile = min(model, 256)

    def normed_term(h, k, own):
        if not own:
            net.wait(f"n{h}V", fl.at[k, h], V)
        cut = pl.ds(pl.multiple_of((k * hh + h) * HEAD_DIM, HEAD_DIM), HEAD_DIM)
        for j in range(0, model, ntile):
            columns = contract_last(fl[k, h], wq[j : j + ntile, cut])
            if not own or h:
                columns = columns + na[:, j : j + ntile]
            if own or h < hh - 1:
                na[:, j : j + ntile] = columns
            else:
                ng[:, :, j : j + ntile] = columns.astype(BF).reshape(tp, rows, ntile)

    source(0)
    far(0)
    source(1)
    for h in range(1, hh):
        far(h)
    source(2)
    source_sum(0)
    source_rest(0)
    source(3)
    source_sum(1)
    source_sum(2)
    net.wait("kY", cols.at[:, ty], Y)
    net.same("kF", cols.at[:, ty], C)
    source_sum(3)
    for n in range(1, quarters):
        source_rest(n)
    for h in range(hh):
        flat_far(h)
    source_pass(1)
    source_pass(2)
    flat_near(0)
    normed_term(0, v, True)
    net.wait("kC", cols.at[:, tc], C)
    net.wait("kF", cols.at[:, tyc], C)
    for h in range(1, hh):
        flat_near(h)
        normed_term(h, v, True)
    source_pass(3)
    weight(0)
    source_pass(0)
    normed_term(0, 1 - v, False)
    for h in range(1, hh):
        weight(h)
    for h in range(1, hh):
        normed_term(h, 1 - v, False)
    normed = PairScatter(p, lambda n: ng.at[n], ng1, ng2, ng3, *sems)
    normed.start()
    source_end(0)
    source_end(1)
    normed.middle()
    source_end(2)
    raw_value, gain_value = raw[...].astype(F32), gain[...].astype(F32).reshape(1, model)
    inverse = lax.rsqrt(jnp.mean(raw_value * raw_value, axis=1, keepdims=True) + EPSILON)
    scaled = normed.finish() * gain_value
    tgt_out[...] = inverse * scaled - raw_value * (inverse * inverse * inverse) * jnp.mean(
        scaled * raw_value, axis=1, keepdims=True
    )
    keep(tgt_out, tgt_h_out)
    source_end(3)
    for h in range(hh):
        net.wait(f"W{h}", ws.at[1 - v, h], V)
        keep(ws.at[1 - v, h], ws_h.at[1 - v, h])
    net.drain()
    for copy in kept:
        copy.wait()


def finish_kernel(ws, src_in, tgt_in, weight_out, src_out, tgt_out):
    parts, hh = ws.shape[0], ws.shape[1]
    for k in range(parts):
        for h in range(hh):
            n = (k * hh + h) * HEAD_DIM
            weight_out[:, n : n + HEAD_DIM] = ws[k, h].astype(F32)
    quarters, mq = src_in.shape[0], src_in.shape[2]
    for n in range(quarters):
        src_out[:, n * mq : (n + 1) * mq] = src_in[n]
    tgt_out[...] = tgt_in[...]


def grid_body(
    target_rows, source_rows, norm_gain, query_weight, key_weight, value_weight, output_weight,
    saved_output, norm_offset, output_grad
):
    tp, sp = lax.axis_size("tp"), lax.axis_size("sp")
    model, width = query_weight.shape
    heads = width // HEAD_DIM
    hh, half = heads // 2, width // 2
    rows, srows = target_rows.shape[0], source_rows.shape[0]
    block, sblock, sw = rows * tp, srows * tp, model // sp
    Y = tp // 2
    dma, vm = pltpu.SemaphoreType.DMA, pltpu.VMEM
    whole = pl.BlockSpec(memory_space=pl.ANY)
    quarters = len(Y_FIRST)
    mq = model // quarters
    ws, source_grad, target_grad = pl.pallas_call(
        functools.partial(grid_kernel, sp, tp, math.log(sblock * sp)),
        out_shape=[
            jax.ShapeDtypeStruct((2, hh, sw, HEAD_DIM), BF),
            jax.ShapeDtypeStruct((quarters, srows, mq), F32),
            jax.ShapeDtypeStruct((rows, model), F32),
        ],
        in_specs=[whole] * 10,
        out_specs=[whole] * 3,
        scratch_shapes=[vm((rows, model), BF), vm((model,), BF), vm((block, width), BF), vm((heads, block), BF)]
        + [vm((2, hh, sw, HEAD_DIM), BF), vm((quarters, srows, mq), F32), vm((rows, model), F32)]
        + [vm((tp, rows, model), BF)] * 2
        + [vm((2, tp, srows, model), BF)]
        + [vm((2, 2, rows, 2 * sw), BF), vm((sp, tp, rows, 2 * sw), BF)]
        + [vm((2, block, half), BF)] * 2
        + [vm((2, 16, 2 * block), BF)]
        + [vm((2, 2, 2, block, half), BF)] * 2
        + [vm((2, 2, 2, 16, 2 * block), BF)]
        + [vm((model, width), BF)] * 2
        + [vm((width, model), BF)]
        + [vm((2 * sblock, width), BF)]
        + [vm((hh, 2 * sblock, 4 * block), BF)] * 2
        + [vm((2, 2, hh, 2, block, HEAD_DIM), BF)]
        + [vm((2, hh, 2, block, HEAD_DIM), BF)] * 3
        + [vm((2, 2, hh, 2, block, HEAD_DIM), BF)]
        + [vm((2, hh, block, HEAD_DIM), BF)]
        + [vm((2 * sblock, width), F32), vm((2 * sblock, width), BF)]
        + [vm((quarters, 4, 2, srows, mq), BF)]
        + [vm((quarters, 4, srows, mq), BF)] * 2
        + [vm((quarters, 2, srows, mq), BF)]
        + [vm((quarters, srows, mq), BF)] * 2
        + [vm((block, model), F32)]
        + [vm((tp, rows, model), BF)]
        + [vm((Y, rows, model), BF)] * 3
        + [vm((hh, 2, sw, HEAD_DIM), BF)]
        + [dma((10,)), dma((quarters + 2 * hh + 1,)), dma((SENDS,)), dma((66 + 11 * hh,))]
        + [dma((Y,))] * 4,
        name="grid_kernel",
        compiler_params=pltpu.CompilerParams(
            collective_id=1, has_side_effects=True, vmem_limit_bytes=58 * 2**20
        ),
    )(
        target_rows, output_grad, source_rows, norm_gain, saved_output, norm_offset.T,
        query_weight, key_weight, value_weight, output_weight,
    )
    weight_grad, source_grad, target_grad = pl.pallas_call(
        finish_kernel,
        out_shape=[
            jax.ShapeDtypeStruct((sw, width), F32),
            jax.ShapeDtypeStruct((srows, model), F32),
            jax.ShapeDtypeStruct((rows, model), F32),
        ],
        in_specs=[VMEM] * 3,
        out_specs=[VMEM] * 3,
        name="finish_kernel",
    )(ws, source_grad, target_grad)
    return (target_grad, source_grad, weight_grad)


def on_grid(target_rows, query_weight):
    pairs = (lax.axis_size("sp"), lax.axis_size("tp")) == (2**3, 2**2)
    heads = query_weight.shape[1] // HEAD_DIM
    return pairs and heads % 2 == 0 and 2 * target_rows.shape[0] * lax.axis_size("tp") % 128 == 0


def layer(*args):
    return (grid_body if on_grid(args[0], args[3]) else body)(*args)


def solution(mesh):
    in_specs = (
        P(("sp", "tp"), None),
        P(("sp", "tp"), None),
        P(),
        P(None, "tp"),
        P(None, "tp"),
        P(None, "tp"),
        P("tp", None),
        P("sp", "tp"),
        P("sp", "tp"),
        P(("sp", "tp"), None),
    )
    out_specs = (P(("sp", "tp"), None), P(("sp", "tp"), None), P("sp", "tp"))
    return jax.shard_map(layer, mesh=mesh, in_specs=in_specs, out_specs=out_specs, check_vma=False)
```

```python
import functools
import math

import jax
import jax.numpy as jnp
from jax import lax
from jax.experimental import pallas as pl
from jax.experimental.pallas import tpu as pltpu
from jax.sharding import PartitionSpec as P

HEAD_DIM = 256
EPSILON = 1e-06
MESH = pl.DeviceIdType.MESH
BF = jnp.bfloat16
F32 = jnp.float32
VMEM = pl.BlockSpec(memory_space=pltpu.VMEM)


def contract_last(left, right):
    return lax.dot_general(left, right, (((1,), (1,)), ((), ())), preferred_element_type=F32)


def push(src, dst, send, recv, device):
    return pltpu.make_async_remote_copy(
        src_ref=src, dst_ref=dst, send_sem=send, recv_sem=recv, device_id=device, device_id_type=MESH
    )


def greet(devices):
    barrier = pltpu.get_barrier_semaphore()
    for device in devices:
        pl.semaphore_signal(barrier, inc=1, device_id=device, device_id_type=MESH)
    pl.semaphore_wait(barrier, len(devices))


class Place:
    def __init__(self, sp, tp):
        self.sp, self.tp, self.Z, self.Y = sp, tp, sp // 2, tp // 2
        self.s, self.t = lax.axis_index("sp"), lax.axis_index("tp")
        self.z, self.x = self.s // 2, self.s % 2
        self.y, self.c = self.t // 2, self.t % 2
        self.partner = (self.s, self.y * 2 + 1 - self.c)
        self.across = (self.z * 2 + 1 - self.x, self.t)

    def chip_y(self, d):
        return (self.s, lax.rem(self.y + d + self.Y, self.Y) * 2 + self.c)

    def chip_z(self, d):
        return (lax.rem(self.z + d + self.Z, self.Z) * 2 + self.x, self.t)


class LineGather:
    def __init__(self, place, pairs, up_s, up_r, dn_s, dn_r, x_s, x_r):
        self.p, self.pairs = place, pairs
        self.sems = (up_s, up_r, dn_s, dn_r, x_s, x_r)

    def up(self, n, d, own=False):
        p, (own_ref, all_ref) = self.p, self.pairs[n]
        block = p.s - 2 * (d - 1)
        src = own_ref if own else all_ref.at[block]
        return push(src, all_ref.at[block], self.sems[0].at[n, d], self.sems[1].at[n, d], (p.s + 2, p.t))

    def up_wait(self, n, d):
        p, (_, all_ref) = self.p, self.pairs[n]
        ref = all_ref.at[p.s - 2 * d]
        return push(ref, ref, self.sems[0].at[n, d], self.sems[1].at[n, d], (p.s - 2, p.t))

    def dn(self, n, d, own=False):
        p, (own_ref, all_ref) = self.p, self.pairs[n]
        block = p.s + 2 * (d - 1)
        src = own_ref if own else all_ref.at[block]
        return push(src, all_ref.at[block], self.sems[2].at[n, d], self.sems[3].at[n, d], (p.s - 2, p.t))

    def dn_wait(self, n, d):
        p, (_, all_ref) = self.p, self.pairs[n]
        ref = all_ref.at[p.s + 2 * d]
        return push(ref, ref, self.sems[2].at[n, d], self.sems[3].at[n, d], (p.s + 2, p.t))

    def over(self, n, d):
        p, (own_ref, all_ref) = self.p, self.pairs[n]
        block = p.s - 2 * d
        k = d + p.Z - 1
        src = own_ref if d == 0 else all_ref.at[block]
        return push(src, all_ref.at[block], self.sems[4].at[n, k], self.sems[5].at[n, k], p.across)

    def over_wait(self, n, d):
        p, (_, all_ref) = self.p, self.pairs[n]
        ref = all_ref.at[p.z * 2 + 1 - p.x - 2 * d]
        k = d + p.Z - 1
        return push(ref, ref, self.sems[4].at[n, k], self.sems[5].at[n, k], p.across)

    def start(self, count):
        p = self.p

        @pl.when(p.z + 1 < p.Z)
        def _():
            for n in count:
                self.up(n, 1, True).start()

        @pl.when(p.z >= 1)
        def _():
            for n in count:
                self.dn(n, 1, True).start()

        for n in count:
            self.over(n, 0).start()

    def step(self, d):
        p = self.p
        for n in range(len(self.pairs)):

            @pl.when(p.z - d >= 0)
            def _():
                self.up_wait(n, d).wait_recv()

                @pl.when(p.z + 1 < p.Z)
                def _():
                    self.up(n, d + 1).start()

                self.over(n, d).start()

            @pl.when(p.z + d < p.Z)
            def _():
                self.dn_wait(n, d).wait_recv()

                @pl.when(p.z >= 1)
                def _():
                    self.dn(n, d + 1).start()

                self.over(n, -d).start()

    def arrive(self, sign, d):
        for n in range(len(self.pairs)):
            self.over_wait(n, sign * d).wait_recv()

    def side(self, sign, d):
        return self.p.z - d >= 0 if sign > 0 else self.p.z + d < self.p.Z

    def finish(self):
        p = self.p
        for n in range(len(self.pairs)):
            for d in range(p.Z):
                for sign in (1, -1) if d else (1,):

                    @pl.when(self.side(sign, d))
                    def _():
                        self.over(n, sign * d).wait_send()

            for d in range(1, p.Z):

                @pl.when(jnp.logical_and(p.z - d + 1 >= 0, p.z + 1 < p.Z))
                def _():
                    self.up(n, d).wait_send()

                @pl.when(jnp.logical_and(p.z + d - 1 < p.Z, p.z >= 1))
                def _():
                    self.dn(n, d).wait_send()


def line_sems(p_z, n):
    return [pltpu.SemaphoreType.DMA((n, p_z + 1))] * 4 + [pltpu.SemaphoreType.DMA((n, 2 * p_z))] * 2


class PairScatter:
    def __init__(self, p, part, first, summed, second, fs, fr, ss, sr):
        self.p, self.part, self.first, self.summed, self.second = p, part, first, summed, second
        self.sems = (fs, fr, ss, sr)
        self.started = []

    def start(self):
        p = self.p
        for d in range(p.Y):
            y = lax.rem(p.y + d, p.Y)
            copy = push(
                self.part(y * 2 + 1 - p.c), self.first.at[d], self.sems[0].at[d], self.sems[1].at[d], p.partner
            )
            copy.start()
            self.started.append(copy)

    def middle(self):
        p = self.p
        for d in list(range(1, p.Y)) + [0]:
            y = lax.rem(p.y + d, p.Y)
            self.started[d].wait_recv()
            total = self.part(y * 2 + p.c)[...].astype(F32) + self.first[d].astype(F32)
            self.summed[d] = total.astype(BF)
            if d:
                copy = push(
                    self.summed.at[d], self.second.at[d], self.sems[2].at[d], self.sems[3].at[d], p.chip_y(d)
                )
                copy.start()
                self.started.append(copy)

    def finish(self):
        p = self.p
        total = self.part(p.t)[...].astype(F32) + self.first[0].astype(F32)
        for d in range(1, p.Y):
            self.started[p.Y + d - 1].wait_recv()
            total = total + self.second[d].astype(F32)
        for copy in self.started:
            copy.wait_send()
        return total


class PairGather:
    def __init__(self, p, own, spot, ys, yr, ps, pr):
        self.p, self.own, self.spot, self.sems = p, own, spot, (ys, yr, ps, pr)
        self.started = []

    def start(self):
        p = self.p
        for d in range(1, p.Y):
            copy = push(self.own, self.spot(p.t), self.sems[0].at[d], self.sems[1].at[d], p.chip_y(d))
            copy.start()
            self.started.append(copy)
        copy = push(self.own, self.spot(p.t), self.sems[2].at[0], self.sems[3].at[0], p.partner)
        copy.start()
        self.started.append(copy)

    def forward(self):
        p = self.p
        for d in range(1, p.Y):
            ref = self.spot(lax.rem(p.y - d + p.Y, p.Y) * 2 + p.c)
            push(ref, ref, self.sems[0].at[d], self.sems[1].at[d], p.chip_y(-d)).wait_recv()
            copy = push(ref, ref, self.sems[2].at[d], self.sems[3].at[d], p.partner)
            copy.start()
            self.started.append(copy)

    def arrive(self):
        p = self.p
        for d in range(p.Y):
            ref = self.spot(lax.rem(p.y - d + p.Y, p.Y) * 2 + 1 - p.c)
            push(ref, ref, self.sems[2].at[d], self.sems[3].at[d], p.partner).wait_recv()

    def finish(self):
        for copy in self.started:
            copy.wait_send()


def layer_kernel(
    sp, tp, shift_base,
    raw, to, src, gain, saved, offs, wq_h, wk_h, wv_h, wo_h,
    flat_all, src_out, tgt_out, cols_all,
    tn, pieces, wq, wk, wv, wo, tn_all, to_all, src_all, cols, tn_b, to_b,
    q_all, hg_all, small_all, k_s, v_s, p_s, d_s, part, kf, vf, sg,
    xr, xz, zr, sg1, sg2, sg3, ng, ng1, ng2, ng3,
    wsem, loc, es, er, *sems
):
    p = Place(sp, tp)
    pair_sems = [sems[4 * i : 4 * i + 4] for i in range(6)]
    xs_s, xs_r, zs_s, zs_r = sems[24:28]
    line_a, line_b = sems[28:34], sems[34:40]
    rows, block = raw.shape[0], saved.shape[0]
    width, model = wq.shape[1], wq.shape[0]
    heads = width // HEAD_DIM
    scale = HEAD_DIM ** (-0.5)
    loads = [
        pltpu.make_async_copy(h, v, wsem.at[i])
        for i, (h, v) in enumerate(((wq_h, wq), (wo_h, wo), (wk_h, wk), (wv_h, wv)))
    ]
    for copy in loads:
        copy.start()
    raw_value, gain_value = raw[...].astype(F32), gain[...].astype(F32).reshape(1, model)
    inverse = lax.rsqrt(jnp.mean(raw_value * raw_value, axis=1, keepdims=True) + EPSILON)
    normed_value = (raw_value * inverse * gain_value).astype(BF)
    tn[...] = normed_value
    slice_width = model // sp
    for s in range(sp):
        pieces[s] = normed_value[:, s * slice_width : (s + 1) * slice_width]
    greet(
        [p.partner]
        + [p.chip_y(d) for d in range(1, p.Y)]
        + [(lax.rem(p.s + e, sp), p.t) for e in range(1, sp)]
    )
    g_tn = PairGather(p, tn, lambda t: tn_all.at[t], *pair_sems[0])
    g_to = PairGather(p, to, lambda t: to_all.at[t], *pair_sems[1])
    g_src = PairGather(p, src, lambda t: src_all.at[t], *pair_sems[2])
    g_cols = PairGather(p, cols, lambda t: cols_all.at[:, t], *pair_sems[3])
    for g in (g_tn, g_to, g_src):
        g.start()
    swaps = []
    for e in range(1, sp):
        s = lax.rem(p.s + e, sp)
        copy = push(pieces.at[s], cols.at[p.s], es.at[e], er.at[e], (s, p.t))
        copy.start()
        swaps.append(copy)
    mine = [
        pltpu.make_async_copy(tn, tn_all.at[p.t], loc.at[0]),
        pltpu.make_async_copy(to, to_all.at[p.t], loc.at[1]),
        pltpu.make_async_copy(src, src_all.at[p.t], loc.at[2]),
        pltpu.make_async_copy(pieces.at[p.s], cols.at[p.s], loc.at[3]),
    ]
    for copy in mine:
        copy.start()
    for copy in mine:
        copy.wait()
    tile = min(width, 256)
    gather = LineGather(
        p, ((q_all.at[p.s], q_all), (hg_all.at[p.s], hg_all), (small_all.at[p.s], small_all)), *line_a
    )

    g_tn.forward()
    g_to.forward()
    g_tn.arrive()
    for t in range(tp):
        tn_b[t * rows : (t + 1) * rows, :] = tn_all[t]
    loads[0].wait()
    for j in range(0, width, tile):
        q_all[p.s, :, j : j + tile] = jnp.dot(
            tn_b[...], wq[:, j : j + tile], preferred_element_type=F32
        ).astype(BF)
    gather.start((0,))
    g_to.arrive()
    for t in range(tp):
        to_b[t * rows : (t + 1) * rows, :] = to_all[t]
    loads[1].wait()
    lane = lax.broadcasted_iota(jnp.int32, (block, 128), 1)
    pick = lax.broadcasted_iota(jnp.int32, (heads, 128), 0) == lax.broadcasted_iota(jnp.int32, (heads, 128), 1)
    small = lax.dot_general(
        offs[...].astype(F32), pick.astype(F32), (((0,), (0,)), ((), ())), precision=lax.Precision.HIGHEST,
        preferred_element_type=F32,
    )
    for h in range(heads):
        cut = slice(h * HEAD_DIM, (h + 1) * HEAD_DIM)
        part_h = contract_last(to_b[...], wo[cut, :]).astype(BF)
        hg_all[p.s, :, cut] = part_h
        delta = jnp.sum(part_h.astype(F32) * saved[:, cut].astype(F32), axis=1, keepdims=True)
        small = jnp.where(lane == heads + h, delta, small)
    small_all[p.s] = small.astype(BF)
    gather.start((1, 2))

    g_src.forward()
    g_src.arrive()
    gather.step(1)
    source_count = k_s.shape[0]
    loads[2].wait()
    loads[3].wait()

    @pl.loop(0, width // tile)
    def _(j):
        cut = pl.ds(pl.multiple_of(j * tile, tile), tile)
        rows_value = src_all[...].reshape(source_count, model)
        k_s[:, cut] = jnp.dot(rows_value, wk[:, cut], preferred_element_type=F32).astype(BF)
        v_s[:, cut] = jnp.dot(rows_value, wv[:, cut], preferred_element_type=F32).astype(BF)

    for e in range(1, sp):
        s = lax.rem(p.s - e + sp, sp)
        push(cols.at[s], cols.at[s], es.at[e], er.at[e], (s, p.t)).wait_recv()
    g_cols.start()
    keep = pltpu.make_async_copy(cols, cols_all.at[:, p.t], loc.at[4])
    keep.start()

    def into(k):
        z = lax.rem(p.z + k, p.Z)
        return push(part.at[z * 2 + 1 - p.x], xr.at[k], xs_s.at[k], xs_r.at[k], p.across)

    def attend(z):
        pair = pl.ds(2 * z, 2)
        spot = pl.ds(pl.multiple_of(z * (2 * block), 2 * block), 2 * block)
        tiny = small_all[pair].reshape(2 * block, 128).astype(F32)
        for h in range(heads):
            cut = slice(h * HEAD_DIM, (h + 1) * HEAD_DIM)
            q_h = q_all[pair, :, cut].reshape(2 * block, HEAD_DIM)
            g_h = hg_all[pair, :, cut].reshape(2 * block, HEAD_DIM)
            prob = jnp.exp(contract_last(q_h, k_s[:, cut]) * scale - (shift_base + tiny[:, h : h + 1]))
            grad = contract_last(g_h, v_s[:, cut])
            score = (prob * (grad - tiny[:, heads + h : heads + h + 1]) * scale).astype(BF)
            p_s[h, spot, :] = prob.astype(BF)
            d_s[h, spot, :] = score
            term = jnp.dot(score, k_s[:, cut], preferred_element_type=F32).astype(BF)
            part[pair, :, cut] = term.reshape(2, block, HEAD_DIM)

    def reached(sign, d):
        gather.arrive(sign, d)
        attend(p.z - sign * d)
        into((-sign * d) % p.Z).start()

    for d in range(1, p.Z):
        if d > 1:
            gather.step(d)
        for sign in (1, -1) if d > 1 else (1,):

            @pl.when(gather.side(sign, d - 1))
            def _():
                reached(sign, d - 1)

        if d == 1:
            g_cols.forward()
    for sign in (1, -1):

        @pl.when(gather.side(sign, p.Z - 1))
        def _():
            reached(sign, p.Z - 1)

    order = sorted(range(1, p.Z), key=lambda k: min(k, p.Z - k))
    hops = {}

    def relay(k):
        into(k).wait_recv()
        z = lax.rem(p.z + k, p.Z)
        xz[k] = (part[z * 2 + p.x].astype(F32) + xr[k].astype(F32)).astype(BF)
        hops[k] = push(xz.at[k], zr.at[k], zs_s.at[k], zs_r.at[k], p.chip_z(k))
        hops[k].start()

    for k in order[:1]:
        relay(k)
    count = sp * block

    for h in range(heads):
        cut = slice(h * HEAD_DIM, (h + 1) * HEAD_DIM)
        dims = (((0,), (0,)), ((), ()))
        q_h = q_all[:, :, cut].reshape(count, HEAD_DIM)
        g_h = hg_all[:, :, cut].reshape(count, HEAD_DIM)
        kf[:, cut] = lax.dot_general(d_s[h], q_h, dims, preferred_element_type=F32).astype(BF)
        vf[:, cut] = lax.dot_general(p_s[h], g_h, dims, preferred_element_type=F32).astype(BF)
    for k in order[1:2]:
        relay(k)
    stile = min(model, 256)

    def source_term(j):
        cut = pl.ds(pl.multiple_of(j * stile, stile), stile)
        value = contract_last(kf[...], wk[cut, :]) + contract_last(vf[...], wv[cut, :])
        sg[:, :, cut] = value.astype(BF).reshape(tp, source_count // tp, stile)

    half = model // stile // 2
    pl.loop(0, half)(source_term)
    for k in order[2:]:
        relay(k)
    pl.loop(half, model // stile)(source_term)
    source = PairScatter(p, lambda t: sg.at[t], sg1, sg2, sg3, *pair_sems[4])
    source.start()
    source.middle()
    into(0).wait_recv()
    total = part[p.s].astype(F32) + xr[0].astype(F32)
    for k in order:
        hops[k].wait_recv()
        total = total + zr[k].astype(F32)
    flat = total.astype(BF)
    flat_all[p.s] = flat
    spread = LineGather(p, ((flat_all.at[p.s], flat_all),), *line_b)
    spread.start((0,))
    for j in range(0, model, stile):
        columns = contract_last(flat, wq[j : j + stile, :]).astype(BF)
        for t in range(tp):
            ng[t, :, j : j + stile] = columns[t * rows : (t + 1) * rows]
    normed = PairScatter(p, lambda t: ng.at[t], ng1, ng2, ng3, *pair_sems[5])
    normed.start()
    for d in range(1, p.Z):
        spread.step(d)
        if d == 1:
            normed.middle()
    src_out[...] = source.finish()
    raw_value, gain_value = raw[...].astype(F32), gain[...].astype(F32).reshape(1, model)
    inverse = lax.rsqrt(jnp.mean(raw_value * raw_value, axis=1, keepdims=True) + EPSILON)
    scaled = normed.finish() * gain_value
    tgt_out[...] = inverse * scaled - raw_value * (inverse * inverse * inverse) * jnp.mean(
        scaled * raw_value, axis=1, keepdims=True
    )
    g_cols.arrive()
    for d in range(p.Z):
        for sign in (1, -1) if d else (1,):

            @pl.when(spread.side(sign, d))
            def _():
                spread.arrive(sign, d)

    gather.finish()
    spread.finish()
    for g in (g_tn, g_to, g_src, g_cols):
        g.finish()
    for copy in swaps:
        copy.wait_send()
    keep.wait()
    for k in range(p.Z):
        into(k).wait_send()
    for k in order:
        hops[k].wait_send()


def body(
    target_rows,
    source_rows,
    norm_gain,
    query_weight,
    key_weight,
    value_weight,
    output_weight,
    saved_output,
    norm_offset,
    output_grad,
):
    tp, sp = lax.axis_size("tp"), lax.axis_size("sp")
    Z, Y = sp // 2, tp // 2
    model, width = query_weight.shape
    heads = width // HEAD_DIM
    rows, srows = target_rows.shape[0], source_rows.shape[0]
    block = rows * tp
    count = block * sp
    source_count = srows * tp
    shift_base = math.log(source_count * sp)
    slice_width = model // sp
    dma = pltpu.SemaphoreType.DMA

    vm = pltpu.VMEM
    whole = pl.BlockSpec(memory_space=pl.ANY)
    flat_all, source_grad, target_grad, cols_all = pl.pallas_call(
        functools.partial(layer_kernel, sp, tp, shift_base),
        out_shape=[
            jax.ShapeDtypeStruct((sp, block, width), BF),
            jax.ShapeDtypeStruct((srows, model), F32),
            jax.ShapeDtypeStruct((rows, model), F32),
            jax.ShapeDtypeStruct((sp, tp, rows, slice_width), BF),
        ],
        in_specs=[VMEM] * 6 + [whole] * 4,
        out_specs=[VMEM] * 4,
        scratch_shapes=[vm((rows, model), BF), vm((sp, rows, slice_width), BF)]
        + [vm((model, width), BF)] * 3
        + [vm((width, model), BF)]
        + [vm((tp, rows, model), BF)] * 2
        + [vm((tp, srows, model), BF), vm((sp, rows, slice_width), BF)]
        + [vm((block, model), BF)] * 2
        + [vm((sp, block, width), BF)] * 2
        + [vm((sp, block, 128), BF)]
        + [vm((source_count, width), BF)] * 2
        + [vm((heads, count, source_count), BF)] * 2
        + [vm((sp, block, width), BF)]
        + [vm((source_count, width), BF)] * 2
        + [vm((tp, srows, model), BF)]
        + [vm((Z, block, width), BF)] * 3
        + [vm((Y, srows, model), BF)] * 3
        + [vm((tp, rows, model), BF)]
        + [vm((Y, rows, model), BF)] * 3
        + [dma((4,)), dma((5,)), dma((sp,)), dma((sp,))]
        + [dma((Y,))] * 24
        + [dma((Z,))] * 4
        + line_sems(Z, 3)
        + line_sems(Z, 1),
        name="layer_kernel",
        compiler_params=pltpu.CompilerParams(
            collective_id=1, has_side_effects=True, vmem_limit_bytes=58 * 2**20
        ),
    )(
        target_rows,
        output_grad,
        source_rows,
        norm_gain,
        saved_output,
        norm_offset.T,
        query_weight,
        key_weight,
        value_weight,
        output_weight,
    )
    weight_grad = lax.dot_general(
        cols_all.reshape(count, slice_width),
        flat_all.reshape(count, width),
        (((0,), (0,)), ((), ())),
        preferred_element_type=F32,
    )
    return (target_grad, source_grad, weight_grad)


class Net:
    def __init__(self, send, recv):
        self.send, self.recv, self.ids = send, recv, {}
        self.free, self.started = list(range(send.shape[0])), []

    def _copy(self, name, src, dst, device, slot=0):
        n = self.ids.setdefault(name, len(self.ids))
        return push(src, dst, self.send.at[slot], self.recv.at[n], device)

    def go(self, name, src, dst, device):
        if not self.free:
            self.drain(1)
        slot = self.free.pop(0)
        copy = self._copy(name, src, dst, device, slot)
        copy.start()
        self.started.append((slot, copy))

    def same(self, name, ref, device):
        self.go(name, ref, ref, device)

    def wait(self, name, landed, device):
        self._copy(name, landed, landed, device).wait_recv()

    def drain(self, count=None):
        count = len(self.started) if count is None else count
        for slot, copy in self.started[:count]:
            copy.wait_send()
            self.free.append(slot)
        self.started = self.started[count:]


SENDS = 20
Y_FIRST = (False, True, True, True)


def grid_kernel(
    sp, tp, shift_base,
    raw_h, to_h, src_h, gain_h, saved_h, offs_h, wq_h, wk_h, wv_h, wo_h,
    ws_h, src_h_out, tgt_h_out,
    raw, gain, saved, offs, src_out, tgt_out,
    tn_all, to_all, src_all, pieces, cols, q_st, g_st, sm_st, q_all, g_all, sm_all,
    wq, wkv, wo, kv, p_s, d_s, part, xr, xs, ur, flat_all, fl, kv_sum, kvf,
    sg, sd, ss, es, fs, fr, na, ng, nr, wt,
    wsem, osem, send, recv
):
    p = Place(sp, tp)
    s, t, y, c, x = p.s, p.t, p.y, p.c, p.x
    u, v = p.z // 2, p.z % 2
    net = Net(send, recv)

    def at(u, v, x):
        return ((u * 2 + v) * 2 + x, t)

    C, Y, V, X, U = p.partner, p.chip_y(1), at(u, 1 - v, x), at(u, v, 1 - x), at(1 - u, v, x)
    ty, tc, tyc = (1 - y) * 2 + c, y * 2 + 1 - c, (1 - y) * 2 + 1 - c
    others = [
        (a, b, d, u + a - 2 * u * a, v + b - 2 * v * b, x + d - 2 * x * d)
        for a in range(2) for b in range(2) for d in range(2) if a + b + d
    ]
    barrier = pltpu.get_barrier_semaphore()
    D = (s, tyc)
    friends = [C, Y, D] + [at(*o[3:]) for o in others]
    for device in friends:
        pl.semaphore_signal(barrier, inc=1, device_id=device, device_id_type=MESH)
    rows, block, srows = raw.shape[0], saved.shape[0], src_h.shape[0]
    model, width = wq.shape
    heads = width // HEAD_DIM
    hh, half = heads // 2, width // 2
    sblock = srows * tp
    sw = model // sp
    quarters = len(Y_FIRST)
    mq = model // quarters
    scale = HEAD_DIM ** (-0.5)
    mine = pl.ds(pl.multiple_of(v * half, half), half)
    loads = [
        pltpu.make_async_copy(h, w, wsem.at[i])
        for i, (h, w) in enumerate(
            (
                (wq_h, wq), (wo_h, wo), (wk_h.at[:, mine], wkv.at[:, :half]), (wv_h.at[:, mine], wkv.at[:, half:]),
                (raw_h, raw), (gain_h, gain), (src_h, src_all.at[v, t]), (to_h, to_all.at[t]),
                (saved_h, saved), (offs_h, offs),
            )
        )
    ]
    for n in (4, 5, 6, 7, 0, 1, 8, 9, 2, 3):
        loads[n].start()
    loads[4].wait()
    loads[5].wait()
    raw_value, gain_value = raw[...].astype(F32), gain[...].astype(F32).reshape(1, model)
    inverse = lax.rsqrt(jnp.mean(raw_value * raw_value, axis=1, keepdims=True) + EPSILON)
    normed_value = (raw_value * inverse * gain_value).astype(BF)
    tn_all[t] = normed_value
    for a in range(2):
        for b in range(2):
            for k in range(2):
                n = (2 * a + k) * 2 + b
                pieces[a, b, :, k * sw : (k + 1) * sw] = normed_value[:, n * sw : (n + 1) * sw]
    loads[6].wait()
    loads[7].wait()
    pl.semaphore_wait(barrier, len(friends))
    A, B = pl.ds(0, srows // 2), pl.ds(srows // 2, srows // 2)

    net.same("tnY", tn_all.at[t], Y)
    net.same("sVB", src_all.at[v, t, B], V)
    net.same("tnC", tn_all.at[t], C)
    net.same("toY", to_all.at[t], Y)
    net.same("toC", to_all.at[t], C)
    net.same("sYA", src_all.at[v, t, A], Y)
    net.same("sVA", src_all.at[v, t, A], V)
    net.same("sYB", src_all.at[v, t, B], Y)
    net.same("sC", src_all.at[v, t], C)
    net.wait("tnY", tn_all.at[ty], Y)
    net.same("tnF", tn_all.at[ty], C)
    net.wait("toY", to_all.at[ty], Y)
    net.same("toF", to_all.at[ty], C)
    net.wait("tnC", tn_all.at[tc], C)
    net.wait("tnF", tn_all.at[tyc], C)
    loads[0].wait()
    tn_b = tn_all[...].reshape(block, model)
    for k in range(2):
        for j in range(0, half, HEAD_DIM):
            q_st[k, :, j : j + HEAD_DIM] = jnp.dot(
                tn_b, wq[:, k * half + j : k * half + j + HEAD_DIM], preferred_element_type=F32
            ).astype(BF)
    net.go("qV", q_st.at[1 - v], q_all.at[u, x, v], V)
    q_all[u, x, v] = q_st[v]
    net.same("q0U", q_all.at[u, x, v], U)
    net.same("q0X", q_all.at[u, x, v], X)
    net.wait("sVB", src_all.at[1 - v, t, B], V)
    net.same("fVB", src_all.at[1 - v, t, B], Y)
    net.same("cVB", src_all.at[1 - v, t, B], C)
    net.wait("toC", to_all.at[tc], C)
    net.wait("toF", to_all.at[tyc], C)
    loads[1].wait()
    loads[8].wait()
    loads[9].wait()
    to_b = to_all[...].reshape(block, model)
    products = []
    for n in range(heads):
        cut = slice(n * HEAD_DIM, (n + 1) * HEAD_DIM)
        part_h = contract_last(to_b, wo[cut, :]).astype(BF)
        g_st[n // hh, :, n % hh * HEAD_DIM : (n % hh + 1) * HEAD_DIM] = part_h
        products.append(part_h.astype(F32) * saved[:, cut].astype(F32))
    net.go("gV", g_st.at[1 - v], g_all.at[u, x, v], V)
    g_all[u, x, v] = g_st[v]
    net.same("g0U", g_all.at[u, x, v], U)
    net.same("g0X", g_all.at[u, x, v], X)
    lines, lanes = sm_st.shape[1], 2 * block
    place = (
        lax.broadcasted_iota(jnp.int32, (block, lanes), 1)
        == lax.broadcasted_iota(jnp.int32, (block, lanes), 0) + v * block
    ).astype(F32)
    spread = jnp.dot(offs[...].astype(F32), place, precision=lax.Precision.HIGHEST, preferred_element_type=F32)
    product = jnp.concatenate(products, axis=1)
    line = lax.broadcasted_iota(jnp.int32, (2 * lines, width), 0)
    head = lax.broadcasted_iota(jnp.int32, (2 * lines, width), 1) // HEAD_DIM
    pick = (line == head // hh * lines + hh + head % hh).astype(BF)
    deltas = 0.0
    for term in range(3):
        narrow = product.astype(BF)
        product = product - narrow.astype(F32)
        padded = jnp.concatenate(
            [jnp.where(v == 0, narrow, jnp.zeros_like(narrow)), jnp.where(v == 1, narrow, jnp.zeros_like(narrow))],
            axis=0,
        )
        deltas = deltas + contract_last(pick, padded)
    line = lax.broadcasted_iota(jnp.int32, (lines, lanes), 0)
    for k in range(2):
        small = deltas[k * lines : (k + 1) * lines]
        for h in range(hh):
            n = k * hh + h
            small = jnp.where(line == h, jnp.broadcast_to(spread[n : n + 1], small.shape), small)
        sm_st[k] = small.astype(BF)
    net.go("mV", sm_st.at[1 - v], sm_all.at[u, x, v], V)
    sm_all[u, x, v] = sm_st[v]
    net.same("m0U", sm_all.at[u, x, v], U)
    net.same("m0X", sm_all.at[u, x, v], X)

    net.wait("sYA", src_all.at[v, ty, A], Y)
    net.same("cYA", src_all.at[v, ty, A], C)
    net.wait("qV", q_all.at[u, x, 1 - v], V)
    net.same("q1U", q_all.at[u, x, 1 - v], U)
    net.same("q1X", q_all.at[u, x, 1 - v], X)
    net.wait("sVA", src_all.at[1 - v, t, A], V)
    net.same("fVA", src_all.at[1 - v, t, A], Y)
    net.same("cVA", src_all.at[1 - v, t, A], C)
    net.wait("gV", g_all.at[u, x, 1 - v], V)
    net.same("g1U", g_all.at[u, x, 1 - v], U)
    net.same("g1X", g_all.at[u, x, 1 - v], X)
    net.wait("sYB", src_all.at[v, ty, B], Y)
    net.same("cYB", src_all.at[v, ty, B], C)
    net.wait("mV", sm_all.at[u, x, 1 - v], V)
    net.same("m1U", sm_all.at[u, x, 1 - v], U)
    net.same("m1X", sm_all.at[u, x, 1 - v], X)
    def project(k, y):
        count = 2 * srows
        spot = pl.ds(pl.multiple_of(k * sblock + y * count, count), count)

        @pl.loop(0, 2)
        def _(j):
            cut = pl.ds(pl.multiple_of(j * half, half), half)
            value = src_all[k, pl.ds(2 * y, 2)].reshape(count, model)
            kv[spot, cut] = jnp.dot(value, wkv[:, cut], preferred_element_type=F32).astype(BF)

    net.wait("sC", src_all.at[v, tc], C)
    loads[2].wait()
    loads[3].wait()
    net.wait("fVB", src_all.at[1 - v, ty, B], Y)
    net.same("dVB", src_all.at[1 - v, ty, B], C)
    project(v, y)
    spot = (u * 2 + x) * 2 + v
    for a, b, d, u2, v2, x2 in others:
        net.go(f"p{a}{b}{d}", pieces.at[u2, x2], cols.at[spot, t], at(u2, v2, x2))
    cols[spot, t] = pieces[u, x]
    net.wait("q0U", q_all.at[1 - u, x, v], U)
    net.same("q2X", q_all.at[1 - u, x, v], X)
    net.wait("cVB", src_all.at[1 - v, tc, B], C)
    net.wait("cVA", src_all.at[1 - v, tc, A], C)
    project(1 - v, y)
    net.wait("cYA", src_all.at[v, tyc, A], C)
    net.wait("cYB", src_all.at[v, tyc, B], C)
    net.wait("g0U", g_all.at[1 - u, x, v], U)
    net.same("g2X", g_all.at[1 - u, x, v], X)
    project(v, 1 - y)
    net.wait("fVA", src_all.at[1 - v, ty, A], Y)
    net.same("dVA", src_all.at[1 - v, ty, A], C)
    net.wait("m0U", sm_all.at[1 - u, x, v], U)
    net.same("m2X", sm_all.at[1 - u, x, v], X)
    net.wait("q1U", q_all.at[1 - u, x, 1 - v], U)
    net.same("q3X", q_all.at[1 - u, x, 1 - v], X)
    net.wait("dVB", src_all.at[1 - v, tyc, B], C)
    net.wait("dVA", src_all.at[1 - v, tyc, A], C)
    project(1 - v, 1 - y)

    def attend(w, after):
        little = sm_all[w].astype(F32)
        little = jnp.concatenate([little[0, 0] + little[0, 1], little[1, 0] + little[1, 1]], axis=1)
        for h in range(hh):
            cut = slice(h * HEAD_DIM, (h + 1) * HEAD_DIM)
            q_h = q_all[w, :, :, :, cut].reshape(4 * block, HEAD_DIM)
            g_h = g_all[w, :, :, :, cut].reshape(4 * block, HEAD_DIM)
            prob = jnp.exp(contract_last(kv[:, cut], q_h) * scale - (shift_base + little[h : h + 1]))
            grad = contract_last(kv[:, half + h * HEAD_DIM : half + (h + 1) * HEAD_DIM], g_h)
            score = (prob * (grad - little[hh + h : hh + h + 1]) * scale).astype(BF)
            p_s[h] = prob.astype(BF)
            d_s[h] = score
            term = lax.dot_general(score, kv[:, cut], (((0,), (0,)), ((), ())), preferred_element_type=F32)
            part[w, :, h] = term.astype(BF).reshape(2, 2, block, HEAD_DIM)
            after(h)

    def source_terms(w):
        for h in range(hh):
            cut = slice(h * HEAD_DIM, (h + 1) * HEAD_DIM)
            q_h = q_all[w, :, :, :, cut].reshape(4 * block, HEAD_DIM)
            g_h = g_all[w, :, :, :, cut].reshape(4 * block, HEAD_DIM)
            yield cut, jnp.dot(d_s[h], q_h, preferred_element_type=F32)
            cut = slice(half + h * HEAD_DIM, half + (h + 1) * HEAD_DIM)
            yield cut, jnp.dot(p_s[h], g_h, preferred_element_type=F32)

    def send_near(h):
        net.go(f"a{h}X", part.at[u, 1 - x, h], xr.at[0, h], X)

    def send_far(h):
        for k in range(2):
            net.go(f"b{h}{k}X", part.at[1 - u, 1 - x, h, k], xr.at[1, h, k], X)

    for n, k in ((0, v), (1, 1 - v)):
        net.wait(f"q{n}X", q_all.at[u, 1 - x, k], X)
        net.wait(f"m{n}X", sm_all.at[u, 1 - x, k], X)
        net.wait(f"g{n}X", g_all.at[u, 1 - x, k], X)
    net.wait("g1U", g_all.at[1 - u, x, 1 - v], U)
    net.same("g3X", g_all.at[1 - u, x, 1 - v], X)
    net.wait("m1U", sm_all.at[1 - u, x, 1 - v], U)
    net.same("m3X", sm_all.at[1 - u, x, 1 - v], X)
    attend(u, send_near)
    for cut, value in source_terms(u):
        kv_sum[:, cut] = value

    def near(h):
        net.wait(f"a{h}X", xr.at[0, h], X)
        xs[0, h] = (part[u, x, h].astype(F32) + xr[0, h].astype(F32)).astype(BF)
        net.go(f"s{h}U", xs.at[0, h], ur.at[1, h], U)

    for n, k in ((2, v), (3, 1 - v)):
        net.wait(f"q{n}X", q_all.at[1 - u, 1 - x, k], X)
        net.wait(f"m{n}X", sm_all.at[1 - u, 1 - x, k], X)
        net.wait(f"g{n}X", g_all.at[1 - u, 1 - x, k], X)
    attend(1 - u, send_far)
    near(0)
    for cut, value in source_terms(1 - u):
        kvf[:, cut] = (kv_sum[:, cut] + value).astype(BF)
    for h in range(1, hh):
        near(h)
    for a, b, d, u2, v2, x2 in others:
        net.wait(f"p{a}{b}{d}", cols.at[(u2 * 2 + x2) * 2 + v2, t], at(u2, v2, x2))
    net.same("kY", cols.at[:, t], Y)
    net.same("kC", cols.at[:, t], C)
    stile = min(mq, 256)

    def source(n):
        for j in range(0, mq, stile):
            value = contract_last(kvf[...], wkv[n * mq + j : n * mq + j + stile, :]).astype(BF)
            sg[n, :, :, :, j : j + stile] = value.reshape(4, 2, srows, stile)
        net.go(f"d{n}", sg.at[n, :, 1 - c], sd.at[n], C)

    def source_sum(n):
        net.wait(f"d{n}", sd.at[n], C)
        for k in range(4):
            ss[n, k] = (sg[n, k, c].astype(F32) + sd[n, k].astype(F32)).astype(BF)
        net.go(f"e{n}1", ss.at[n, 2 * (1 - v) + 1 - y], es.at[n, 1], Y if Y_FIRST[n] else V)

    def source_rest(n):
        first, near = (Y, 2 * v + 1 - y) if Y_FIRST[n] else (V, 2 * (1 - v) + y)
        net.go(f"e{n}0", ss.at[n, near], es.at[n, 0], first)

    def source_pass(n):
        first, last = (Y, V) if Y_FIRST[n] else (V, Y)
        keep = 2 * (1 - v) + y if Y_FIRST[n] else 2 * v + 1 - y
        net.wait(f"e{n}1", es.at[n, 1], first)
        fs[n] = (ss[n, keep].astype(F32) + es[n, 1].astype(F32)).astype(BF)
        net.go(f"f{n}", fs.at[n], fr.at[n], last)

    kept = []

    def keep(ref, out):
        copy = pltpu.make_async_copy(ref, out, osem.at[len(kept)])
        copy.start()
        kept.append(copy)

    def source_end(n):
        first, last = (Y, V) if Y_FIRST[n] else (V, Y)
        net.wait(f"e{n}0", es.at[n, 0], first)
        net.wait(f"f{n}", fr.at[n], last)
        src_out[n] = ss[n, 2 * v + y].astype(F32) + es[n, 0].astype(F32) + fr[n].astype(F32)
        keep(src_out.at[n], src_h_out.at[n])

    def far(h):
        for k in range(2):
            net.wait(f"b{h}{k}X", xr.at[1, h, k], X)
            xs[1, h, k] = (part[1 - u, x, h, k].astype(F32) + xr[1, h, k].astype(F32)).astype(BF)
            net.go(f"z{h}{k}U", xs.at[1, h, k], ur.at[0, h, k], U)

    def flat_far(h):
        net.wait(f"s{h}U", ur.at[1, h], U)
        flat_all[1 - u, x, h] = (xs[1, h].astype(F32) + ur[1, h].astype(F32)).astype(BF)
        net.same(f"w{h}X", flat_all.at[1 - u, x, h], X)

    def flat_near(h):
        for k in range(2):
            net.wait(f"z{h}{k}U", ur.at[0, h, k], U)
            flat_all[u, x, h, k] = (xs[0, h, k].astype(F32) + ur[0, h, k].astype(F32)).astype(BF)
            net.same(f"r{h}{k}X", flat_all.at[u, x, h, k], X)
        net.go(f"n{h}V", flat_all.at[u, x, h, 1 - v], fl.at[v, h], V)
        fl[v, h] = flat_all[u, x, h, v]

    def weight(h):
        for k in range(2):
            net.wait(f"r{h}{k}X", flat_all.at[u, 1 - x, h, k], X)
        net.wait(f"w{h}X", flat_all.at[1 - u, 1 - x, h], X)
        flat_h = flat_all[:, :, h].reshape(sp * block, HEAD_DIM)
        for k in range(2):
            wt[h, k] = lax.dot_general(
                cols[:, :, :, k * sw : (k + 1) * sw].reshape(sp * block, sw), flat_h,
                (((0,), (0,)), ((), ())), preferred_element_type=F32,
            ).astype(BF)
        net.go(f"W{h}", wt.at[h, 1 - v], ws_h.at[v, h], V)
        keep(wt.at[h, v], ws_h.at[v, h])

    ntile = min(model, 256)

    def normed_term(h, k, own):
        if not own:
            net.wait(f"n{h}V", fl.at[k, h], V)
        cut = pl.ds(pl.multiple_of((k * hh + h) * HEAD_DIM, HEAD_DIM), HEAD_DIM)
        for j in range(0, model, ntile):
            columns = contract_last(fl[k, h], wq[j : j + ntile, cut])
            if not own or h:
                columns = columns + na[:, j : j + ntile]
            if own or h < hh - 1:
                na[:, j : j + ntile] = columns
            else:
                ng[:, :, j : j + ntile] = columns.astype(BF).reshape(tp, rows, ntile)

    source(0)
    far(0)
    source(1)
    for h in range(1, hh):
        far(h)
    source(2)
    source_sum(0)
    source_rest(0)
    source(3)
    source_sum(1)
    source_sum(2)
    net.wait("kY", cols.at[:, ty], Y)
    net.same("kF", cols.at[:, ty], C)
    source_sum(3)
    for n in range(1, quarters):
        source_rest(n)
    source_pass(1)
    for h in range(hh):
        flat_far(h)
    flat_near(0)
    source_pass(0)
    normed_term(0, v, True)
    net.wait("kC", cols.at[:, tc], C)
    net.wait("kF", cols.at[:, tyc], C)
    for h in range(1, hh):
        flat_near(h)
        normed_term(h, v, True)
    source_pass(2)
    weight(0)
    source_pass(3)
    for h in range(1, hh):
        weight(h)
    for h in range(hh):
        normed_term(h, 1 - v, False)
    owners = ((tyc, D), (ty, Y), (tc, C))
    for n, (k, device) in enumerate(owners):
        net.go(f"o{n}", ng.at[k], nr.at[n], device)
    for n in (0, 1, 2, 3):
        source_end(n)
    raw_value, gain_value = raw[...].astype(F32), gain[...].astype(F32).reshape(1, model)
    inverse = lax.rsqrt(jnp.mean(raw_value * raw_value, axis=1, keepdims=True) + EPSILON)
    scaled = ng[t].astype(F32)
    for n, (_, device) in enumerate(owners):
        net.wait(f"o{n}", nr.at[n], device)
        scaled = scaled + nr[n].astype(F32)
    scaled = scaled * gain_value
    tgt_out[...] = inverse * scaled - raw_value * (inverse * inverse * inverse) * jnp.mean(
        scaled * raw_value, axis=1, keepdims=True
    )
    keep(tgt_out, tgt_h_out)
    for h in range(hh):
        net.wait(f"W{h}", ws_h.at[1 - v, h], V)
    net.drain()
    for copy in kept:
        copy.wait()


def finish_kernel(ws, src_in, tgt_in, weight_out, src_out, tgt_out):
    parts, hh = ws.shape[0], ws.shape[1]
    for k in range(parts):
        for h in range(hh):
            n = (k * hh + h) * HEAD_DIM
            weight_out[:, n : n + HEAD_DIM] = ws[k, h].astype(F32)
    quarters, mq = src_in.shape[0], src_in.shape[2]
    for n in range(quarters):
        src_out[:, n * mq : (n + 1) * mq] = src_in[n]
    tgt_out[...] = tgt_in[...]


def grid_body(
    target_rows, source_rows, norm_gain, query_weight, key_weight, value_weight, output_weight,
    saved_output, norm_offset, output_grad
):
    tp, sp = lax.axis_size("tp"), lax.axis_size("sp")
    model, width = query_weight.shape
    heads = width // HEAD_DIM
    hh, half = heads // 2, width // 2
    rows, srows = target_rows.shape[0], source_rows.shape[0]
    block, sblock, sw = rows * tp, srows * tp, model // sp
    dma, vm = pltpu.SemaphoreType.DMA, pltpu.VMEM
    whole = pl.BlockSpec(memory_space=pl.ANY)
    quarters = len(Y_FIRST)
    mq = model // quarters
    ws, source_grad, target_grad = pl.pallas_call(
        functools.partial(grid_kernel, sp, tp, math.log(sblock * sp)),
        out_shape=[
            jax.ShapeDtypeStruct((2, hh, sw, HEAD_DIM), BF),
            jax.ShapeDtypeStruct((quarters, srows, mq), F32),
            jax.ShapeDtypeStruct((rows, model), F32),
        ],
        in_specs=[whole] * 10,
        out_specs=[whole] * 3,
        scratch_shapes=[vm((rows, model), BF), vm((model,), BF), vm((block, width), BF), vm((heads, block), BF)]
        + [vm((quarters, srows, mq), F32), vm((rows, model), F32)]
        + [vm((tp, rows, model), BF)] * 2
        + [vm((2, tp, srows, model), BF)]
        + [vm((2, 2, rows, 2 * sw), BF), vm((sp, tp, rows, 2 * sw), BF)]
        + [vm((2, block, half), BF)] * 2
        + [vm((2, 16, 2 * block), BF)]
        + [vm((2, 2, 2, block, half), BF)] * 2
        + [vm((2, 2, 2, 16, 2 * block), BF)]
        + [vm((model, width), BF)] * 2
        + [vm((width, model), BF)]
        + [vm((2 * sblock, width), BF)]
        + [vm((hh, 2 * sblock, 4 * block), BF)] * 2
        + [vm((2, 2, hh, 2, block, HEAD_DIM), BF)]
        + [vm((2, hh, 2, block, HEAD_DIM), BF)] * 3
        + [vm((2, 2, hh, 2, block, HEAD_DIM), BF)]
        + [vm((2, hh, block, HEAD_DIM), BF)]
        + [vm((2 * sblock, width), F32), vm((2 * sblock, width), BF)]
        + [vm((quarters, 4, 2, srows, mq), BF)]
        + [vm((quarters, 4, srows, mq), BF)] * 2
        + [vm((quarters, 2, srows, mq), BF)]
        + [vm((quarters, srows, mq), BF)] * 2
        + [vm((block, model), F32)]
        + [vm((tp, rows, model), BF)]
        + [vm((3, rows, model), BF)]
        + [vm((hh, 2, sw, HEAD_DIM), BF)]
        + [dma((10,)), dma((quarters + hh + 1,)), dma((SENDS,)), dma((69 + 11 * hh,))],
        name="grid_kernel",
        compiler_params=pltpu.CompilerParams(
            collective_id=1, has_side_effects=True, vmem_limit_bytes=58 * 2**20
        ),
    )(
        target_rows, output_grad, source_rows, norm_gain, saved_output, norm_offset.T,
        query_weight, key_weight, value_weight, output_weight,
    )
    weight_grad, source_grad, target_grad = pl.pallas_call(
        finish_kernel,
        out_shape=[
            jax.ShapeDtypeStruct((sw, width), F32),
            jax.ShapeDtypeStruct((srows, model), F32),
            jax.ShapeDtypeStruct((rows, model), F32),
        ],
        in_specs=[VMEM] * 3,
        out_specs=[VMEM] * 3,
        name="finish_kernel",
    )(ws, source_grad, target_grad)
    return (target_grad, source_grad, weight_grad)


def on_grid(target_rows, query_weight):
    pairs = (lax.axis_size("sp"), lax.axis_size("tp")) == (2**3, 2**2)
    heads = query_weight.shape[1] // HEAD_DIM
    return pairs and heads % 2 == 0 and 2 * target_rows.shape[0] * lax.axis_size("tp") % 128 == 0


def layer(*args):
    return (grid_body if on_grid(args[0], args[3]) else body)(*args)


def solution(mesh):
    in_specs = (
        P(("sp", "tp"), None),
        P(("sp", "tp"), None),
        P(),
        P(None, "tp"),
        P(None, "tp"),
        P(None, "tp"),
        P("tp", None),
        P("sp", "tp"),
        P("sp", "tp"),
        P(("sp", "tp"), None),
    )
    out_specs = (P(("sp", "tp"), None), P(("sp", "tp"), None), P("sp", "tp"))
    return jax.shard_map(layer, mesh=mesh, in_specs=in_specs, out_specs=out_specs, check_vma=False)
```

```python
import functools
import math

import jax
import jax.numpy as jnp
from jax import lax
from jax.experimental import pallas as pl
from jax.experimental.pallas import tpu as pltpu
from jax.sharding import PartitionSpec as P

HEAD_DIM = 256
EPSILON = 1e-06
MESH = pl.DeviceIdType.MESH
BF = jnp.bfloat16
F32 = jnp.float32
VMEM = pl.BlockSpec(memory_space=pltpu.VMEM)


def contract_last(left, right):
    return lax.dot_general(left, right, (((1,), (1,)), ((), ())), preferred_element_type=F32)


def push(src, dst, send, recv, device):
    return pltpu.make_async_remote_copy(
        src_ref=src, dst_ref=dst, send_sem=send, recv_sem=recv, device_id=device, device_id_type=MESH
    )


def greet(devices):
    barrier = pltpu.get_barrier_semaphore()
    for device in devices:
        pl.semaphore_signal(barrier, inc=1, device_id=device, device_id_type=MESH)
    pl.semaphore_wait(barrier, len(devices))


class Place:
    def __init__(self, sp, tp):
        self.sp, self.tp, self.Z, self.Y = sp, tp, sp // 2, tp // 2
        self.s, self.t = lax.axis_index("sp"), lax.axis_index("tp")
        self.z, self.x = self.s // 2, self.s % 2
        self.y, self.c = self.t // 2, self.t % 2
        self.partner = (self.s, self.y * 2 + 1 - self.c)
        self.across = (self.z * 2 + 1 - self.x, self.t)

    def chip_y(self, d):
        return (self.s, lax.rem(self.y + d + self.Y, self.Y) * 2 + self.c)

    def chip_z(self, d):
        return (lax.rem(self.z + d + self.Z, self.Z) * 2 + self.x, self.t)


class LineGather:
    def __init__(self, place, pairs, up_s, up_r, dn_s, dn_r, x_s, x_r):
        self.p, self.pairs = place, pairs
        self.sems = (up_s, up_r, dn_s, dn_r, x_s, x_r)

    def up(self, n, d, own=False):
        p, (own_ref, all_ref) = self.p, self.pairs[n]
        block = p.s - 2 * (d - 1)
        src = own_ref if own else all_ref.at[block]
        return push(src, all_ref.at[block], self.sems[0].at[n, d], self.sems[1].at[n, d], (p.s + 2, p.t))

    def up_wait(self, n, d):
        p, (_, all_ref) = self.p, self.pairs[n]
        ref = all_ref.at[p.s - 2 * d]
        return push(ref, ref, self.sems[0].at[n, d], self.sems[1].at[n, d], (p.s - 2, p.t))

    def dn(self, n, d, own=False):
        p, (own_ref, all_ref) = self.p, self.pairs[n]
        block = p.s + 2 * (d - 1)
        src = own_ref if own else all_ref.at[block]
        return push(src, all_ref.at[block], self.sems[2].at[n, d], self.sems[3].at[n, d], (p.s - 2, p.t))

    def dn_wait(self, n, d):
        p, (_, all_ref) = self.p, self.pairs[n]
        ref = all_ref.at[p.s + 2 * d]
        return push(ref, ref, self.sems[2].at[n, d], self.sems[3].at[n, d], (p.s + 2, p.t))

    def over(self, n, d):
        p, (own_ref, all_ref) = self.p, self.pairs[n]
        block = p.s - 2 * d
        k = d + p.Z - 1
        src = own_ref if d == 0 else all_ref.at[block]
        return push(src, all_ref.at[block], self.sems[4].at[n, k], self.sems[5].at[n, k], p.across)

    def over_wait(self, n, d):
        p, (_, all_ref) = self.p, self.pairs[n]
        ref = all_ref.at[p.z * 2 + 1 - p.x - 2 * d]
        k = d + p.Z - 1
        return push(ref, ref, self.sems[4].at[n, k], self.sems[5].at[n, k], p.across)

    def start(self, count):
        p = self.p

        @pl.when(p.z + 1 < p.Z)
        def _():
            for n in count:
                self.up(n, 1, True).start()

        @pl.when(p.z >= 1)
        def _():
            for n in count:
                self.dn(n, 1, True).start()

        for n in count:
            self.over(n, 0).start()

    def step(self, d):
        p = self.p
        for n in range(len(self.pairs)):

            @pl.when(p.z - d >= 0)
            def _():
                self.up_wait(n, d).wait_recv()

                @pl.when(p.z + 1 < p.Z)
                def _():
                    self.up(n, d + 1).start()

                self.over(n, d).start()

            @pl.when(p.z + d < p.Z)
            def _():
                self.dn_wait(n, d).wait_recv()

                @pl.when(p.z >= 1)
                def _():
                    self.dn(n, d + 1).start()

                self.over(n, -d).start()

    def arrive(self, sign, d):
        for n in range(len(self.pairs)):
            self.over_wait(n, sign * d).wait_recv()

    def side(self, sign, d):
        return self.p.z - d >= 0 if sign > 0 else self.p.z + d < self.p.Z

    def finish(self):
        p = self.p
        for n in range(len(self.pairs)):
            for d in range(p.Z):
                for sign in (1, -1) if d else (1,):

                    @pl.when(self.side(sign, d))
                    def _():
                        self.over(n, sign * d).wait_send()

            for d in range(1, p.Z):

                @pl.when(jnp.logical_and(p.z - d + 1 >= 0, p.z + 1 < p.Z))
                def _():
                    self.up(n, d).wait_send()

                @pl.when(jnp.logical_and(p.z + d - 1 < p.Z, p.z >= 1))
                def _():
                    self.dn(n, d).wait_send()


def line_sems(p_z, n):
    return [pltpu.SemaphoreType.DMA((n, p_z + 1))] * 4 + [pltpu.SemaphoreType.DMA((n, 2 * p_z))] * 2


class PairScatter:
    def __init__(self, p, part, first, summed, second, fs, fr, ss, sr):
        self.p, self.part, self.first, self.summed, self.second = p, part, first, summed, second
        self.sems = (fs, fr, ss, sr)
        self.started = []

    def start(self):
        p = self.p
        for d in range(p.Y):
            y = lax.rem(p.y + d, p.Y)
            copy = push(
                self.part(y * 2 + 1 - p.c), self.first.at[d], self.sems[0].at[d], self.sems[1].at[d], p.partner
            )
            copy.start()
            self.started.append(copy)

    def middle(self):
        p = self.p
        for d in list(range(1, p.Y)) + [0]:
            y = lax.rem(p.y + d, p.Y)
            self.started[d].wait_recv()
            total = self.part(y * 2 + p.c)[...].astype(F32) + self.first[d].astype(F32)
            self.summed[d] = total.astype(BF)
            if d:
                copy = push(
                    self.summed.at[d], self.second.at[d], self.sems[2].at[d], self.sems[3].at[d], p.chip_y(d)
                )
                copy.start()
                self.started.append(copy)

    def finish(self):
        p = self.p
        total = self.part(p.t)[...].astype(F32) + self.first[0].astype(F32)
        for d in range(1, p.Y):
            self.started[p.Y + d - 1].wait_recv()
            total = total + self.second[d].astype(F32)
        for copy in self.started:
            copy.wait_send()
        return total


class PairGather:
    def __init__(self, p, own, spot, ys, yr, ps, pr):
        self.p, self.own, self.spot, self.sems = p, own, spot, (ys, yr, ps, pr)
        self.started = []

    def start(self):
        p = self.p
        for d in range(1, p.Y):
            copy = push(self.own, self.spot(p.t), self.sems[0].at[d], self.sems[1].at[d], p.chip_y(d))
            copy.start()
            self.started.append(copy)
        copy = push(self.own, self.spot(p.t), self.sems[2].at[0], self.sems[3].at[0], p.partner)
        copy.start()
        self.started.append(copy)

    def forward(self):
        p = self.p
        for d in range(1, p.Y):
            ref = self.spot(lax.rem(p.y - d + p.Y, p.Y) * 2 + p.c)
            push(ref, ref, self.sems[0].at[d], self.sems[1].at[d], p.chip_y(-d)).wait_recv()
            copy = push(ref, ref, self.sems[2].at[d], self.sems[3].at[d], p.partner)
            copy.start()
            self.started.append(copy)

    def arrive(self):
        p = self.p
        for d in range(p.Y):
            ref = self.spot(lax.rem(p.y - d + p.Y, p.Y) * 2 + 1 - p.c)
            push(ref, ref, self.sems[2].at[d], self.sems[3].at[d], p.partner).wait_recv()

    def finish(self):
        for copy in self.started:
            copy.wait_send()


def layer_kernel(
    sp, tp, shift_base,
    raw, to, src, gain, saved, offs, wq_h, wk_h, wv_h, wo_h,
    flat_all, src_out, tgt_out, cols_all,
    tn, pieces, wq, wk, wv, wo, tn_all, to_all, src_all, cols, tn_b, to_b,
    q_all, hg_all, small_all, k_s, v_s, p_s, d_s, part, kf, vf, sg,
    xr, xz, zr, sg1, sg2, sg3, ng, ng1, ng2, ng3,
    wsem, loc, es, er, *sems
):
    p = Place(sp, tp)
    pair_sems = [sems[4 * i : 4 * i + 4] for i in range(6)]
    xs_s, xs_r, zs_s, zs_r = sems[24:28]
    line_a, line_b = sems[28:34], sems[34:40]
    rows, block = raw.shape[0], saved.shape[0]
    width, model = wq.shape[1], wq.shape[0]
    heads = width // HEAD_DIM
    scale = HEAD_DIM ** (-0.5)
    loads = [
        pltpu.make_async_copy(h, v, wsem.at[i])
        for i, (h, v) in enumerate(((wq_h, wq), (wo_h, wo), (wk_h, wk), (wv_h, wv)))
    ]
    for copy in loads:
        copy.start()
    raw_value, gain_value = raw[...].astype(F32), gain[...].astype(F32).reshape(1, model)
    inverse = lax.rsqrt(jnp.mean(raw_value * raw_value, axis=1, keepdims=True) + EPSILON)
    normed_value = (raw_value * inverse * gain_value).astype(BF)
    tn[...] = normed_value
    slice_width = model // sp
    for s in range(sp):
        pieces[s] = normed_value[:, s * slice_width : (s + 1) * slice_width]
    greet(
        [p.partner]
        + [p.chip_y(d) for d in range(1, p.Y)]
        + [(lax.rem(p.s + e, sp), p.t) for e in range(1, sp)]
    )
    g_tn = PairGather(p, tn, lambda t: tn_all.at[t], *pair_sems[0])
    g_to = PairGather(p, to, lambda t: to_all.at[t], *pair_sems[1])
    g_src = PairGather(p, src, lambda t: src_all.at[t], *pair_sems[2])
    g_cols = PairGather(p, cols, lambda t: cols_all.at[:, t], *pair_sems[3])
    for g in (g_tn, g_to, g_src):
        g.start()
    swaps = []
    for e in range(1, sp):
        s = lax.rem(p.s + e, sp)
        copy = push(pieces.at[s], cols.at[p.s], es.at[e], er.at[e], (s, p.t))
        copy.start()
        swaps.append(copy)
    mine = [
        pltpu.make_async_copy(tn, tn_all.at[p.t], loc.at[0]),
        pltpu.make_async_copy(to, to_all.at[p.t], loc.at[1]),
        pltpu.make_async_copy(src, src_all.at[p.t], loc.at[2]),
        pltpu.make_async_copy(pieces.at[p.s], cols.at[p.s], loc.at[3]),
    ]
    for copy in mine:
        copy.start()
    for copy in mine:
        copy.wait()
    tile = min(width, 256)
    gather = LineGather(
        p, ((q_all.at[p.s], q_all), (hg_all.at[p.s], hg_all), (small_all.at[p.s], small_all)), *line_a
    )

    g_tn.forward()
    g_to.forward()
    g_tn.arrive()
    for t in range(tp):
        tn_b[t * rows : (t + 1) * rows, :] = tn_all[t]
    loads[0].wait()
    for j in range(0, width, tile):
        q_all[p.s, :, j : j + tile] = jnp.dot(
            tn_b[...], wq[:, j : j + tile], preferred_element_type=F32
        ).astype(BF)
    gather.start((0,))
    g_to.arrive()
    for t in range(tp):
        to_b[t * rows : (t + 1) * rows, :] = to_all[t]
    loads[1].wait()
    lane = lax.broadcasted_iota(jnp.int32, (block, 128), 1)
    pick = lax.broadcasted_iota(jnp.int32, (heads, 128), 0) == lax.broadcasted_iota(jnp.int32, (heads, 128), 1)
    small = lax.dot_general(
        offs[...].astype(F32), pick.astype(F32), (((0,), (0,)), ((), ())), precision=lax.Precision.HIGHEST,
        preferred_element_type=F32,
    )
    for h in range(heads):
        cut = slice(h * HEAD_DIM, (h + 1) * HEAD_DIM)
        part_h = contract_last(to_b[...], wo[cut, :]).astype(BF)
        hg_all[p.s, :, cut] = part_h
        delta = jnp.sum(part_h.astype(F32) * saved[:, cut].astype(F32), axis=1, keepdims=True)
        small = jnp.where(lane == heads + h, delta, small)
    small_all[p.s] = small.astype(BF)
    gather.start((1, 2))

    g_src.forward()
    g_src.arrive()
    gather.step(1)
    source_count = k_s.shape[0]
    loads[2].wait()
    loads[3].wait()

    @pl.loop(0, width // tile)
    def _(j):
        cut = pl.ds(pl.multiple_of(j * tile, tile), tile)
        rows_value = src_all[...].reshape(source_count, model)
        k_s[:, cut] = jnp.dot(rows_value, wk[:, cut], preferred_element_type=F32).astype(BF)
        v_s[:, cut] = jnp.dot(rows_value, wv[:, cut], preferred_element_type=F32).astype(BF)

    for e in range(1, sp):
        s = lax.rem(p.s - e + sp, sp)
        push(cols.at[s], cols.at[s], es.at[e], er.at[e], (s, p.t)).wait_recv()
    g_cols.start()
    keep = pltpu.make_async_copy(cols, cols_all.at[:, p.t], loc.at[4])
    keep.start()

    def into(k):
        z = lax.rem(p.z + k, p.Z)
        return push(part.at[z * 2 + 1 - p.x], xr.at[k], xs_s.at[k], xs_r.at[k], p.across)

    def attend(z):
        pair = pl.ds(2 * z, 2)
        spot = pl.ds(pl.multiple_of(z * (2 * block), 2 * block), 2 * block)
        tiny = small_all[pair].reshape(2 * block, 128).astype(F32)
        for h in range(heads):
            cut = slice(h * HEAD_DIM, (h + 1) * HEAD_DIM)
            q_h = q_all[pair, :, cut].reshape(2 * block, HEAD_DIM)
            g_h = hg_all[pair, :, cut].reshape(2 * block, HEAD_DIM)
            prob = jnp.exp(contract_last(q_h, k_s[:, cut]) * scale - (shift_base + tiny[:, h : h + 1]))
            grad = contract_last(g_h, v_s[:, cut])
            score = (prob * (grad - tiny[:, heads + h : heads + h + 1]) * scale).astype(BF)
            p_s[h, spot, :] = prob.astype(BF)
            d_s[h, spot, :] = score
            term = jnp.dot(score, k_s[:, cut], preferred_element_type=F32).astype(BF)
            part[pair, :, cut] = term.reshape(2, block, HEAD_DIM)

    def reached(sign, d):
        gather.arrive(sign, d)
        attend(p.z - sign * d)
        into((-sign * d) % p.Z).start()

    for d in range(1, p.Z):
        if d > 1:
            gather.step(d)
        for sign in (1, -1) if d > 1 else (1,):

            @pl.when(gather.side(sign, d - 1))
            def _():
                reached(sign, d - 1)

        if d == 1:
            g_cols.forward()
    for sign in (1, -1):

        @pl.when(gather.side(sign, p.Z - 1))
        def _():
            reached(sign, p.Z - 1)

    order = sorted(range(1, p.Z), key=lambda k: min(k, p.Z - k))
    hops = {}

    def relay(k):
        into(k).wait_recv()
        z = lax.rem(p.z + k, p.Z)
        xz[k] = (part[z * 2 + p.x].astype(F32) + xr[k].astype(F32)).astype(BF)
        hops[k] = push(xz.at[k], zr.at[k], zs_s.at[k], zs_r.at[k], p.chip_z(k))
        hops[k].start()

    for k in order[:1]:
        relay(k)
    count = sp * block

    for h in range(heads):
        cut = slice(h * HEAD_DIM, (h + 1) * HEAD_DIM)
        dims = (((0,), (0,)), ((), ()))
        q_h = q_all[:, :, cut].reshape(count, HEAD_DIM)
        g_h = hg_all[:, :, cut].reshape(count, HEAD_DIM)
        kf[:, cut] = lax.dot_general(d_s[h], q_h, dims, preferred_element_type=F32).astype(BF)
        vf[:, cut] = lax.dot_general(p_s[h], g_h, dims, preferred_element_type=F32).astype(BF)
    for k in order[1:2]:
        relay(k)
    stile = min(model, 256)

    def source_term(j):
        cut = pl.ds(pl.multiple_of(j * stile, stile), stile)
        value = contract_last(kf[...], wk[cut, :]) + contract_last(vf[...], wv[cut, :])
        sg[:, :, cut] = value.astype(BF).reshape(tp, source_count // tp, stile)

    half = model // stile // 2
    pl.loop(0, half)(source_term)
    for k in order[2:]:
        relay(k)
    pl.loop(half, model // stile)(source_term)
    source = PairScatter(p, lambda t: sg.at[t], sg1, sg2, sg3, *pair_sems[4])
    source.start()
    source.middle()
    into(0).wait_recv()
    total = part[p.s].astype(F32) + xr[0].astype(F32)
    for k in order:
        hops[k].wait_recv()
        total = total + zr[k].astype(F32)
    flat = total.astype(BF)
    flat_all[p.s] = flat
    spread = LineGather(p, ((flat_all.at[p.s], flat_all),), *line_b)
    spread.start((0,))
    for j in range(0, model, stile):
        columns = contract_last(flat, wq[j : j + stile, :]).astype(BF)
        for t in range(tp):
            ng[t, :, j : j + stile] = columns[t * rows : (t + 1) * rows]
    normed = PairScatter(p, lambda t: ng.at[t], ng1, ng2, ng3, *pair_sems[5])
    normed.start()
    for d in range(1, p.Z):
        spread.step(d)
        if d == 1:
            normed.middle()
    src_out[...] = source.finish()
    raw_value, gain_value = raw[...].astype(F32), gain[...].astype(F32).reshape(1, model)
    inverse = lax.rsqrt(jnp.mean(raw_value * raw_value, axis=1, keepdims=True) + EPSILON)
    scaled = normed.finish() * gain_value
    tgt_out[...] = inverse * scaled - raw_value * (inverse * inverse * inverse) * jnp.mean(
        scaled * raw_value, axis=1, keepdims=True
    )
    g_cols.arrive()
    for d in range(p.Z):
        for sign in (1, -1) if d else (1,):

            @pl.when(spread.side(sign, d))
            def _():
                spread.arrive(sign, d)

    gather.finish()
    spread.finish()
    for g in (g_tn, g_to, g_src, g_cols):
        g.finish()
    for copy in swaps:
        copy.wait_send()
    keep.wait()
    for k in range(p.Z):
        into(k).wait_send()
    for k in order:
        hops[k].wait_send()


def body(
    target_rows,
    source_rows,
    norm_gain,
    query_weight,
    key_weight,
    value_weight,
    output_weight,
    saved_output,
    norm_offset,
    output_grad,
):
    tp, sp = lax.axis_size("tp"), lax.axis_size("sp")
    Z, Y = sp // 2, tp // 2
    model, width = query_weight.shape
    heads = width // HEAD_DIM
    rows, srows = target_rows.shape[0], source_rows.shape[0]
    block = rows * tp
    count = block * sp
    source_count = srows * tp
    shift_base = math.log(source_count * sp)
    slice_width = model // sp
    dma = pltpu.SemaphoreType.DMA

    vm = pltpu.VMEM
    whole = pl.BlockSpec(memory_space=pl.ANY)
    flat_all, source_grad, target_grad, cols_all = pl.pallas_call(
        functools.partial(layer_kernel, sp, tp, shift_base),
        out_shape=[
            jax.ShapeDtypeStruct((sp, block, width), BF),
            jax.ShapeDtypeStruct((srows, model), F32),
            jax.ShapeDtypeStruct((rows, model), F32),
            jax.ShapeDtypeStruct((sp, tp, rows, slice_width), BF),
        ],
        in_specs=[VMEM] * 6 + [whole] * 4,
        out_specs=[VMEM] * 4,
        scratch_shapes=[vm((rows, model), BF), vm((sp, rows, slice_width), BF)]
        + [vm((model, width), BF)] * 3
        + [vm((width, model), BF)]
        + [vm((tp, rows, model), BF)] * 2
        + [vm((tp, srows, model), BF), vm((sp, rows, slice_width), BF)]
        + [vm((block, model), BF)] * 2
        + [vm((sp, block, width), BF)] * 2
        + [vm((sp, block, 128), BF)]
        + [vm((source_count, width), BF)] * 2
        + [vm((heads, count, source_count), BF)] * 2
        + [vm((sp, block, width), BF)]
        + [vm((source_count, width), BF)] * 2
        + [vm((tp, srows, model), BF)]
        + [vm((Z, block, width), BF)] * 3
        + [vm((Y, srows, model), BF)] * 3
        + [vm((tp, rows, model), BF)]
        + [vm((Y, rows, model), BF)] * 3
        + [dma((4,)), dma((5,)), dma((sp,)), dma((sp,))]
        + [dma((Y,))] * 24
        + [dma((Z,))] * 4
        + line_sems(Z, 3)
        + line_sems(Z, 1),
        name="layer_kernel",
        compiler_params=pltpu.CompilerParams(
            collective_id=1, has_side_effects=True, vmem_limit_bytes=58 * 2**20
        ),
    )(
        target_rows,
        output_grad,
        source_rows,
        norm_gain,
        saved_output,
        norm_offset.T,
        query_weight,
        key_weight,
        value_weight,
        output_weight,
    )
    weight_grad = lax.dot_general(
        cols_all.reshape(count, slice_width),
        flat_all.reshape(count, width),
        (((0,), (0,)), ((), ())),
        preferred_element_type=F32,
    )
    return (target_grad, source_grad, weight_grad)


class Net:
    def __init__(self, send, recv):
        self.send, self.recv, self.ids = send, recv, {}
        self.free, self.started = list(range(send.shape[0])), []

    def _copy(self, name, src, dst, device, slot=0):
        n = self.ids.setdefault(TOGETHER.get(name, name), len(self.ids))
        return push(src, dst, self.send.at[slot], self.recv.at[n], device)

    def go(self, name, src, dst, device):
        if not self.free:
            self.drain(1)
        slot = self.free.pop(0)
        copy = self._copy(name, src, dst, device, slot)
        copy.start()
        self.started.append((slot, copy))

    def same(self, name, ref, device):
        self.go(name, ref, ref, device)

    def wait(self, name, landed, device):
        self._copy(name, landed, landed, device).wait_recv()

    def drain(self, count=None):
        count = len(self.started) if count is None else count
        for slot, copy in self.started[:count]:
            copy.wait_send()
            self.free.append(slot)
        self.started = self.started[count:]


SENDS = 26
TOGETHER = {f"p{n:03b}": "p" for n in range(8)}
for first, second in (("q0X", "q1X"), ("g0X", "g1X"), ("m0X", "m1X"), ("q2X", "q3X"), ("g2X", "g3X"), ("m2X", "m3X"), ("cVB", "cVA"), ("dVB", "dVA"), ("cYA", "cYB")):
    TOGETHER[second] = first
Y_FIRST = (False, True, True, True)


def grid_kernel(
    sp, tp, shift_base,
    raw_h, to_h, src_h, gain_h, saved_h, offs_h, wq_h, wk_h, wv_h, wo_h,
    ws_h, src_h_out, tgt_h_out,
    raw, gain, saved, offs, src_out, tgt_out,
    tn_all, to_all, src_all, pieces, cols, q_st, g_st, sm_st, q_all, g_all, sm_all,
    wq, wkv, wo, kv, p_s, d_s, part, xr, xs, ur, flat_all, fl, kv_sum, kvf,
    sg, sd, ss, es, fs, fr, na, ng, nr, wt,
    wsem, osem, send, recv
):
    p = Place(sp, tp)
    s, t, y, c, x = p.s, p.t, p.y, p.c, p.x
    u, v = p.z // 2, p.z % 2
    net = Net(send, recv)

    def at(u, v, x):
        return ((u * 2 + v) * 2 + x, t)

    C, Y, V, X, U = p.partner, p.chip_y(1), at(u, 1 - v, x), at(u, v, 1 - x), at(1 - u, v, x)
    ty, tc, tyc = (1 - y) * 2 + c, y * 2 + 1 - c, (1 - y) * 2 + 1 - c
    others = [
        (a, b, d, u + a - 2 * u * a, v + b - 2 * v * b, x + d - 2 * x * d)
        for a in range(2) for b in range(2) for d in range(2) if a + b + d
    ]
    barrier = pltpu.get_barrier_semaphore()
    D = (s, tyc)
    friends = [C, Y, D] + [at(*o[3:]) for o in others]
    for device in friends:
        pl.semaphore_signal(barrier, inc=1, device_id=device, device_id_type=MESH)
    rows, block, srows = raw.shape[0], saved.shape[0], src_h.shape[0]
    model, width = wq.shape
    heads = width // HEAD_DIM
    hh, half = heads // 2, width // 2
    sblock = srows * tp
    sw = model // sp
    quarters = len(Y_FIRST)
    mq = model // quarters
    scale = HEAD_DIM ** (-0.5)
    mine = pl.ds(pl.multiple_of(v * half, half), half)
    loads = [
        pltpu.make_async_copy(h, w, wsem.at[i])
        for i, (h, w) in enumerate(
            (
                (wq_h, wq), (wo_h, wo), (wk_h.at[:, mine], wkv.at[:, :half]), (wv_h.at[:, mine], wkv.at[:, half:]),
                (raw_h, raw), (gain_h, gain), (src_h, src_all.at[v, t]), (to_h, to_all.at[t]),
                (saved_h, saved), (offs_h, offs),
            )
        )
    ]
    for n in (4, 5, 6, 7, 0, 1, 8, 9, 2, 3):
        loads[n].start()
    loads[4].wait()
    loads[5].wait()
    raw_value, gain_value = raw[...].astype(F32), gain[...].astype(F32).reshape(1, model)
    inverse = lax.rsqrt(jnp.mean(raw_value * raw_value, axis=1, keepdims=True) + EPSILON)
    normed_value = (raw_value * inverse * gain_value).astype(BF)
    tn_all[t] = normed_value
    for a in range(2):
        for b in range(2):
            for k in range(2):
                n = (2 * a + k) * 2 + b
                pieces[a, b, :, k * sw : (k + 1) * sw] = normed_value[:, n * sw : (n + 1) * sw]
    loads[6].wait()
    loads[7].wait()
    pl.semaphore_wait(barrier, len(friends))
    A, B = pl.ds(0, srows // 2), pl.ds(srows // 2, srows // 2)

    net.same("tnY", tn_all.at[t], Y)
    net.same("sVB", src_all.at[v, t, B], V)
    net.same("tnC", tn_all.at[t], C)
    net.same("toY", to_all.at[t], Y)
    net.same("toC", to_all.at[t], C)
    net.same("sYA", src_all.at[v, t, A], Y)
    net.same("sVA", src_all.at[v, t, A], V)
    net.same("sYB", src_all.at[v, t, B], Y)
    net.same("sC", src_all.at[v, t], C)
    net.wait("tnY", tn_all.at[ty], Y)
    net.same("tnF", tn_all.at[ty], C)
    net.wait("toY", to_all.at[ty], Y)
    net.same("toF", to_all.at[ty], C)
    net.wait("tnC", tn_all.at[tc], C)
    net.wait("tnF", tn_all.at[tyc], C)
    loads[0].wait()
    tn_b = tn_all[...].reshape(block, model)
    for k in range(2):
        for j in range(0, half, HEAD_DIM):
            q_st[k, :, j : j + HEAD_DIM] = jnp.dot(
                tn_b, wq[:, k * half + j : k * half + j + HEAD_DIM], preferred_element_type=F32
            ).astype(BF)
    net.go("qV", q_st.at[1 - v], q_all.at[u, x, v], V)
    q_all[u, x, v] = q_st[v]
    net.same("q0U", q_all.at[u, x, v], U)
    net.same("q0X", q_all.at[u, x, v], X)
    net.wait("sVB", src_all.at[1 - v, t, B], V)
    net.same("fVB", src_all.at[1 - v, t, B], Y)
    net.same("cVB", src_all.at[1 - v, t, B], C)
    net.wait("toC", to_all.at[tc], C)
    net.wait("toF", to_all.at[tyc], C)
    loads[1].wait()
    loads[8].wait()
    loads[9].wait()
    to_b = to_all[...].reshape(block, model)
    products = []
    for n in range(heads):
        cut = slice(n * HEAD_DIM, (n + 1) * HEAD_DIM)
        part_h = contract_last(to_b, wo[cut, :]).astype(BF)
        g_st[n // hh, :, n % hh * HEAD_DIM : (n % hh + 1) * HEAD_DIM] = part_h
        products.append(part_h.astype(F32) * saved[:, cut].astype(F32))
    net.go("gV", g_st.at[1 - v], g_all.at[u, x, v], V)
    g_all[u, x, v] = g_st[v]
    net.same("g0U", g_all.at[u, x, v], U)
    net.same("g0X", g_all.at[u, x, v], X)
    lines, lanes = sm_st.shape[1], 2 * block
    place = (
        lax.broadcasted_iota(jnp.int32, (block, lanes), 1)
        == lax.broadcasted_iota(jnp.int32, (block, lanes), 0) + v * block
    ).astype(F32)
    spread = jnp.dot(offs[...].astype(F32), place, precision=lax.Precision.HIGHEST, preferred_element_type=F32)
    product = jnp.concatenate(products, axis=1)
    line = lax.broadcasted_iota(jnp.int32, (2 * lines, width), 0)
    head = lax.broadcasted_iota(jnp.int32, (2 * lines, width), 1) // HEAD_DIM
    pick = (line == head // hh * lines + hh + head % hh).astype(BF)
    deltas = 0.0
    for term in range(3):
        narrow = product.astype(BF)
        product = product - narrow.astype(F32)
        padded = jnp.concatenate(
            [jnp.where(v == 0, narrow, jnp.zeros_like(narrow)), jnp.where(v == 1, narrow, jnp.zeros_like(narrow))],
            axis=0,
        )
        deltas = deltas + contract_last(pick, padded)
    line = lax.broadcasted_iota(jnp.int32, (lines, lanes), 0)
    for k in range(2):
        small = deltas[k * lines : (k + 1) * lines]
        for h in range(hh):
            n = k * hh + h
            small = jnp.where(line == h, jnp.broadcast_to(spread[n : n + 1], small.shape), small)
        sm_st[k] = small.astype(BF)
    net.go("mV", sm_st.at[1 - v], sm_all.at[u, x, v], V)
    sm_all[u, x, v] = sm_st[v]
    net.same("m0U", sm_all.at[u, x, v], U)
    net.same("m0X", sm_all.at[u, x, v], X)

    net.wait("sYA", src_all.at[v, ty, A], Y)
    net.same("cYA", src_all.at[v, ty, A], C)
    net.wait("qV", q_all.at[u, x, 1 - v], V)
    net.same("q1U", q_all.at[u, x, 1 - v], U)
    net.same("q1X", q_all.at[u, x, 1 - v], X)
    net.wait("sVA", src_all.at[1 - v, t, A], V)
    net.same("fVA", src_all.at[1 - v, t, A], Y)
    net.same("cVA", src_all.at[1 - v, t, A], C)
    net.wait("gV", g_all.at[u, x, 1 - v], V)
    net.same("g1U", g_all.at[u, x, 1 - v], U)
    net.same("g1X", g_all.at[u, x, 1 - v], X)
    net.wait("sYB", src_all.at[v, ty, B], Y)
    net.same("cYB", src_all.at[v, ty, B], C)
    net.wait("mV", sm_all.at[u, x, 1 - v], V)
    net.same("m1U", sm_all.at[u, x, 1 - v], U)
    net.same("m1X", sm_all.at[u, x, 1 - v], X)
    def project(k, y):
        count = 2 * srows
        spot = pl.ds(pl.multiple_of(k * sblock + y * count, count), count)

        @pl.loop(0, 2)
        def _(j):
            cut = pl.ds(pl.multiple_of(j * half, half), half)
            value = src_all[k, pl.ds(2 * y, 2)].reshape(count, model)
            kv[spot, cut] = jnp.dot(value, wkv[:, cut], preferred_element_type=F32).astype(BF)

    net.wait("sC", src_all.at[v, tc], C)
    loads[2].wait()
    loads[3].wait()
    net.wait("fVB", src_all.at[1 - v, ty, B], Y)
    net.same("dVB", src_all.at[1 - v, ty, B], C)
    project(v, y)
    spot = (u * 2 + x) * 2 + v
    for a, b, d, u2, v2, x2 in others:
        net.go(f"p{a}{b}{d}", pieces.at[u2, x2], cols.at[spot, t], at(u2, v2, x2))
    cols[spot, t] = pieces[u, x]
    net.wait("q0U", q_all.at[1 - u, x, v], U)
    net.same("q2X", q_all.at[1 - u, x, v], X)
    net.wait("cVB", src_all.at[1 - v, tc], C)
    project(1 - v, y)
    net.wait("cYA", src_all.at[v, tyc], C)
    net.wait("g0U", g_all.at[1 - u, x, v], U)
    net.same("g2X", g_all.at[1 - u, x, v], X)
    project(v, 1 - y)
    net.wait("fVA", src_all.at[1 - v, ty, A], Y)
    net.same("dVA", src_all.at[1 - v, ty, A], C)
    net.wait("m0U", sm_all.at[1 - u, x, v], U)
    net.same("m2X", sm_all.at[1 - u, x, v], X)
    net.wait("q1U", q_all.at[1 - u, x, 1 - v], U)
    net.same("q3X", q_all.at[1 - u, x, 1 - v], X)
    net.wait("dVB", src_all.at[1 - v, tyc], C)
    project(1 - v, 1 - y)

    def attend(w, after):
        little = sm_all[w].astype(F32)
        little = jnp.concatenate([little[0, 0] + little[0, 1], little[1, 0] + little[1, 1]], axis=1)
        for h in range(hh):
            cut = slice(h * HEAD_DIM, (h + 1) * HEAD_DIM)
            q_h = q_all[w, :, :, :, cut].reshape(4 * block, HEAD_DIM)
            g_h = g_all[w, :, :, :, cut].reshape(4 * block, HEAD_DIM)
            prob = jnp.exp(contract_last(kv[:, cut], q_h) * scale - (shift_base + little[h : h + 1]))
            grad = contract_last(kv[:, half + h * HEAD_DIM : half + (h + 1) * HEAD_DIM], g_h)
            score = (prob * (grad - little[hh + h : hh + h + 1]) * scale).astype(BF)
            p_s[h] = prob.astype(BF)
            d_s[h] = score
            term = lax.dot_general(score, kv[:, cut], (((0,), (0,)), ((), ())), preferred_element_type=F32)
            part[w, :, h] = term.astype(BF).reshape(2, 2, block, HEAD_DIM)
            after(h)

    def source_terms(w):
        for h in range(hh):
            cut = slice(h * HEAD_DIM, (h + 1) * HEAD_DIM)
            q_h = q_all[w, :, :, :, cut].reshape(4 * block, HEAD_DIM)
            g_h = g_all[w, :, :, :, cut].reshape(4 * block, HEAD_DIM)
            yield cut, jnp.dot(d_s[h], q_h, preferred_element_type=F32)
            cut = slice(half + h * HEAD_DIM, half + (h + 1) * HEAD_DIM)
            yield cut, jnp.dot(p_s[h], g_h, preferred_element_type=F32)

    def send_near(h):
        net.go(f"a{h}X", part.at[u, 1 - x, h], xr.at[0, h], X)

    def send_far(h):
        for k in range(2):
            net.go(f"b{h}{k}X", part.at[1 - u, 1 - x, h, k], xr.at[1, h, k], X)

    net.wait("q0X", q_all.at[u, 1 - x], X)
    net.wait("m0X", sm_all.at[u, 1 - x], X)
    net.wait("g0X", g_all.at[u, 1 - x], X)
    net.wait("g1U", g_all.at[1 - u, x, 1 - v], U)
    net.same("g3X", g_all.at[1 - u, x, 1 - v], X)
    net.wait("m1U", sm_all.at[1 - u, x, 1 - v], U)
    net.same("m3X", sm_all.at[1 - u, x, 1 - v], X)
    attend(u, send_near)
    for cut, value in source_terms(u):
        kv_sum[:, cut] = value

    def near(h):
        net.wait(f"a{h}X", xr.at[0, h], X)
        xs[0, h] = (part[u, x, h].astype(F32) + xr[0, h].astype(F32)).astype(BF)
        net.go(f"s{h}U", xs.at[0, h], ur.at[1, h], U)

    net.wait("q2X", q_all.at[1 - u, 1 - x], X)
    net.wait("m2X", sm_all.at[1 - u, 1 - x], X)
    net.wait("g2X", g_all.at[1 - u, 1 - x], X)
    attend(1 - u, send_far)
    near(0)
    for cut, value in source_terms(1 - u):
        kvf[:, cut] = (kv_sum[:, cut] + value).astype(BF)
    for h in range(1, hh):
        near(h)
    net.wait("p", cols.at[: len(others), t], V)
    net.same("kY", cols.at[:, t], Y)
    net.same("kC", cols.at[:, t], C)
    stile = min(mq, 256)

    def source(n):
        for j in range(0, mq, stile):
            value = contract_last(kvf[...], wkv[n * mq + j : n * mq + j + stile, :]).astype(BF)
            sg[n, :, :, :, j : j + stile] = value.reshape(4, 2, srows, stile)
        net.go(f"d{n}", sg.at[n, :, 1 - c], sd.at[n], C)

    def source_sum(n):
        net.wait(f"d{n}", sd.at[n], C)
        for k in range(4):
            ss[n, k] = (sg[n, k, c].astype(F32) + sd[n, k].astype(F32)).astype(BF)
        net.go(f"e{n}1", ss.at[n, 2 * (1 - v) + 1 - y], es.at[n, 1], Y if Y_FIRST[n] else V)

    def source_rest(n):
        first, near = (Y, 2 * v + 1 - y) if Y_FIRST[n] else (V, 2 * (1 - v) + y)
        net.go(f"e{n}0", ss.at[n, near], es.at[n, 0], first)

    def source_pass(n):
        first, last = (Y, V) if Y_FIRST[n] else (V, Y)
        keep = 2 * (1 - v) + y if Y_FIRST[n] else 2 * v + 1 - y
        net.wait(f"e{n}1", es.at[n, 1], first)
        fs[n] = (ss[n, keep].astype(F32) + es[n, 1].astype(F32)).astype(BF)
        net.go(f"f{n}", fs.at[n], fr.at[n], last)

    kept = []

    def keep(ref, out):
        copy = pltpu.make_async_copy(ref, out, osem.at[len(kept)])
        copy.start()
        kept.append(copy)

    def source_end(n):
        first, last = (Y, V) if Y_FIRST[n] else (V, Y)
        net.wait(f"e{n}0", es.at[n, 0], first)
        net.wait(f"f{n}", fr.at[n], last)
        src_out[n] = ss[n, 2 * v + y].astype(F32) + es[n, 0].astype(F32) + fr[n].astype(F32)
        keep(src_out.at[n], src_h_out.at[n])

    def far(h):
        for k in range(2):
            net.wait(f"b{h}{k}X", xr.at[1, h, k], X)
            xs[1, h, k] = (part[1 - u, x, h, k].astype(F32) + xr[1, h, k].astype(F32)).astype(BF)
            net.go(f"z{h}{k}U", xs.at[1, h, k], ur.at[0, h, k], U)

    def flat_far(h):
        net.wait(f"s{h}U", ur.at[1, h], U)
        flat_all[1 - u, x, h] = (xs[1, h].astype(F32) + ur[1, h].astype(F32)).astype(BF)
        net.same(f"w{h}X", flat_all.at[1 - u, x, h], X)

    def flat_near(h):
        for k in range(2):
            net.wait(f"z{h}{k}U", ur.at[0, h, k], U)
            flat_all[u, x, h, k] = (xs[0, h, k].astype(F32) + ur[0, h, k].astype(F32)).astype(BF)
            net.same(f"r{h}{k}X", flat_all.at[u, x, h, k], X)
        net.go(f"n{h}V", flat_all.at[u, x, h, 1 - v], fl.at[v, h], V)
        fl[v, h] = flat_all[u, x, h, v]

    def weight(h):
        for k in range(2):
            net.wait(f"r{h}{k}X", flat_all.at[u, 1 - x, h, k], X)
        net.wait(f"w{h}X", flat_all.at[1 - u, 1 - x, h], X)
        flat_h = flat_all[:, :, h].reshape(sp * block, HEAD_DIM)
        for k in range(2):
            wt[h, k] = lax.dot_general(
                cols[:, :, :, k * sw : (k + 1) * sw].reshape(sp * block, sw), flat_h,
                (((0,), (0,)), ((), ())), preferred_element_type=F32,
            ).astype(BF)
        net.go(f"W{h}", wt.at[h, 1 - v], ws_h.at[v, h], V)
        keep(wt.at[h, v], ws_h.at[v, h])

    ntile = min(model, 256)

    def normed_term(h, k, own):
        if not own:
            net.wait(f"n{h}V", fl.at[k, h], V)
        cut = pl.ds(pl.multiple_of((k * hh + h) * HEAD_DIM, HEAD_DIM), HEAD_DIM)
        for j in range(0, model, ntile):
            columns = contract_last(fl[k, h], wq[j : j + ntile, cut])
            if not own or h:
                columns = columns + na[:, j : j + ntile]
            if own or h < hh - 1:
                na[:, j : j + ntile] = columns
            else:
                ng[:, :, j : j + ntile] = columns.astype(BF).reshape(tp, rows, ntile)

    source(0)
    far(0)
    source(1)
    for h in range(1, hh):
        far(h)
    source(2)
    source_sum(0)
    source_rest(0)
    source(3)
    source_sum(1)
    source_sum(2)
    net.wait("kY", cols.at[:, ty], Y)
    net.same("kF", cols.at[:, ty], C)
    source_sum(3)
    for n in range(1, quarters):
        source_rest(n)
    source_pass(1)
    for h in range(hh):
        flat_far(h)
    flat_near(0)
    source_pass(0)
    normed_term(0, v, True)
    net.wait("kC", cols.at[:, tc], C)
    net.wait("kF", cols.at[:, tyc], C)
    for h in range(1, hh):
        flat_near(h)
        normed_term(h, v, True)
    source_pass(2)
    weight(0)
    source_pass(3)
    for h in range(1, hh):
        weight(h)
    for h in range(hh):
        normed_term(h, 1 - v, False)
    owners = ((tyc, D), (ty, Y), (tc, C))
    for n, (k, device) in enumerate(owners):
        net.go(f"o{n}", ng.at[k], nr.at[n], device)
    for n in (0, 1, 2, 3):
        source_end(n)
    raw_value, gain_value = raw[...].astype(F32), gain[...].astype(F32).reshape(1, model)
    inverse = lax.rsqrt(jnp.mean(raw_value * raw_value, axis=1, keepdims=True) + EPSILON)
    scaled = ng[t].astype(F32)
    for n, (_, device) in enumerate(owners):
        net.wait(f"o{n}", nr.at[n], device)
        scaled = scaled + nr[n].astype(F32)
    scaled = scaled * gain_value
    tgt_out[...] = inverse * scaled - raw_value * (inverse * inverse * inverse) * jnp.mean(
        scaled * raw_value, axis=1, keepdims=True
    )
    keep(tgt_out, tgt_h_out)
    for h in range(hh):
        net.wait(f"W{h}", ws_h.at[1 - v, h], V)
    net.drain()
    for copy in kept:
        copy.wait()


def finish_kernel(ws, src_in, tgt_in, weight_out, src_out, tgt_out):
    parts, hh = ws.shape[0], ws.shape[1]
    for k in range(parts):
        for h in range(hh):
            n = (k * hh + h) * HEAD_DIM
            weight_out[:, n : n + HEAD_DIM] = ws[k, h].astype(F32)
    quarters, mq = src_in.shape[0], src_in.shape[2]
    for n in range(quarters):
        src_out[:, n * mq : (n + 1) * mq] = src_in[n]
    tgt_out[...] = tgt_in[...]


def grid_body(
    target_rows, source_rows, norm_gain, query_weight, key_weight, value_weight, output_weight,
    saved_output, norm_offset, output_grad
):
    tp, sp = lax.axis_size("tp"), lax.axis_size("sp")
    model, width = query_weight.shape
    heads = width // HEAD_DIM
    hh, half = heads // 2, width // 2
    rows, srows = target_rows.shape[0], source_rows.shape[0]
    block, sblock, sw = rows * tp, srows * tp, model // sp
    dma, vm = pltpu.SemaphoreType.DMA, pltpu.VMEM
    whole = pl.BlockSpec(memory_space=pl.ANY)
    quarters = len(Y_FIRST)
    mq = model // quarters
    ws, source_grad, target_grad = pl.pallas_call(
        functools.partial(grid_kernel, sp, tp, math.log(sblock * sp)),
        out_shape=[
            jax.ShapeDtypeStruct((2, hh, sw, HEAD_DIM), BF),
            jax.ShapeDtypeStruct((quarters, srows, mq), F32),
            jax.ShapeDtypeStruct((rows, model), F32),
        ],
        in_specs=[whole] * 10,
        out_specs=[whole] * 3,
        scratch_shapes=[vm((rows, model), BF), vm((model,), BF), vm((block, width), BF), vm((heads, block), BF)]
        + [vm((quarters, srows, mq), F32), vm((rows, model), F32)]
        + [vm((tp, rows, model), BF)] * 2
        + [vm((2, tp, srows, model), BF)]
        + [vm((2, 2, rows, 2 * sw), BF), vm((sp, tp, rows, 2 * sw), BF)]
        + [vm((2, block, half), BF)] * 2
        + [vm((2, 16, 2 * block), BF)]
        + [vm((2, 2, 2, block, half), BF)] * 2
        + [vm((2, 2, 2, 16, 2 * block), BF)]
        + [vm((model, width), BF)] * 2
        + [vm((width, model), BF)]
        + [vm((2 * sblock, width), BF)]
        + [vm((hh, 2 * sblock, 4 * block), BF)] * 2
        + [vm((2, 2, hh, 2, block, HEAD_DIM), BF)]
        + [vm((2, hh, 2, block, HEAD_DIM), BF)] * 3
        + [vm((2, 2, hh, 2, block, HEAD_DIM), BF)]
        + [vm((2, hh, block, HEAD_DIM), BF)]
        + [vm((2 * sblock, width), F32), vm((2 * sblock, width), BF)]
        + [vm((quarters, 4, 2, srows, mq), BF)]
        + [vm((quarters, 4, srows, mq), BF)] * 2
        + [vm((quarters, 2, srows, mq), BF)]
        + [vm((quarters, srows, mq), BF)] * 2
        + [vm((block, model), F32)]
        + [vm((tp, rows, model), BF)]
        + [vm((3, rows, model), BF)]
        + [vm((hh, 2, sw, HEAD_DIM), BF)]
        + [dma((10,)), dma((quarters + hh + 1,)), dma((SENDS,)), dma((54 + 11 * hh,))],
        name="grid_kernel",
        compiler_params=pltpu.CompilerParams(
            collective_id=1, has_side_effects=True, vmem_limit_bytes=58 * 2**20
        ),
    )(
        target_rows, output_grad, source_rows, norm_gain, saved_output, norm_offset.T,
        query_weight, key_weight, value_weight, output_weight,
    )
    weight_grad, source_grad, target_grad = pl.pallas_call(
        finish_kernel,
        out_shape=[
            jax.ShapeDtypeStruct((sw, width), F32),
            jax.ShapeDtypeStruct((srows, model), F32),
            jax.ShapeDtypeStruct((rows, model), F32),
        ],
        in_specs=[VMEM] * 3,
        out_specs=[VMEM] * 3,
        name="finish_kernel",
    )(ws, source_grad, target_grad)
    return (target_grad, source_grad, weight_grad)


def on_grid(target_rows, query_weight):
    pairs = (lax.axis_size("sp"), lax.axis_size("tp")) == (2**3, 2**2)
    heads = query_weight.shape[1] // HEAD_DIM
    return pairs and heads % 2 == 0 and 2 * target_rows.shape[0] * lax.axis_size("tp") % 128 == 0


def layer(*args):
    return (grid_body if on_grid(args[0], args[3]) else body)(*args)


def solution(mesh):
    in_specs = (
        P(("sp", "tp"), None),
        P(("sp", "tp"), None),
        P(),
        P(None, "tp"),
        P(None, "tp"),
        P(None, "tp"),
        P("tp", None),
        P("sp", "tp"),
        P("sp", "tp"),
        P(("sp", "tp"), None),
    )
    out_specs = (P(("sp", "tp"), None), P(("sp", "tp"), None), P("sp", "tp"))
    return jax.shard_map(layer, mesh=mesh, in_specs=in_specs, out_specs=out_specs, check_vma=False)
```
